256 devices in a mesh: sp: 32 (over z, x), tp: 4 (over y), dp: 2 (over core).
Axes of the slice: x: 4, y: 4, z: 8, core: 2. Of those that a mesh axis runs over, the one named last changes fastest.
Arguments:
- latents: bfloat16 [2, 8192, 4096], P('dp', ('sp', 'tp')), may hold values from -8 to 8
- cond: bfloat16 [2, 4096], P('dp', 'sp'), may hold values from -6 to 6
- cond_ctx: bfloat16 [4096], P('sp'), may hold values from -6 to 6
- context: bfloat16 [2, 1024, 4096], P('dp', 'sp'), may hold values from -8 to 8
- w_shift: bfloat16 [4096, 4096], P('sp', 'tp'), may hold values from -0.09375 to 0.09375
- w_scale: bfloat16 [4096, 4096], P('sp', 'tp'), may hold values from -0.09375 to 0.09375
- w_gate: bfloat16 [4096, 4096], P('sp', 'tp'), may hold values from -0.1875 to 0.1875
- gain_pre: bfloat16 [4096], replicated, may hold values from 0.099609375 to 1.8984375
- gain_post: bfloat16 [4096], replicated, may hold values from 0.099609375 to 1.8984375
- w_query: bfloat16 [4096, 1024], P('dp', 'tp'), may hold values from -0.09375 to 0.09375
- w_key: bfloat16 [4096, 1024], P('dp', 'tp'), may hold values from -0.09375 to 0.09375
- w_value: bfloat16 [4096, 2048], P('dp', 'tp'), may hold values from -0.09375 to 0.09375
- w_outgate: bfloat16 [4096, 2048], P('dp', 'tp'), may hold values from -0.09375 to 0.09375
- w_down: bfloat16 [4096, 32], replicated, may hold values from -0.25 to 0.25
- decay_up: bfloat16 [2, 16, 1024], P(None, None, 'tp'), may hold values from -1.5 to 1.5
- decay_bias: float32 [2, 1024], P(None, 'tp'), may hold values from -0.5 to 11
- head_gain: bfloat16 [2048], P('tp'), may hold values from 0.099609375 to 1.8984375
- w_out: bfloat16 [2048, 4096], P('tp', 'dp'), may hold values from -0.125 to 0.125
Outputs:
- mixer_out: bfloat16 [2, 8192, 4096], P('dp', ('sp', 'tp'))
The draws below stay inside these ranges and needn't reach their ends.
All inputs are finite; a program needn't handle non-finite values.
Results may differ from the reference program's by a relative error of at most 0.015.
Values may be sent and summed in bfloat16 or wider, within the bound.
A program may use at most 128 MiB of HBM per device.

```python
import jax
import jax.numpy as jnp
from jax import lax

D = 4096
HEADS = 4
DK_HEAD = 256
DV_HEAD = 512
RANK = 16
BLOCK = 128
CTX = 1024
TOK_DEV = 256
SAMPLES = 2
TOKENS = 8192
DK = 1024
DVAL = 2048
N_TP = 4


def draw_latents(key, part):
    key_noise, key_offset = jax.random.split(key, 2)
    noise_field = jax.random.normal(key_noise, (SAMPLES, TOKENS, D), jnp.float32)
    offsets = 0.25 * jax.random.normal(key_offset, (SAMPLES, TOKENS // TOK_DEV, 1, D), jnp.float32)
    shifted = noise_field.reshape(SAMPLES, TOKENS // TOK_DEV, TOK_DEV, D) + offsets
    return jnp.clip(shifted.reshape(SAMPLES, TOKENS, D), -8.0, 8.0).astype(jnp.bfloat16)


def draw_context(key, part):
    key_noise = jax.random.fold_in(jax.random.fold_in(key, 7), 0)
    noise_field = jax.random.normal(key_noise, (SAMPLES, CTX, D), jnp.float32)
    return jnp.clip(noise_field, -8.0, 8.0).astype(jnp.bfloat16)


def draw_decay_bias(key, part):
    key_pick, key_fast, key_middle, key_slow = jax.random.split(jax.random.fold_in(key, 11), 4)
    picks = jax.random.randint(key_pick, (2, DK), 0, 10)
    fast_values = jax.random.uniform(key_fast, (2, DK), jnp.float32, -0.5, 1.5)
    fast_share = 3
    middle_share = 7
    middle_values = jax.random.uniform(key_middle, (2, DK), jnp.float32, 7.5, 9.5)
    slow_values = jax.random.uniform(key_slow, (2, DK), jnp.float32, 9.5, 11.0)
    chosen = jnp.where(picks < fast_share, fast_values, jnp.where(picks < middle_share, middle_values, slow_values))
    return chosen.astype(jnp.float32)


def shard_levels(own_key, extent, pieces, smallest, top_value):
    loudness = 1.0
    for position, blocks in pieces:
        draws = jax.random.uniform(jax.random.fold_in(jax.random.fold_in(own_key, 6), position), (blocks,), jnp.float32, smallest / len(pieces), top_value / len(pieces))
        loudness = loudness * jnp.repeat(jnp.exp(draws), extent[position] // blocks).reshape((-1,) + (1,) * (len(extent) - 1 - position))
    return loudness


def scatter_about(rng, extent, scale, most, cuts=(), held_as=jnp.bfloat16):
    values = scale * jax.random.normal(rng, extent, jnp.float32)
    if cuts:
        values = values * shard_levels(rng, extent, cuts, -0.22, 0.18)
    return jnp.clip(values, -most, most).astype(held_as)


def setup_inputs(seed: int = 0) -> dict:
    arg_keys = jax.random.split(jax.random.key(seed), 19)
    latents = draw_latents(jax.random.fold_in(arg_keys[18], 71), 0)
    cond = scatter_about(arg_keys[1], (SAMPLES, D), 1.0, 6.0, ((0, 2), (1, 32)))
    cond_ctx = scatter_about(arg_keys[2], (D,), 1.0, 6.0, ((0, 32),))
    context = draw_context(jax.random.fold_in(arg_keys[18], 71), 0)
    w_shift = scatter_about(arg_keys[4], (D, D), D ** -0.5, 0.09375, ((0, 32), (1, 4)))
    w_scale = scatter_about(arg_keys[5], (D, D), D ** -0.5, 0.09375, ((0, 32), (1, 4)))
    w_gate = scatter_about(arg_keys[6], (D, D), (D // 4) ** -0.5, 0.1875, ((0, 32), (1, 4)))
    gain_pre = jnp.clip(1.0 + 0.18 * jax.random.normal(arg_keys[7], (D,), jnp.float32), 0.099609375, 1.8984375).astype(jnp.bfloat16)
    gain_post = jnp.clip(1.0 + 0.18 * jax.random.normal(arg_keys[8], (D,), jnp.float32), 0.099609375, 1.8984375).astype(jnp.bfloat16)
    w_query = scatter_about(arg_keys[9], (D, DK), D ** -0.5, 0.09375, ((0, 2), (1, 4)))
    w_key = scatter_about(arg_keys[10], (D, DK), D ** -0.5, 0.09375, ((0, 2), (1, 4)))
    w_value = scatter_about(arg_keys[11], (D, DVAL), D ** -0.5, 0.09375, ((0, 2), (1, 4)))
    w_outgate = scatter_about(arg_keys[12], (D, DVAL), D ** -0.5, 0.09375, ((0, 2), (1, 4)))
    w_down = scatter_about(arg_keys[13], (D, 2 * RANK), (D // 9) ** -0.5, 0.25)
    decay_up = scatter_about(arg_keys[14], (2, RANK, DK), RANK ** -0.5, 1.5, ((2, 4),))
    decay_bias = draw_decay_bias(jax.random.fold_in(arg_keys[18], 71), 0)
    head_gain = jnp.clip(1.0 + 0.18 * jax.random.normal(arg_keys[16], (DVAL,), jnp.float32), 0.099609375, 1.8984375).astype(jnp.bfloat16)
    w_out = scatter_about(arg_keys[17], (DVAL, D), DVAL ** -0.5, 0.125, ((0, 4), (1, 2)))
    return dict(latents=latents, cond=cond, cond_ctx=cond_ctx, context=context, w_shift=w_shift, w_scale=w_scale, w_gate=w_gate, gain_pre=gain_pre, gain_post=gain_post, w_query=w_query, w_key=w_key, w_value=w_value, w_outgate=w_outgate, w_down=w_down, decay_up=decay_up, decay_bias=decay_bias, head_gain=head_gain, w_out=w_out)


EPS = 1e-06
TAU = 16.0
HIGH_ACCURACY = lax.Precision.HIGHEST

def matmul(left, right):
    return jnp.dot(left, right, preferred_element_type=jnp.float32)

def rms_scale(vectors, gain):
    return vectors * lax.rsqrt(lax.optimization_barrier(jnp.mean(vectors * vectors, axis=-1, keepdims=True)) + EPS) * gain

def log_decays(lowrank, decay_up, decay_bias):
    result = []
    for direction in range(2):
        preact = matmul(lowrank[:, direction * RANK:(direction + 1) * RANK], decay_up[direction]) + decay_bias[direction]
        result.append(jax.nn.log_sigmoid(preact) / TAU)
    return result

def context_states(ctx_keys, ctx_values, forward_decay, backward_decay):
    keys_float = ctx_keys.astype(jnp.float32)
    values_float = ctx_values.astype(jnp.float32)
    running_decay_sum = jnp.cumsum(forward_decay, axis=0)
    weight_fwd = jnp.exp(running_decay_sum[-1:] - running_decay_sum)
    weight_bwd = jnp.exp(jnp.cumsum(backward_decay, axis=0) - backward_decay)
    start_fwd = jnp.dot((keys_float * weight_fwd).T, values_float, precision=HIGH_ACCURACY)
    start_bwd = jnp.dot((keys_float * weight_bwd).T, values_float, precision=HIGH_ACCURACY)
    return (start_fwd, start_bwd)

def recurrence(queries, keys_in, values, decays, start):
    count = queries.shape[0] // BLOCK

    def blocks(array):
        return array.reshape(count, BLOCK, array.shape[-1])
    causal = jnp.tril(jnp.ones((BLOCK, BLOCK), bool))[:, :, None]

    def advance(carried_state, inputs):
        query_block_tile, key_block_tile, value_block_tile, block_g = inputs
        running_decay_sum = jnp.cumsum(block_g, axis=0)
        decay_pairs = jnp.exp(jnp.where(causal, running_decay_sum[:, None, :] - running_decay_sum[None, :, :], -jnp.inf))
        scores = jnp.einsum('tk,tsk,sk->ts', query_block_tile, decay_pairs, key_block_tile, precision=HIGH_ACCURACY)
        output = jnp.dot(scores, value_block_tile, precision=HIGH_ACCURACY) + jnp.dot(query_block_tile * jnp.exp(running_decay_sum), carried_state, precision=HIGH_ACCURACY)
        final_state_value = running_decay_sum[-1]
        carried_state = carried_state * jnp.exp(final_state_value)[:, None] + jnp.dot((key_block_tile * jnp.exp(final_state_value - running_decay_sum)).T, value_block_tile, precision=HIGH_ACCURACY)
        return (carried_state, output)
    carried_state, output = lax.scan(advance, start, (blocks(queries), blocks(keys_in), blocks(values), blocks(decays)))
    return output.reshape(-1, values.shape[-1])

def reference(latents, cond, cond_ctx, context, w_shift, w_scale, w_gate, gain_pre, gain_post, w_query, w_key, w_value, w_outgate, w_down, decay_up, decay_bias, head_gain, w_out):
    activated = jax.nn.silu(cond.astype(jnp.float32)).astype(jnp.bfloat16)
    activated_ctx = jax.nn.silu(cond_ctx.astype(jnp.float32)).astype(jnp.bfloat16)[None, :]
    shift_vec = matmul(activated, w_shift)
    scale_vec = matmul(activated, w_scale)
    gate_vec = matmul(activated, w_gate)
    shift_ctx = matmul(activated_ctx, w_shift)[0]
    scale_ctx = matmul(activated_ctx, w_scale)[0]
    gain_in = gain_pre.astype(jnp.float32)
    gain_out = gain_post.astype(jnp.float32)
    gains_head = head_gain.astype(jnp.float32)
    heads_dev = HEADS // N_TP
    group_width = heads_dev * DV_HEAD
    outputs = []
    for sample in range(SAMPLES):
        latent_rows = latents[sample].astype(jnp.float32)
        modulated = (rms_scale(latent_rows, gain_in) * (1.0 + scale_vec[sample]) + shift_vec[sample]).astype(jnp.bfloat16)
        ctx_rows = context[sample].astype(jnp.float32)
        modulated_ctx = (rms_scale(ctx_rows, gain_in) * (1.0 + scale_ctx) + shift_ctx).astype(jnp.bfloat16)
        queries = matmul(modulated, w_query).astype(jnp.bfloat16)
        latent_keys = matmul(modulated, w_key).astype(jnp.bfloat16)
        values = matmul(modulated, w_value).astype(jnp.bfloat16)
        out_gate = matmul(modulated, w_outgate).astype(jnp.bfloat16)
        lowrank = matmul(modulated, w_down).astype(jnp.bfloat16)
        ctx_keys = matmul(modulated_ctx, w_key).astype(jnp.bfloat16)
        ctx_values = matmul(modulated_ctx, w_value).astype(jnp.bfloat16)
        ctx_lowrank = matmul(modulated_ctx, w_down).astype(jnp.bfloat16)
        decay_fwd, decay_bwd = log_decays(lowrank, decay_up, decay_bias)
        ctx_fwd, ctx_bwd = log_decays(ctx_lowrank, decay_up, decay_bias)
        head_rows = []
        for head_index in range(HEADS):
            key_lo = head_index * DK_HEAD
            value_lo = head_index * DV_HEAD
            start_fwd, start_bwd = context_states(ctx_keys[:, key_lo:key_lo + DK_HEAD], ctx_values[:, value_lo:value_lo + DV_HEAD], ctx_fwd[:, key_lo:key_lo + DK_HEAD], ctx_bwd[:, key_lo:key_lo + DK_HEAD])
            head_query_rows = queries[:, key_lo:key_lo + DK_HEAD].astype(jnp.float32) * DK_HEAD ** (-0.5)
            head_k = latent_keys[:, key_lo:key_lo + DK_HEAD].astype(jnp.float32)
            head_v = values[:, value_lo:value_lo + DV_HEAD].astype(jnp.float32)
            forward_out = recurrence(head_query_rows, head_k, head_v, decay_fwd[:, key_lo:key_lo + DK_HEAD], start_fwd)
            backward_out = jnp.flip(recurrence(jnp.flip(head_query_rows, 0), jnp.flip(head_k, 0), jnp.flip(head_v, 0), jnp.flip(decay_bwd[:, key_lo:key_lo + DK_HEAD], 0), start_bwd), 0)
            mixed_sum = forward_out + backward_out
            gated_rows = rms_scale(mixed_sum, gains_head[value_lo:value_lo + DV_HEAD]) * jax.nn.silu(out_gate[:, value_lo:value_lo + DV_HEAD].astype(jnp.float32))
            head_rows.append(gated_rows.astype(jnp.bfloat16))
        heads_out = jnp.concatenate(head_rows, axis=1)
        projected = jnp.zeros((TOKENS, D), jnp.float32)
        for group_index in range(N_TP):
            lower = group_index * group_width
            partial_value = matmul(heads_out[:, lower:lower + group_width], w_out[lower:lower + group_width]).astype(jnp.bfloat16)
            partial_value = lax.optimization_barrier(partial_value)
            projected = projected + partial_value.astype(jnp.float32)
        result_rows = latent_rows + gate_vec[sample] * rms_scale(projected, gain_out)
        outputs.append(result_rows.astype(jnp.bfloat16))
    return jnp.stack(outputs)
```

```python
import jax
import jax.numpy as jnp
from jax import lax
from jax.experimental import pallas as pl
from jax.experimental.pallas import tpu as pltpu
from jax.sharding import Mesh
from jax.sharding import PartitionSpec as P

DK_HEAD = 256
DV_HEAD = 512
RANK = 16
BLOCK = 128
SP_TP = ("sp_0", "sp_1", "tp")
SP = ("sp_0", "sp_1")
NZ, NX, NY = 8, 4, 4
WIDTH = 4096
HALF = 2048
ANY = pl.BlockSpec(memory_space=pl.ANY)
VM = pl.BlockSpec(memory_space=pltpu.VMEM)
BF, F32 = jnp.bfloat16, jnp.float32


EPS = 1e-06
TAU = 16.0


def matmul(left, right):
    return jnp.dot(left, right, preferred_element_type=jnp.float32)


def rms_scale(vectors, gain):
    return vectors * lax.rsqrt(jnp.mean(vectors * vectors, axis=-1, keepdims=True) + EPS) * gain


def shape_of(*dims, dtype=BF):
    return jax.ShapeDtypeStruct(dims, dtype)


def send(src, dst, send_sem, recv_sem, **where):
    copy = pltpu.make_async_remote_copy(
        src_ref=src,
        dst_ref=dst,
        send_sem=send_sem,
        recv_sem=recv_sem,
        device_id=where,
        device_id_type=pl.DeviceIdType.MESH,
    )
    copy.start()
    return copy


def greet(partners):
    barrier = pltpu.get_barrier_semaphore()
    for where in partners:
        pl.semaphore_signal(
            barrier, inc=1, device_id=where, device_id_type=pl.DeviceIdType.MESH
        )
    return lambda: pl.semaphore_wait(barrier, len(partners))


def position():
    return tuple(lax.axis_index(a) for a in ("sp_0", "sp_1", "tp", "dp"))


def gather_kernel(
    lat, cond, cond_ctx, w_shift, w_scale, w_gate, wq, wk, wv, wg, wo,
    mods, lat_all, wq2, wk2, wv2, wg2, wo2,
    w_mod, lat_here, partial, arrived, tile,
    load_sem, s1, r1, s2, r2, sl, rl, sw, rw,
):
    z, x, y, c = position()
    at_sp = [
        (k, dict(sp_0=lax.rem(z + k // NX, NZ), sp_1=lax.rem(x + k % NX, NX)))
        for k in range(1, NZ * NX)
    ]
    at_yz = [
        (k, dict(sp_0=lax.rem(z + k // NY, NZ), tp=lax.rem(y + k % NY, NY)))
        for k in range(1, NZ * NY)
    ]
    other = dict(dp=1 - c)
    up, down = dict(tp=lax.rem(y + 1, NY)), dict(tp=lax.rem(y + 3, NY))
    entered = greet(
        [w for _, w in at_sp] + [w for k, w in at_yz if k % NY != 0] + [other]
    )
    loads = [
        pltpu.make_async_copy(src, dst, load_sem.at[k])
        for k, (src, dst) in enumerate(
            [(w_shift, w_mod.at[0]), (w_scale, w_mod.at[1]), (w_gate, w_mod.at[2]),
             (lat, lat_here)]
        )
    ]
    for load in loads:
        load.start()
    own = pltpu.make_async_copy(lat, lat_all.at[y], load_sem.at[4])
    own.start()
    rows = lax.broadcasted_iota(jnp.int32, (16, 128), 0)
    act = jax.nn.silu(cond[...].astype(F32))
    act_ctx = jax.nn.silu(cond_ctx[...].astype(F32))
    total = None
    for k in range(3):
        left = jnp.where(rows == k, act, jnp.where(rows == k + 3, act_ctx, 0.0)).astype(BF)
        loads[k].wait()
        part = matmul(left, w_mod[k])
        total = part if total is None else total + part
    for k in range(NZ):
        partial[k] = total[:8, k * 128 : (k + 1) * 128]
    entered()
    sends = [
        send(partial.at[w["sp_0"]], arrived.at[k], s1.at[k], r1.at[k], **w) for k, w in at_sp
    ]
    loads[3].wait()
    to_up = send(lat_here, lat_all.at[y], sl.at[0], rl.at[0], **up)
    to_down = send(lat_here, lat_all.at[y], sl.at[1], rl.at[1], **down)
    weights = [
        send(src, dst, sw.at[k], rw.at[k], **other)
        for k, (src, dst) in enumerate(
            [(wq, wq2), (wk, wk2), (wv, wv2), (wg, wg2), (wo, wo2)]
        )
    ]
    for copy in sends:
        copy.wait()
    summed = partial[z]
    for k in range(1, NZ * NX):
        summed = summed + arrived[k]
    tile[...] = summed
    here = y * NZ + z
    mods[here] = summed
    sends = [send(tile, mods.at[here], s2.at[k], r2.at[k], **w) for k, w in at_yz]
    for copy in sends:
        copy.wait()
    to_up.wait()
    before = lat_all.at[lax.rem(y + 3, NY), pl.ds(0, 32)]
    relay_up = send(before, before, sl.at[2], rl.at[2], **up)
    to_down.wait()
    after = lat_all.at[lax.rem(y + 1, NY), pl.ds(32, 32)]
    relay_down = send(after, after, sl.at[3], rl.at[3], **down)
    own.wait()
    relay_up.wait()
    relay_down.wait()
    for copy in weights:
        copy.wait()


def gather_inputs(lat, cond, cond_ctx, w_shift, w_scale, w_gate, *weights):
    dma = pltpu.SemaphoreType.DMA
    return pl.pallas_call(
        gather_kernel,
        out_shape=[shape_of(NY * NZ, 8, 128, dtype=F32), shape_of(NY, *lat.shape)]
        + [shape_of(*w.shape) for w in weights],
        in_specs=[ANY, VM, VM] + [ANY] * 8,
        out_specs=[VM, VM] + [ANY] * 5,
        scratch_shapes=[
            pltpu.VMEM((3, 128, 1024), BF),
            pltpu.VMEM(lat.shape, BF),
            pltpu.VMEM((NZ, 8, 128), F32),
            pltpu.VMEM((NZ * NX, 8, 128), F32),
            pltpu.VMEM((8, 128), F32),
            dma((5,)), dma((32,)), dma((32,)), dma((32,)), dma((32,)),
            dma((4,)), dma((4,)), dma((5,)), dma((5,)),
        ],
        compiler_params=pltpu.CompilerParams(collective_id=0, has_side_effects=True),
        name="gather_inputs",
    )(lat, cond, cond_ctx, w_shift, w_scale, w_gate, *weights)


def exchange_x_kernel(count, *refs):
    ins, outs, (s, r) = refs[:count], refs[count : 2 * count], refs[2 * count :]
    x = lax.axis_index("sp_1")
    peers = [(d, lax.rem(x + d, NX)) for d in range(1, NX)]
    entered = greet([dict(sp_1=p) for _, p in peers])
    for a, b in zip(ins, outs):
        b[x] = a[x]
    entered()
    copies = [
        send(a.at[p], b.at[x], s.at[k, d], r.at[k, d], sp_1=p)
        for k, (a, b) in enumerate(zip(ins, outs))
        for d, p in peers
    ]
    for copy in copies:
        copy.wait()


def exchange_x(collective_id, *arrays):
    n = len(arrays)
    return pl.pallas_call(
        lambda *refs: exchange_x_kernel(n, *refs),
        out_shape=[shape_of(*a.shape, dtype=a.dtype) for a in arrays],
        in_specs=[VM] * n,
        out_specs=[VM] * n,
        scratch_shapes=[pltpu.SemaphoreType.DMA((n, NX))] * 2,
        compiler_params=pltpu.CompilerParams(
            collective_id=collective_id, has_side_effects=True
        ),
        name=f"exchange_x_{collective_id}",
    )(*arrays)


def scan_z_kernel(group, decays, entry, got, got_decays, back, s, r, s_dec, r_dec, s_back, r_back):
    z = lax.axis_index("sp_0")
    peers = [(d, lax.rem(z + d, NZ)) for d in range(1, NZ)]
    entered = greet([dict(sp_0=p) for _, p in peers])
    got[z] = group[z]
    got_decays[z] = decays[...]
    entered()
    copies = []
    for d, p in peers:
        copies.append(send(group.at[p], got.at[z], s.at[d], r.at[d], sp_0=p))
        copies.append(send(decays, got_decays.at[z], s_dec.at[d], r_dec.at[d], sp_0=p))
    for copy in copies:
        copy.wait()
    for way in range(2):
        order = range(NZ) if way == 0 else range(NZ - 1, -1, -1)
        state = jnp.zeros((16, 256), F32)
        for k in order:
            state = state * jnp.exp(got_decays[k, 2 + way : 3 + way]) + got[k, 2 + way].astype(F32)
        for k in order:
            back[k, way] = state.astype(BF)
            state = state * jnp.exp(got_decays[k, way : way + 1]) + got[k, way].astype(F32)
    entry[z] = back[z]
    copies = [send(back.at[p], entry.at[z], s_back.at[d], r_back.at[d], sp_0=p) for d, p in peers]
    for copy in copies:
        copy.wait()


def scan_z(group, decays):
    dma = pltpu.SemaphoreType.DMA((NZ,))
    return pl.pallas_call(
        scan_z_kernel,
        out_shape=shape_of(NZ, 2, 16, 256),
        in_specs=[VM, VM],
        out_specs=VM,
        scratch_shapes=[
            pltpu.VMEM((NZ, 4, 16, 256), BF),
            pltpu.VMEM((NZ, 8, 256), F32),
            pltpu.VMEM((NZ, 2, 16, 256), BF),
        ]
        + [dma] * 6,
        compiler_params=pltpu.CompilerParams(collective_id=2, has_side_effects=True),
        name="scan_z",
    )(group, decays)


def reduce_y_kernel(pa, pb, out_a, out_b, near_a, near_b, far_a, far_b, sum_a, sum_b, relay_a, relay_b, s, r):
    y = lax.axis_index("tp")
    above, below, across = (lax.rem(y + k, NY) for k in (1, 3, 2))
    up, down = dict(tp=above), dict(tp=below)
    greet([up, down])()
    first_a = send(pa.at[across], relay_a, s.at[0], r.at[0], **down)
    first_b = send(pb.at[across], relay_b, s.at[1], r.at[1], **up)
    direct_b = send(pb.at[below], near_b, s.at[2], r.at[2], **down)
    direct_a = send(pa.at[above], near_a, s.at[3], r.at[3], **up)
    first_a.wait()
    sum_a[...] = (relay_a[...].astype(F32) + pa[below].astype(F32)).astype(BF)
    second_a = send(sum_a, far_a, s.at[4], r.at[4], **down)
    first_b.wait()
    sum_b[...] = (relay_b[...].astype(F32) + pb[above].astype(F32)).astype(BF)
    second_b = send(sum_b, far_b, s.at[5], r.at[5], **up)
    direct_a.wait()
    direct_b.wait()
    second_a.wait()
    out_a[...] = pa[y].astype(F32) + near_a[...].astype(F32) + far_a[...].astype(F32)
    second_b.wait()
    out_b[...] = pb[y].astype(F32) + near_b[...].astype(F32) + far_b[...].astype(F32)


def reduce_y(pa, pb):
    block = pltpu.VMEM(pa.shape[1:], BF)
    dma = pltpu.SemaphoreType.DMA((6,))
    return pl.pallas_call(
        reduce_y_kernel,
        out_shape=[shape_of(*pa.shape[1:], dtype=F32)] * 2,
        in_specs=[VM, VM],
        out_specs=[VM, VM],
        scratch_shapes=[block] * 8 + [dma] * 2,
        compiler_params=pltpu.CompilerParams(collective_id=4, has_side_effects=True),
        name="reduce_y",
    )(pa, pb)


def log_decays(lowrank, decay_up, decay_bias):
    return [
        jax.nn.log_sigmoid(
            matmul(lowrank[:, way * RANK : (way + 1) * RANK], decay_up[way]) + decay_bias[way]
        )
        / TAU
        for way in range(2)
    ]


def running_sums(decay_fwd, decay_bwd):
    n = decay_fwd.shape[0]
    lower = jnp.tril(jnp.ones((n, n), F32))
    fwd = jnp.dot(lower, decay_fwd, precision=lax.Precision.HIGHEST)
    bwd = jnp.dot(lower.T, decay_bwd, precision=lax.Precision.HIGHEST)
    return fwd, bwd


def across(left, right):
    return lax.dot_general(left, right, (((1,), (1,)), ((), ())), preferred_element_type=F32)


def outer(left, right):
    return lax.dot_general(left, right, (((0,), (0,)), ((), ())), preferred_element_type=F32)


def scores_of(queries, keys_in, fwd, bwd):
    tri = jnp.tril(jnp.ones((BLOCK, BLOCK), bool))
    bf = lambda a: a.astype(BF)
    rows = []
    for b in range(2):
        sl = slice(b * BLOCK, (b + 1) * BLOCK)
        q, k, f, g = queries[sl], keys_in[sl], fwd[sl], bwd[sl]
        cf, cg = f[BLOCK // 2 : BLOCK // 2 + 1], g[BLOCK // 2 - 1 : BLOCK // 2]
        sf = across(bf(q * jnp.exp(f - cf)), bf(k * jnp.exp(cf - f)))
        sb = across(bf(q * jnp.exp(g - cg)), bf(k * jnp.exp(cg - g)))
        near = jnp.where(tri, sf, 0.0) + jnp.where(tri.T, sb, 0.0)
        osl = slice((1 - b) * BLOCK, (2 - b) * BLOCK)
        if b == 0:
            edge = bwd[BLOCK : BLOCK + 1]
            far = across(bf(q * jnp.exp(g - edge)), bf(keys_in[osl] * jnp.exp(edge - bwd[osl])))
            rows.append(jnp.concatenate([near, far], axis=1))
        else:
            edge = fwd[BLOCK - 1 : BLOCK]
            far = across(bf(q * jnp.exp(f - edge)), bf(keys_in[osl] * jnp.exp(edge - fwd[osl])))
            rows.append(jnp.concatenate([far, near], axis=1))
    return jnp.concatenate(rows, axis=0)


def body(
    latents, cond, cond_ctx, context, w_shift, w_scale, w_gate, gain_pre, gain_post,
    w_query, w_key, w_value, w_outgate, w_down, decay_up, decay_bias, head_gain, w_out,
):
    z, x, y, c = position()
    latents, context = latents[0], context[0]
    mods, lat_all, wq2, wk2, wv2, wg2, wo2 = gather_inputs(
        latents, cond, cond_ctx[None], w_shift, w_scale, w_gate,
        w_query, w_key, w_value, w_outgate, w_out,
    )
    mods = jnp.moveaxis(mods, 0, 1).reshape(8, WIDTH)
    shift_vec, scale_vec, gate_vec, shift_ctx, scale_ctx = (mods[k : k + 1] for k in range(5))
    gain_in = gain_pre.astype(F32)

    def halves(array):
        return (
            lax.dynamic_slice_in_dim(array, c * HALF, HALF, 1),
            lax.dynamic_slice_in_dim(array, (1 - c) * HALF, HALF, 1),
        )

    def project(rows, here, there):
        mine, theirs = rows
        return (matmul(mine, here) + matmul(theirs, there)).astype(BF)

    rows = lat_all.reshape(NY * latents.shape[0], WIDTH).astype(F32)
    modulated = (rms_scale(rows, gain_in) * (1.0 + scale_vec) + shift_vec).astype(BF)
    lowrank = matmul(modulated, w_down).astype(BF)
    modulated = halves(modulated)
    queries = project(modulated, w_query, wq2)
    keys_in = project(modulated, w_key, wk2)
    values = project(modulated, w_value, wv2)
    out_gate = project(modulated, w_outgate, wg2)
    ctx_rows = context.astype(F32)
    modulated_ctx = (rms_scale(ctx_rows, gain_in) * (1.0 + scale_ctx) + shift_ctx).astype(BF)
    ctx_lowrank = matmul(modulated_ctx, w_down).astype(BF)
    modulated_ctx = halves(modulated_ctx)
    ctx_keys = project(modulated_ctx, w_key, wk2)
    ctx_values = project(modulated_ctx, w_value, wv2)

    fwd, bwd = running_sums(*log_decays(lowrank, decay_up, decay_bias))
    q = queries.astype(F32) * DK_HEAD ** (-0.5)
    k = keys_in.astype(F32)
    scores = scores_of(q, k, fwd, bwd)
    out = matmul(scores.astype(BF), values)
    state_f = outer(values, (k * jnp.exp(fwd[-1:] - fwd)).astype(BF)).astype(BF)
    state_b = outer(values, (k * jnp.exp(bwd[:1] - bwd)).astype(BF)).astype(BF)
    states = jnp.stack(
        [state_f.reshape(NX, 128, DK_HEAD), state_b.reshape(NX, 128, DK_HEAD)], axis=1
    )
    totals = jnp.concatenate([fwd[-1:], bwd[:1], jnp.zeros((6, DK_HEAD), F32)], axis=0)
    totals = jnp.broadcast_to(totals[None], (NX, 8, DK_HEAD))
    ctx_count = context.shape[0]
    ctx_pack = jnp.concatenate(
        [
            jnp.broadcast_to(ctx_keys[None], (NX, ctx_count, DK_HEAD)),
            jnp.moveaxis(ctx_values.reshape(ctx_count, NX, 128), 1, 0),
            jnp.broadcast_to(
                jnp.pad(ctx_lowrank, ((0, 0), (0, 128 - 2 * RANK)))[None], (NX, ctx_count, 128)
            ),
        ],
        axis=2,
    )
    states, totals, ctx_pack = exchange_x(1, states, totals, ctx_pack)

    ctx_pack = ctx_pack.reshape(NX * ctx_count, 512)
    ctx_k = ctx_pack[:, :DK_HEAD].astype(F32)
    ctx_v = ctx_pack[:, DK_HEAD : DK_HEAD + 128]
    ctx_lr = ctx_pack[:, DK_HEAD + 128 : DK_HEAD + 128 + 2 * RANK]
    cf, cb = running_sums(*log_decays(ctx_lr, decay_up, decay_bias))
    ctx_f = outer(ctx_v, (ctx_k * jnp.exp(cf[-1:] - cf)).astype(BF))
    ctx_b = outer(ctx_v, (ctx_k * jnp.exp(cb[:1] - cb)).astype(BF))

    def inside(way, order):
        state = jnp.zeros((128, DK_HEAD), F32)
        decay = jnp.zeros((1, DK_HEAD), F32)
        before, passed = [None] * NX, [None] * NX
        for j in order:
            before[j], passed[j] = state, decay
            step = totals[j, way : way + 1]
            state = state * jnp.exp(step) + states[j, way].astype(F32)
            decay = decay + step
        return state, decay, before, passed

    group_f, total_f, before_f, passed_f = inside(0, range(NX))
    group_b, total_b, before_b, passed_b = inside(1, range(NX - 1, -1, -1))
    group = jnp.stack([group_f, group_b, ctx_f, ctx_b]).astype(BF)
    group = jnp.moveaxis(group.reshape(4, NZ, 16, DK_HEAD), 1, 0)
    group_decays = jnp.concatenate(
        [total_f, total_b, cf[-1:], cb[:1], jnp.zeros((4, DK_HEAD), F32)], axis=0
    )
    entry = scan_z(group, group_decays)
    entry = jnp.moveaxis(entry, 1, 0).reshape(2, 128, DK_HEAD).astype(F32)
    entries = jnp.stack(
        [
            jnp.stack(
                [
                    entry[0] * jnp.exp(passed_f[j]) + before_f[j],
                    entry[1] * jnp.exp(passed_b[j]) + before_b[j],
                ]
            )
            for j in range(NX)
        ]
    ).astype(BF)
    (entries,) = exchange_x(3, entries)
    entries = jnp.moveaxis(entries, 1, 0).reshape(2, DV_HEAD, DK_HEAD)
    out = out + across((q * jnp.exp(fwd)).astype(BF), entries[0])
    out = out + across((q * jnp.exp(bwd)).astype(BF), entries[1])

    gated = rms_scale(out, head_gain.astype(F32)[None]) * jax.nn.silu(out_gate.astype(F32))
    heads_out = gated.astype(BF)
    shape = (NY, latents.shape[0], HALF)
    pa = matmul(heads_out, w_out).astype(BF).reshape(shape)
    pb = matmul(heads_out, wo2).astype(BF).reshape(shape)
    mine, theirs = reduce_y(pa, pb)
    first = c == 0
    projected = jnp.concatenate(
        [jnp.where(first, mine, theirs), jnp.where(first, theirs, mine)], axis=1
    )
    result = latents.astype(F32) + gate_vec * rms_scale(projected, gain_post.astype(F32))
    return result.astype(BF)[None]


def solution(mesh):
    finer = Mesh(
        mesh.devices.reshape(8, 4, mesh.shape["tp"], mesh.shape["dp"]), ("sp_0", "sp_1", "tp", "dp")
    )
    in_specs = (
        P("dp", SP_TP, None),
        P("dp", SP),
        P(SP),
        P("dp", SP, None),
        P(SP, "tp"),
        P(SP, "tp"),
        P(SP, "tp"),
        P(),
        P(),
        P("dp", "tp"),
        P("dp", "tp"),
        P("dp", "tp"),
        P("dp", "tp"),
        P(),
        P(None, None, "tp"),
        P(None, "tp"),
        P("tp"),
        P("tp", "dp"),
    )
    out_specs = P("dp", SP_TP, None)
    return jax.shard_map(body, mesh=finer, in_specs=in_specs, out_specs=out_specs, check_vma=False)
```

```python
import jax
import jax.numpy as jnp
from jax import lax
from jax.experimental import pallas as pl
from jax.experimental.pallas import tpu as pltpu
from jax.sharding import Mesh
from jax.sharding import PartitionSpec as P

DK_HEAD = 256
DV_HEAD = 512
RANK = 16
BLOCK = 128
SP_TP = ("sp_0", "sp_1", "tp")
SP = ("sp_0", "sp_1")
NZ, NX, NY = 8, 4, 4
WIDTH = 4096
HALF = 2048
ANY = pl.BlockSpec(memory_space=pl.ANY)
VM = pl.BlockSpec(memory_space=pltpu.VMEM)
BF, F32 = jnp.bfloat16, jnp.float32


EPS = 1e-06
TAU = 16.0


def matmul(left, right):
    return jnp.dot(left, right, preferred_element_type=jnp.float32)


def rms_scale(vectors, gain):
    return vectors * lax.rsqrt(jnp.mean(vectors * vectors, axis=-1, keepdims=True) + EPS) * gain


def shape_of(*dims, dtype=BF):
    return jax.ShapeDtypeStruct(dims, dtype)


def send(src, dst, send_sem, recv_sem, **where):
    copy = pltpu.make_async_remote_copy(
        src_ref=src,
        dst_ref=dst,
        send_sem=send_sem,
        recv_sem=recv_sem,
        device_id=where,
        device_id_type=pl.DeviceIdType.MESH,
    )
    copy.start()
    return copy


def greet(partners):
    barrier = pltpu.get_barrier_semaphore()
    for where in partners:
        pl.semaphore_signal(
            barrier, inc=1, device_id=where, device_id_type=pl.DeviceIdType.MESH
        )
    return lambda: pl.semaphore_wait(barrier, len(partners))


def position():
    return tuple(lax.axis_index(a) for a in ("sp_0", "sp_1", "tp", "dp"))


def gather_kernel(
    lat, context, cond, cond_ctx, gain_pre, w_shift, w_scale, w_gate, wq, wk, wv, wg, wo,
    mods, rows, wq2, wk2, wv2, wg2, wo2,
    w_mod, lat_all, partial, arrived, tile,
    load_sem, s1, r1, s2, r2, sl, rl, sw, rw,
):
    z, x, y, c = position()
    at_sp = [
        (k, dict(sp_0=lax.rem(z + k // NX, NZ), sp_1=lax.rem(x + k % NX, NX)))
        for k in range(1, NZ * NX)
    ]
    at_yz = [
        (k, dict(sp_0=lax.rem(z + k // NY, NZ), tp=lax.rem(y + k % NY, NY)))
        for k in range(1, NZ * NY)
    ]
    other = dict(dp=1 - c)
    above, below, facing = (lax.rem(y + k, NY) for k in (1, 3, 2))
    up, down = dict(tp=above), dict(tp=below)
    entered = greet(
        [w for _, w in at_sp] + [w for k, w in at_yz if k % NY != 0] + [other]
    )
    loads = [
        pltpu.make_async_copy(src, dst, load_sem.at[k])
        for k, (src, dst) in enumerate(
            [(w_shift, w_mod.at[0]), (w_scale, w_mod.at[1]), (w_gate, w_mod.at[2]),
             (lat, lat_all.at[y])]
        )
    ]
    for load in loads:
        load.start()
    line = lax.broadcasted_iota(jnp.int32, (16, 128), 0)
    act = jax.nn.silu(cond[...].astype(F32)).astype(BF).astype(F32)
    act_ctx = jax.nn.silu(cond_ctx[...].astype(F32)).astype(BF).astype(F32)
    total = None
    for k in range(3):
        left = jnp.where(line == k, act, jnp.where(line == k + 3, act_ctx, 0.0)).astype(BF)
        loads[k].wait()
        part = matmul(left, w_mod[k])
        total = part if total is None else total + part
    for k in range(NZ):
        partial[k] = total[:8, k * 128 : (k + 1) * 128]
    loads[3].wait()
    entered()
    sends = [
        send(partial.at[w["sp_0"]], arrived.at[k], s1.at[k], r1.at[k], **w) for k, w in at_sp
    ]
    own = lat_all.at[y]
    to_up = send(own, own, sl.at[0], rl.at[0], **up)
    to_down = send(own, own, sl.at[1], rl.at[1], **down)
    weights = [
        send(src, dst, sw.at[k], rw.at[k], **other)
        for k, (src, dst) in enumerate(
            [(wk, wk2), (wv, wv2), (wq, wq2), (wg, wg2), (wo, wo2)]
        )
    ]
    for copy in sends:
        copy.wait()
    summed = partial[z]
    for k in range(1, NZ * NX):
        summed = summed + arrived[k]
    tile[...] = summed
    here = mods.at[:, pl.ds(pl.multiple_of((y * NZ + z) * 128, 128), 128)]
    here[...] = summed
    sends = [send(tile, here, s2.at[k], r2.at[k], **w) for k, w in at_yz]
    to_up.wait()
    before = lat_all.at[below, pl.ds(0, 32)]
    relay_up = send(before, before, sl.at[2], rl.at[2], **up)
    to_down.wait()
    after = lat_all.at[above, pl.ds(32, 32)]
    relay_down = send(after, after, sl.at[3], rl.at[3], **down)
    for copy in sends:
        copy.wait()
    columns = [pl.ds(pl.multiple_of(k * HALF, HALF), HALF) for k in (c, 1 - c)]

    def modulate(source, target, scale_row, shift_row, length):
        def step(k, carry):
            at = pl.ds(pl.multiple_of(k * 16, 16), 16)
            to = pl.ds(pl.multiple_of(target + k * 16, 16), 16)
            halves = [source[at, columns[h]].astype(F32) for h in range(2)]
            square = sum(jnp.sum(v * v, axis=1, keepdims=True) for v in halves)
            norm = lax.rsqrt(square / WIDTH + EPS)
            for h in range(2):
                weight = gain_pre[:, columns[h]].astype(F32) * (
                    1.0 + mods[scale_row : scale_row + 1, columns[h]]
                )
                shift = mods[shift_row : shift_row + 1, columns[h]]
                rows[h, to] = (halves[h] * norm * weight + shift).astype(BF)
            return carry

        lax.fori_loop(0, length // 16, step, 0)

    modulate(context, NY * 64, 4, 3, 32)
    for block in (y, below, above):
        modulate(lat_all.at[block], block * 64, 1, 0, 64)
    relay_up.wait()
    relay_down.wait()
    modulate(lat_all.at[facing], facing * 64, 1, 0, 64)
    for copy in weights:
        copy.wait()


def gather_inputs(lat, context, cond, cond_ctx, gain, w_shift, w_scale, w_gate, *weights):
    dma = pltpu.SemaphoreType.DMA
    return pl.pallas_call(
        gather_kernel,
        out_shape=[shape_of(8, WIDTH, dtype=F32), shape_of(2, NY * 64 + 32, HALF)]
        + [shape_of(*w.shape) for w in weights],
        in_specs=[ANY, VM, VM, VM, VM] + [ANY] * 8,
        out_specs=[VM, VM] + [ANY] * 5,
        scratch_shapes=[
            pltpu.VMEM((3, 128, 1024), BF),
            pltpu.VMEM((NY, *lat.shape), BF),
            pltpu.VMEM((NZ, 8, 128), F32),
            pltpu.VMEM((NZ * NX, 8, 128), F32),
            pltpu.VMEM((8, 128), F32),
            dma((4,)), dma((32,)), dma((32,)), dma((32,)), dma((32,)),
            dma((4,)), dma((4,)), dma((5,)), dma((5,)),
        ],
        compiler_params=pltpu.CompilerParams(collective_id=0, has_side_effects=True),
        name="gather_inputs",
    )(lat, context, cond, cond_ctx, gain, w_shift, w_scale, w_gate, *weights)


def log_sigmoid(v):
    return jnp.minimum(v, 0.0) - jnp.log1p(jnp.exp(-jnp.abs(v)))


def log_decays(lowrank, decay_up, decay_bias):
    return [
        log_sigmoid(
            matmul(lowrank[:, way * RANK : (way + 1) * RANK], decay_up[way])
            + decay_bias[way : way + 1]
        )
        / TAU
        for way in range(2)
    ]


def triangle(n, lower):
    r = lax.broadcasted_iota(jnp.int32, (n, n), 0)
    c = lax.broadcasted_iota(jnp.int32, (n, n), 1)
    return r >= c if lower else r <= c


def running_sum(decay, lower):
    ones = jnp.where(triangle(decay.shape[0], lower), 1.0, 0.0).astype(BF)
    high = decay.astype(BF)
    rest = decay - high.astype(F32)
    middle = rest.astype(BF)
    low = (rest - middle.astype(F32)).astype(BF)
    return matmul(ones, high) + matmul(ones, middle) + matmul(ones, low)


def across(left, right):
    return lax.dot_general(left, right, (((1,), (1,)), ((), ())), preferred_element_type=F32)


def outer(left, right):
    return lax.dot_general(left, right, (((0,), (0,)), ((), ())), preferred_element_type=F32)


def scores_of(q, k, fwd, bwd, store):
    lower, upper = triangle(BLOCK, True), triangle(BLOCK, False)
    bf = lambda a: a.astype(BF)
    for b in range(2):
        sl = slice(b * BLOCK, (b + 1) * BLOCK)
        osl = slice((1 - b) * BLOCK, (2 - b) * BLOCK)
        f, g = fwd[sl], bwd[sl]
        cf, cg = f[BLOCK // 2 : BLOCK // 2 + 1], g[BLOCK // 2 - 1 : BLOCK // 2]
        sf = across(bf(q[sl] * jnp.exp(f - cf)), bf(k[sl] * jnp.exp(cf - f)))
        sb = across(bf(q[sl] * jnp.exp(g - cg)), bf(k[sl] * jnp.exp(cg - g)))
        store[sl, sl] = bf(jnp.where(lower, sf, 0.0) + jnp.where(upper, sb, 0.0))
        if b == 0:
            mine, other, edge = g, bwd[osl], bwd[BLOCK : BLOCK + 1]
        else:
            mine, other, edge = f, fwd[osl], fwd[BLOCK - 1 : BLOCK]
        store[sl, osl] = bf(across(bf(q[sl] * jnp.exp(mine - edge)), bf(k[osl] * jnp.exp(edge - other))))


def mixer_kernel(
    queries, keys_in, values, out_gate, lowrank, ctx_keys, ctx_values, ctx_lowrank,
    decay_up, decay_bias, head_gain, w_here, w_there, latents, mods, gain_post,
    result,
    w_out, pack, packs, states, got_states, decays, got_decays, scores, local, entering,
    group, groups, group_decays, all_decays, back, entry, before, leaving, entries, heads,
    part_a, part_b, near_a, near_b, far_a, far_b, sum_a, sum_b, relay_a, relay_b,
    s_load, s_x, r_x, s_z, r_z, s_e, r_e, s_y, r_y,
):
    z, x, y, c = position()
    x_peers = [(d, lax.rem(x + d, NX)) for d in (1, 3, 2)]
    z_peers = [(d, lax.rem(z + d, NZ)) for d in (4, 3, 5, 2, 6, 1, 7)]
    above, below, facing = (lax.rem(y + k, NY) for k in (1, 3, 2))
    up, down = dict(tp=above), dict(tp=below)
    entered = greet([dict(sp_1=p) for _, p in x_peers] + [dict(sp_0=p) for _, p in z_peers] + [up, down])
    loads = [
        pltpu.make_async_copy(src, w_out.at[k], s_load.at[k]) for k, src in enumerate((w_here, w_there))
    ]
    for load in loads:
        load.start()
    for j in range(NX):
        pack[j] = jnp.zeros((32, 512), BF)
        pack[j, :, :DK_HEAD] = ctx_keys[...]
        pack[j, :, DK_HEAD : DK_HEAD + 128] = ctx_values[:, j * 128 : (j + 1) * 128]
        pack[j, :, DK_HEAD + 128 : DK_HEAD + 128 + 2 * RANK] = ctx_lowrank[...]
    decay_f, decay_b = log_decays(lowrank[...], decay_up[...], decay_bias[...])
    fwd, bwd = running_sum(decay_f, True), running_sum(decay_b, False)
    decays[0:1] = fwd[-1:]
    decays[1:2] = bwd[:1]
    decays[2:8] = jnp.zeros((6, DK_HEAD), F32)
    k = keys_in[...].astype(F32)
    for way, scaled in enumerate((jnp.exp(fwd[-1:] - fwd), jnp.exp(bwd[:1] - bwd))):
        state = outer(values[...], (k * scaled).astype(BF)).astype(BF)
        for j in range(NX):
            states[j, way] = state[j * 128 : (j + 1) * 128]
    entered()
    x_copies = []
    for n, (a, b) in enumerate([(pack, packs), (states, got_states)]):
        for d, p in x_peers:
            x_copies.append(send(a.at[p], b.at[x], s_x.at[n, d], r_x.at[n, d], sp_1=p))
    for d, p in x_peers:
        x_copies.append(send(decays, got_decays.at[x], s_x.at[2, d], r_x.at[2, d], sp_1=p))
    packs[x] = pack[x]
    got_states[x] = states[x]
    got_decays[x] = decays[...]
    q = queries[...].astype(F32) * DK_HEAD ** (-0.5)
    scores_of(q, k, fwd, bwd, scores)
    local[...] = matmul(scores[...], values[...])
    entering[0] = (q * jnp.exp(fwd)).astype(BF)
    entering[1] = (q * jnp.exp(bwd)).astype(BF)
    for copy in x_copies[:3]:
        copy.wait()
    ctx = packs[...].reshape(NX * 32, 512)
    ctx_k = ctx[:, :DK_HEAD].astype(F32)
    ctx_v = ctx[:, DK_HEAD : DK_HEAD + 128]
    ctx_lr = ctx[:, DK_HEAD + 128 : DK_HEAD + 128 + 2 * RANK]
    cdf, cdb = log_decays(ctx_lr, decay_up[...], decay_bias[...])
    cf, cb = running_sum(cdf, True), running_sum(cdb, False)
    for way, scaled in enumerate((jnp.exp(cf[-1:] - cf), jnp.exp(cb[:1] - cb))):
        state = outer(ctx_v, (ctx_k * scaled).astype(BF)).astype(BF)
        for j in range(NZ):
            group[j, 2 + way] = state[j * 16 : (j + 1) * 16]
    group_decays[2:3] = cf[-1:]
    group_decays[3:4] = cb[:1]
    group_decays[4:8] = jnp.zeros((4, DK_HEAD), F32)
    for copy in x_copies[3:]:
        copy.wait()
    ways = (tuple(range(NX)), tuple(reversed(range(NX))))
    for way in range(2):
        state, total = None, None
        for j in ways[way]:
            step, piece = got_decays[j, way : way + 1], got_states[j, way].astype(F32)
            state = piece if state is None else state * jnp.exp(step) + piece
            total = step if total is None else total + step
        state = state.astype(BF)
        for j in range(NZ):
            group[j, way] = state[j * 16 : (j + 1) * 16]
        group_decays[way : way + 1] = total
    z_copies = []
    for d, p in z_peers:
        z_copies.append(send(group.at[p], groups.at[z], s_z.at[0, d], r_z.at[0, d], sp_0=p))
        z_copies.append(send(group_decays, all_decays.at[z], s_z.at[1, d], r_z.at[1, d], sp_0=p))
    groups[z] = group[z]
    all_decays[z] = group_decays[...]
    for way in range(2):
        state = jnp.zeros((128, DK_HEAD), F32)
        for j in ways[way]:
            before[j, way] = state
            state = state * jnp.exp(got_decays[j, way : way + 1]) + got_states[j, way].astype(F32)
    for copy in z_copies:
        copy.wait()
    orders = (tuple(range(NZ)), tuple(reversed(range(NZ))))
    for way in range(2):
        state = jnp.zeros((16, DK_HEAD), F32)
        for j in orders[way]:
            state = state * jnp.exp(all_decays[j, 2 + way : 3 + way]) + groups[j, 2 + way].astype(F32)
        for j in orders[way]:
            back[j, way] = state.astype(BF)
            state = state * jnp.exp(all_decays[j, way : way + 1]) + groups[j, way].astype(F32)
    z_copies = [send(back.at[p], entry.at[z], s_z.at[2, d], r_z.at[2, d], sp_0=p) for d, p in z_peers]
    entry[z] = back[z]
    for copy in z_copies:
        copy.wait()
    for way in range(2):
        start = jnp.concatenate([entry[j, way] for j in range(NZ)], axis=0).astype(F32)
        passed = jnp.zeros((1, DK_HEAD), F32)
        for j in ways[way]:
            leaving[j, way] = (start * jnp.exp(passed) + before[j, way]).astype(BF)
            passed = passed + got_decays[j, way : way + 1]
    e_copies = [send(leaving.at[p], entries.at[x], s_e.at[d], r_e.at[d], sp_1=p) for d, p in x_peers]
    entries[x] = leaving[x]
    gate = jax.nn.silu(out_gate[...].astype(F32)) * head_gain[...].astype(F32)
    for load in loads:
        load.wait()
    for copy in e_copies:
        copy.wait()
    out = [
        local[:, j * 128 : (j + 1) * 128]
        + across(entering[0], entries[j, 0])
        + across(entering[1], entries[j, 1])
        for j in range(NX)
    ]
    square = sum(jnp.sum(o * o, axis=1, keepdims=True) for o in out)
    scale = lax.rsqrt(square / DV_HEAD + EPS)
    for j in range(NX):
        heads[:, j * 128 : (j + 1) * 128] = (out[j] * scale * gate[:, j * 128 : (j + 1) * 128]).astype(BF)
    count = latents.shape[0]

    def project(owner):
        rows = heads[pl.ds(pl.multiple_of(owner * count, count), count)]
        part_a[owner] = matmul(rows, w_out[0]).astype(BF)
        part_b[owner] = matmul(rows, w_out[1]).astype(BF)

    project(facing)
    first_a = send(part_a.at[facing], relay_a, s_y.at[0], r_y.at[0], **down)
    first_b = send(part_b.at[facing], relay_b, s_y.at[1], r_y.at[1], **up)
    project(below)
    direct_b = send(part_b.at[below], near_b, s_y.at[2], r_y.at[2], **down)
    project(above)
    direct_a = send(part_a.at[above], near_a, s_y.at[3], r_y.at[3], **up)
    first_a.wait()
    sum_a[...] = (relay_a[...].astype(F32) + part_a[below].astype(F32)).astype(BF)
    second_a = send(sum_a, far_a, s_y.at[4], r_y.at[4], **down)
    first_b.wait()
    sum_b[...] = (relay_b[...].astype(F32) + part_b[above].astype(F32)).astype(BF)
    second_b = send(sum_b, far_b, s_y.at[5], r_y.at[5], **up)
    project(y)
    direct_a.wait()
    direct_b.wait()
    second_a.wait()
    second_b.wait()
    here, there = (
        pl.ds(pl.multiple_of(k * HALF, HALF), HALF) for k in (c, 1 - c)
    )

    def finish(k, carry):
        rows = pl.ds(pl.multiple_of(k * 16, 16), 16)
        a = part_a[y, rows].astype(F32) + near_a[rows].astype(F32) + far_a[rows].astype(F32)
        b = part_b[y, rows].astype(F32) + near_b[rows].astype(F32) + far_b[rows].astype(F32)
        square = jnp.sum(a * a, axis=1, keepdims=True) + jnp.sum(b * b, axis=1, keepdims=True)
        scale = lax.rsqrt(square / WIDTH + EPS)
        for columns, half in ((here, a), (there, b)):
            weight = mods[2:3, columns] * gain_post[:, columns].astype(F32)
            result[rows, columns] = (
                latents[rows, columns].astype(F32) + half * scale * weight
            ).astype(BF)
        return carry

    lax.fori_loop(0, count // 16, finish, 0)


def mixer(*args):
    dma = pltpu.SemaphoreType.DMA
    vm = pltpu.VMEM
    half = vm((64, HALF), BF)
    in_specs = [VM] * len(args)
    in_specs[11] = in_specs[12] = ANY
    return pl.pallas_call(
        mixer_kernel,
        out_shape=shape_of(64, WIDTH),
        in_specs=in_specs,
        out_specs=VM,
        scratch_shapes=[
            vm((2, DV_HEAD, HALF), BF),
            vm((NX, 32, 512), BF), vm((NX, 32, 512), BF),
            vm((NX, 2, 128, DK_HEAD), BF), vm((NX, 2, 128, DK_HEAD), BF),
            vm((8, DK_HEAD), F32), vm((NX, 8, DK_HEAD), F32),
            vm((256, 256), BF), vm((256, DV_HEAD), F32), vm((2, 256, DK_HEAD), BF),
            vm((NZ, 4, 16, DK_HEAD), BF), vm((NZ, 4, 16, DK_HEAD), BF),
            vm((8, DK_HEAD), F32), vm((NZ, 8, DK_HEAD), F32),
            vm((NZ, 2, 16, DK_HEAD), BF), vm((NZ, 2, 16, DK_HEAD), BF),
            vm((NX, 2, 128, DK_HEAD), F32),
            vm((NX, 2, 128, DK_HEAD), BF), vm((NX, 2, 128, DK_HEAD), BF),
            vm((256, DV_HEAD), BF),
            vm((NY, 64, HALF), BF), vm((NY, 64, HALF), BF),
            half, half, half, half, half, half, half, half,
            dma((2,)), dma((3, NX)), dma((3, NX)), dma((3, NZ)), dma((3, NZ)),
            dma((NX,)), dma((NX,)), dma((6,)), dma((6,)),
        ],
        compiler_params=pltpu.CompilerParams(
            collective_id=1, has_side_effects=True, vmem_limit_bytes=56 * 2**20
        ),
        name="mixer",
    )(*args)


def body(
    latents, cond, cond_ctx, context, w_shift, w_scale, w_gate, gain_pre, gain_post,
    w_query, w_key, w_value, w_outgate, w_down, decay_up, decay_bias, head_gain, w_out,
):
    latents, context = latents[0], context[0]
    mods, rows, wq2, wk2, wv2, wg2, wo2 = gather_inputs(
        latents, context, cond, cond_ctx[None], gain_pre[None], w_shift, w_scale, w_gate,
        w_query, w_key, w_value, w_outgate, w_out,
    )
    count = NY * latents.shape[0]

    def project(here, there, rows=rows):
        return (matmul(rows[0], here) + matmul(rows[1], there)).astype(BF)

    c = lax.axis_index("dp")
    keys_in = project(w_key, wk2)
    values = project(w_value, wv2)
    down = [lax.dynamic_slice_in_dim(w_down, k * HALF, HALF, 0) for k in (c, 1 - c)]
    lowrank = project(*down)
    main = rows[:, :count]
    queries = project(w_query, wq2, main)
    out_gate = project(w_outgate, wg2, main)
    result = mixer(
        queries, keys_in[:count], values[:count], out_gate, lowrank[:count],
        keys_in[count:], values[count:], lowrank[count:],
        decay_up, decay_bias, head_gain[None], w_out, wo2, latents, mods, gain_post[None],
    )
    return result[None]


def solution(mesh):
    finer = Mesh(
        mesh.devices.reshape(8, 4, mesh.shape["tp"], mesh.shape["dp"]), ("sp_0", "sp_1", "tp", "dp")
    )
    in_specs = (
        P("dp", SP_TP, None),
        P("dp", SP),
        P(SP),
        P("dp", SP, None),
        P(SP, "tp"),
        P(SP, "tp"),
        P(SP, "tp"),
        P(),
        P(),
        P("dp", "tp"),
        P("dp", "tp"),
        P("dp", "tp"),
        P("dp", "tp"),
        P(),
        P(None, None, "tp"),
        P(None, "tp"),
        P("tp"),
        P("tp", "dp"),
    )
    out_specs = P("dp", SP_TP, None)
    return jax.shard_map(body, mesh=finer, in_specs=in_specs, out_specs=out_specs, check_vma=False)
```

```python
import jax
import jax.numpy as jnp
from jax import lax
from jax.experimental import pallas as pl
from jax.experimental.pallas import tpu as pltpu
from jax.sharding import Mesh
from jax.sharding import PartitionSpec as P

DK_HEAD = 256
DV_HEAD = 512
RANK = 16
BLOCK = 128
SP_TP = ("sp_0", "sp_1", "tp")
SP = ("sp_0", "sp_1")
NZ, NX, NY = 8, 4, 4
WIDTH = 4096
HALF = 2048
ANY = pl.BlockSpec(memory_space=pl.ANY)
VM = pl.BlockSpec(memory_space=pltpu.VMEM)
BF, F32 = jnp.bfloat16, jnp.float32


EPS = 1e-06
TAU = 16.0


def matmul(left, right):
    return jnp.dot(left, right, preferred_element_type=jnp.float32)


def rms_scale(vectors, gain):
    return vectors * lax.rsqrt(jnp.mean(vectors * vectors, axis=-1, keepdims=True) + EPS) * gain


def shape_of(*dims, dtype=BF):
    return jax.ShapeDtypeStruct(dims, dtype)


def send(src, dst, send_sem, recv_sem, **where):
    copy = pltpu.make_async_remote_copy(
        src_ref=src,
        dst_ref=dst,
        send_sem=send_sem,
        recv_sem=recv_sem,
        device_id=where,
        device_id_type=pl.DeviceIdType.MESH,
    )
    copy.start()
    return copy


def greet(partners):
    barrier = pltpu.get_barrier_semaphore()
    for where in partners:
        pl.semaphore_signal(
            barrier, inc=1, device_id=where, device_id_type=pl.DeviceIdType.MESH
        )
    return lambda: pl.semaphore_wait(barrier, len(partners))


def position():
    return tuple(lax.axis_index(a) for a in ("sp_0", "sp_1", "tp", "dp"))


def log_sigmoid(v):
    return jnp.minimum(v, 0.0) - jnp.log1p(jnp.exp(-jnp.abs(v)))


def log_decays(lowrank, decay_up, decay_bias):
    return [
        log_sigmoid(
            matmul(lowrank[:, way * RANK : (way + 1) * RANK], decay_up[way])
            + decay_bias[way : way + 1]
        )
        / TAU
        for way in range(2)
    ]


def triangle(n, lower):
    r = lax.broadcasted_iota(jnp.int32, (n, n), 0)
    c = lax.broadcasted_iota(jnp.int32, (n, n), 1)
    return r >= c if lower else r <= c


def running_sum(decay, lower):
    ones = jnp.where(triangle(decay.shape[0], lower), 1.0, 0.0).astype(BF)
    high = decay.astype(BF)
    rest = decay - high.astype(F32)
    middle = rest.astype(BF)
    low = (rest - middle.astype(F32)).astype(BF)
    return matmul(ones, high) + matmul(ones, middle) + matmul(ones, low)


def across(left, right):
    return lax.dot_general(left, right, (((1,), (1,)), ((), ())), preferred_element_type=F32)


def outer(left, right):
    return lax.dot_general(left, right, (((0,), (0,)), ((), ())), preferred_element_type=F32)


def scores_of(q, k, fwd, bwd, store):
    lower, upper = triangle(BLOCK, True), triangle(BLOCK, False)
    bf = lambda a: a.astype(BF)
    for b in range(2):
        sl = slice(b * BLOCK, (b + 1) * BLOCK)
        osl = slice((1 - b) * BLOCK, (2 - b) * BLOCK)
        f, g = fwd[sl], bwd[sl]
        cf, cg = f[BLOCK // 2 : BLOCK // 2 + 1], g[BLOCK // 2 - 1 : BLOCK // 2]
        sf = across(bf(q[sl] * jnp.exp(f - cf)), bf(k[sl] * jnp.exp(cf - f)))
        sb = across(bf(q[sl] * jnp.exp(g - cg)), bf(k[sl] * jnp.exp(cg - g)))
        store[sl, sl] = bf(jnp.where(lower, sf, 0.0) + jnp.where(upper, sb, 0.0))
        if b == 0:
            mine, other, edge = g, bwd[osl], bwd[BLOCK : BLOCK + 1]
        else:
            mine, other, edge = f, fwd[osl], fwd[BLOCK - 1 : BLOCK]
        store[sl, osl] = bf(across(bf(q[sl] * jnp.exp(mine - edge)), bf(k[osl] * jnp.exp(edge - other))))


def mixer_kernel(
    lat, context, cond, cond_ctx, gain_pre, gain_post, head_gain, w_shift, w_scale, w_gate,
    wq, wk, wv, wg, wo, w_down, decay_up, decay_bias,
    result,
    w_mod, partial, arrived, tile, tiles, column_sum, mods, vectors, lat_all, rows, w_all, proj, low, w_out,
    pack, packs, states, got_states, relay_f, relay_b, relay_g, relay_h, decays, got_decays, scores, local, entering,
    group, groups, ctx_group, ctx_groups, group_decays, all_decays, ctx_decays, all_ctx_decays,
    back, entry, before, leaving, entries, heads,
    part_a, part_b, near_a, near_b, far_a, far_b, sum_a, sum_b, relay_a, relay_c,
    s_load, s_m1, r_m1, s_m2, r_m2, s_m3, r_m3, s_l, r_l, s_w, r_w,
    s_x, r_x, s_z, r_z, s_e, r_e, s_y, r_y,
):
    z, x, y, c = position()
    x_peers = [(d, lax.rem(x + d, NX)) for d in (1, 3, 2)]
    z_peers = [(d, lax.rem(z + d, NZ)) for d in (4, 3, 5, 2, 6, 1, 7)]
    xy_peers = [
        (k, dict(sp_1=lax.rem(x + k // NY, NX), tp=lax.rem(y + k % NY, NY)))
        for k in range(1, NX * NY)
    ]
    above, below, facing = (lax.rem(y + k, NY) for k in (1, 3, 2))
    up, down = dict(tp=above), dict(tp=below)
    east, west = lax.rem(x + 1, NX), lax.rem(x + 3, NX)
    opposite = lax.rem(x + 2, NX)
    other = dict(dp=1 - c)
    columns = [pl.ds(pl.multiple_of(k * HALF, HALF), HALF) for k in (c, 1 - c)]
    entered = greet([dict(sp_0=p) for _, p in z_peers] + [w for _, w in xy_peers] + [other])
    spans = (slice(0, 256), slice(256, 512), slice(512, 1024), slice(1024, 1536))
    sources = list(zip((wq, wk, wv, wg), spans))
    loads = [(w_shift, w_mod.at[0]), (w_scale, w_mod.at[1]), (w_gate, w_mod.at[2]), (lat, lat_all.at[y])]
    loads += [(w, w_all.at[0, :, span]) for w, span in sources] + [(wo, w_out.at[0])]
    loads = [pltpu.make_async_copy(src, dst, s_load.at[k]) for k, (src, dst) in enumerate(loads)]
    for load in loads:
        load.start()
    line = lax.broadcasted_iota(jnp.int32, (16, 128), 0)
    act = jax.nn.silu(cond[...].astype(F32)).astype(BF).astype(F32)
    act_ctx = jax.nn.silu(cond_ctx[...].astype(F32)).astype(BF).astype(F32)
    total = None
    for k in range(3):
        left = jnp.where(line == k, act, jnp.where(line == k + 3, act_ctx, 0.0)).astype(BF)
        loads[k].wait()
        part = matmul(left, w_mod[k])
        total = part if total is None else total + part
    for k in range(NZ):
        partial[k] = total[:8, k * 128 : (k + 1) * 128]
    loads[3].wait()
    entered()
    m_copies = [
        send(partial.at[p], arrived.at[d], s_m1.at[d], r_m1.at[d], sp_0=p) for d, p in z_peers
    ]
    top, bottom = pl.ds(0, 32), pl.ds(32, 32)
    up_1 = send(lat_all.at[y, top], lat_all.at[y, top], s_l.at[0], r_l.at[0], **up)
    down_1 = send(lat_all.at[y, bottom], lat_all.at[y, bottom], s_l.at[1], r_l.at[1], **down)
    weights = [
        send(w, w_all.at[1, :, span], s_w.at[k], r_w.at[k], **other)
        for k, (w, span) in enumerate(sources)
    ]
    weights.append(send(wo, w_out.at[1], s_w.at[4], r_w.at[4], **other))
    for copy in m_copies:
        copy.wait()
    summed = partial[z]
    for d in range(1, NZ):
        summed = summed + arrived[d]
    tile[...] = summed
    m_copies = [
        send(tile, tiles.at[y, x], s_m2.at[k], r_m2.at[k], **w) for k, w in xy_peers
    ]
    tiles[y, x] = summed
    up_2 = send(lat_all.at[y, bottom], lat_all.at[y, bottom], s_l.at[2], r_l.at[2], **up)
    down_2 = send(lat_all.at[y, top], lat_all.at[y, top], s_l.at[3], r_l.at[3], **down)
    for copy in m_copies:
        copy.wait()
    for k in range(NY):
        block = tiles[k, 0] + tiles[k, 1] + tiles[k, 2] + tiles[k, 3]
        column_sum[k] = block
        mods[z, k] = block
    m_copies = [
        send(column_sum, mods.at[z], s_m3.at[d], r_m3.at[d], sp_0=p) for d, p in z_peers
    ]
    up_1.wait()
    passed = lat_all.at[below, top]
    relay_up = send(passed, passed, s_l.at[4], r_l.at[4], **up)
    down_1.wait()
    passed = lat_all.at[above, bottom]
    relay_down = send(passed, passed, s_l.at[5], r_l.at[5], **down)
    for copy in m_copies:
        copy.wait()
    for k in range(NY):
        for j in range(NZ):
            at = (k * NZ + j) * 128
            vectors[:, at : at + 128] = mods[j, k]

    def modulate(source, target, scale_row, shift_row, length):
        def step(k, carry):
            at = pl.ds(pl.multiple_of(k * 16, 16), 16)
            to = pl.ds(pl.multiple_of(target + k * 16, 16), 16)
            halves = [source[at, columns[h]].astype(F32) for h in range(2)]
            square = sum(jnp.sum(v * v, axis=1, keepdims=True) for v in halves)
            norm = lax.rsqrt(square / WIDTH + EPS)
            for h in range(2):
                weight = gain_pre[:, columns[h]].astype(F32) * (
                    1.0 + vectors[scale_row : scale_row + 1, columns[h]]
                )
                shift = vectors[shift_row : shift_row + 1, columns[h]]
                rows[h, to] = (halves[h] * norm * weight + shift).astype(BF)
            return carry

        lax.fori_loop(0, length // 16, step, 0)

    def project_rows(at, length, places):
        def step(k, carry):
            span = pl.ds(pl.multiple_of(k * 256, 256), 256)
            out = matmul(rows[0, at : at + length], w_all[0, :, span])
            out = (out + matmul(rows[1, at : at + length], w_all[1, :, span])).astype(BF)
            for offset, place, count in places:
                to = pl.ds(pl.multiple_of(place, 32), count)
                proj[to, span] = out[offset : offset + count]
            return carry

        lax.fori_loop(0, 6, step, 0)
        out = across(rows[0, at : at + length], w_down[:, columns[0]])
        out = (out + across(rows[1, at : at + length], w_down[:, columns[1]])).astype(BF)
        for offset, place, count in places:
            low[pl.ds(pl.multiple_of(place, 32), count)] = out[offset : offset + count]

    modulate(context, 0, 4, 3, 32)
    modulate(lat_all.at[y], 32, 1, 0, 64)
    up_2.wait()
    modulate(lat_all.at[below], 96, 1, 0, 64)
    down_2.wait()
    modulate(lat_all.at[above], 160, 1, 0, 64)
    for load in loads[4:8]:
        load.wait()
    for copy in weights[:4]:
        copy.wait()
    project_rows(0, 224, ((0, 256, 32), (32, y * 64, 64), (96, below * 64, 64), (160, above * 64, 64)))
    for j in range(NX):
        pack[j] = jnp.zeros((32, 512), BF)
        pack[j, :, :DK_HEAD] = proj[256:288, 256:512]
        pack[j, :, DK_HEAD : DK_HEAD + 128] = proj[256:288, 512 + j * 128 : 640 + j * 128]
        pack[j, :, DK_HEAD + 128 : DK_HEAD + 128 + 2 * RANK] = low[256:288]
    c_copies = [send(pack.at[p], packs.at[x], s_x.at[0, d], r_x.at[0, d], sp_1=p) for d, p in x_peers]
    packs[x] = pack[x]
    relay_up.wait()
    relay_down.wait()
    modulate(lat_all.at[facing], 224, 1, 0, 64)
    project_rows(224, 64, ((0, facing * 64, 64),))
    decay_f, decay_b = log_decays(low[:256], decay_up[...], decay_bias[...])
    fwd, bwd = running_sum(decay_f, True), running_sum(decay_b, False)
    decays[0:1] = fwd[-1:]
    decays[1:2] = bwd[:1]
    decays[2:8] = jnp.zeros((6, DK_HEAD), F32)
    x_copies = [
        send(decays, got_decays.at[x], s_x.at[1, d], r_x.at[1, d], sp_1=p) for d, p in x_peers
    ]
    got_decays[x] = decays[...]
    k = proj[:256, 256:512].astype(F32)
    v = proj[:256, 512:1024]

    def local_state(way, scaled):
        state = outer(v, (k * scaled).astype(BF)).astype(BF)
        for j in range(NX):
            states[j, way] = state[j * 128 : (j + 1) * 128]

    def to_neighbour(p, d, way):
        return send(states.at[p, way], got_states.at[x, way], s_x.at[2 + way, d], r_x.at[2 + way, d], sp_1=p)

    local_state(0, jnp.exp(fwd[-1:] - fwd))
    pass_f = send(states.at[opposite, 0], relay_f, s_x.at[2, 2], r_x.at[2, 2], sp_1=east)
    x_copies += [to_neighbour(west, 3, 0), to_neighbour(east, 1, 0)]
    local_state(1, jnp.exp(bwd[:1] - bwd))
    pass_b = send(states.at[opposite, 1], relay_b, s_x.at[3, 2], r_x.at[3, 2], sp_1=west)
    x_copies += [to_neighbour(east, 1, 1), to_neighbour(west, 3, 1)]
    got_states[x] = states[x]
    q = proj[:256, :256].astype(F32) * DK_HEAD ** (-0.5)
    scores_of(q, k, fwd, bwd, scores)
    pass_f.wait()
    x_copies.append(send(relay_f, got_states.at[west, 0], s_x.at[4, 1], r_x.at[4, 1], sp_1=east))
    pass_b.wait()
    x_copies.append(send(relay_b, got_states.at[east, 1], s_x.at[4, 3], r_x.at[4, 3], sp_1=west))
    for copy in c_copies:
        copy.wait()
    ctx = packs[...].reshape(NX * 32, 512)
    ctx_k = ctx[:, :DK_HEAD].astype(F32)
    ctx_v = ctx[:, DK_HEAD : DK_HEAD + 128]
    ctx_lr = ctx[:, DK_HEAD + 128 : DK_HEAD + 128 + 2 * RANK]
    cdf, cdb = log_decays(ctx_lr, decay_up[...], decay_bias[...])
    cf, cb = running_sum(cdf, True), running_sum(cdb, False)
    for way, scaled in enumerate((jnp.exp(cf[-1:] - cf), jnp.exp(cb[:1] - cb))):
        state = outer(ctx_v, (ctx_k * scaled).astype(BF)).astype(BF)
        for j in range(NZ):
            ctx_group[j, way] = state[j * 16 : (j + 1) * 16]
    ctx_decays[0:1] = cf[-1:]
    ctx_decays[1:2] = cb[:1]
    ctx_decays[2:8] = jnp.zeros((6, DK_HEAD), F32)
    c_copies = []
    for d, p in z_peers:
        c_copies.append(send(ctx_group.at[p], ctx_groups.at[z], s_z.at[0, d], r_z.at[0, d], sp_0=p))
        c_copies.append(send(ctx_decays, all_ctx_decays.at[z], s_z.at[1, d], r_z.at[1, d], sp_0=p))
    ctx_groups[z] = ctx_group[z]
    all_ctx_decays[z] = ctx_decays[...]
    local[...] = matmul(scores[...], v)
    entering[0] = (q * jnp.exp(fwd)).astype(BF)
    entering[1] = (q * jnp.exp(bwd)).astype(BF)
    for copy in x_copies:
        copy.wait()
    ways = (tuple(range(NX)), tuple(reversed(range(NX))))
    for way in range(2):
        state, total = None, None
        for j in ways[way]:
            step, piece = got_decays[j, way : way + 1], got_states[j, way].astype(F32)
            state = piece if state is None else state * jnp.exp(step) + piece
            total = step if total is None else total + step
        state = state.astype(BF)
        for j in range(NZ):
            group[j, way] = state[j * 16 : (j + 1) * 16]
        group_decays[way : way + 1] = total
    group_decays[2:8] = jnp.zeros((6, DK_HEAD), F32)
    z_copies = []
    for d, p in z_peers:
        z_copies.append(send(group.at[p], groups.at[z], s_z.at[2, d], r_z.at[2, d], sp_0=p))
        z_copies.append(send(group_decays, all_decays.at[z], s_z.at[3, d], r_z.at[3, d], sp_0=p))
    groups[z] = group[z]
    all_decays[z] = group_decays[...]
    for way in range(2):
        state = jnp.zeros((128, DK_HEAD), F32)
        for j in ways[way]:
            before[j, way] = state
            state = state * jnp.exp(got_decays[j, way : way + 1]) + got_states[j, way].astype(F32)
    orders = (tuple(range(NZ)), tuple(reversed(range(NZ))))
    for copy in c_copies:
        copy.wait()
    starts = []
    for way in range(2):
        state = jnp.zeros((16, DK_HEAD), F32)
        for j in orders[way]:
            state = state * jnp.exp(all_ctx_decays[j, way : way + 1]) + ctx_groups[j, way].astype(F32)
        starts.append(state)
    for copy in z_copies:
        copy.wait()
    for way in range(2):
        state = starts[way]
        for j in orders[way]:
            back[j, way] = state.astype(BF)
            state = state * jnp.exp(all_decays[j, way : way + 1]) + groups[j, way].astype(F32)
    z_copies = [send(back.at[p], entry.at[z], s_z.at[4, d], r_z.at[4, d], sp_0=p) for d, p in z_peers]
    entry[z] = back[z]
    gate = jax.nn.silu(proj[:256, 1024:1536].astype(F32)) * head_gain[...].astype(F32)
    for copy in z_copies:
        copy.wait()
    for way in range(2):
        start = jnp.concatenate([entry[j, way] for j in range(NZ)], axis=0).astype(F32)
        passed = jnp.zeros((1, DK_HEAD), F32)
        for j in ways[way]:
            leaving[j, way] = (start * jnp.exp(passed) + before[j, way]).astype(BF)
            passed = passed + got_decays[j, way : way + 1]

    def return_to(p, d, way):
        return send(leaving.at[p, way], entries.at[x, way], s_e.at[way, d], r_e.at[way, d], sp_1=p)

    pass_f = send(leaving.at[opposite, 0], relay_g, s_e.at[0, 2], r_e.at[0, 2], sp_1=east)
    pass_b = send(leaving.at[opposite, 1], relay_h, s_e.at[1, 2], r_e.at[1, 2], sp_1=west)
    e_copies = [return_to(p, d, way) for way in range(2) for p, d in ((east, 1), (west, 3))]
    entries[x] = leaving[x]
    pass_f.wait()
    e_copies.append(send(relay_g, entries.at[west, 0], s_e.at[2, 1], r_e.at[2, 1], sp_1=east))
    pass_b.wait()
    e_copies.append(send(relay_h, entries.at[east, 1], s_e.at[2, 3], r_e.at[2, 3], sp_1=west))
    loads[8].wait()
    weights[4].wait()
    for copy in e_copies:
        copy.wait()
    out = [
        local[:, j * 128 : (j + 1) * 128]
        + across(entering[0], entries[j, 0])
        + across(entering[1], entries[j, 1])
        for j in range(NX)
    ]
    square = sum(jnp.sum(o * o, axis=1, keepdims=True) for o in out)
    scale = lax.rsqrt(square / DV_HEAD + EPS)
    for j in range(NX):
        heads[:, j * 128 : (j + 1) * 128] = (out[j] * scale * gate[:, j * 128 : (j + 1) * 128]).astype(BF)
    count = 64

    def project(owner):
        at = heads[pl.ds(pl.multiple_of(owner * count, count), count)]
        part_a[owner] = matmul(at, w_out[0]).astype(BF)
        part_b[owner] = matmul(at, w_out[1]).astype(BF)

    project(facing)
    first_a = send(part_a.at[facing], relay_a, s_y.at[0], r_y.at[0], **down)
    first_b = send(part_b.at[facing], relay_c, s_y.at[1], r_y.at[1], **up)
    project(below)
    direct_b = send(part_b.at[below], near_b, s_y.at[2], r_y.at[2], **down)
    project(above)
    direct_a = send(part_a.at[above], near_a, s_y.at[3], r_y.at[3], **up)
    first_a.wait()
    sum_a[...] = (relay_a[...].astype(F32) + part_a[below].astype(F32)).astype(BF)
    second_a = send(sum_a, far_a, s_y.at[4], r_y.at[4], **down)
    first_b.wait()
    sum_b[...] = (relay_c[...].astype(F32) + part_b[above].astype(F32)).astype(BF)
    second_b = send(sum_b, far_b, s_y.at[5], r_y.at[5], **up)
    project(y)
    direct_a.wait()
    direct_b.wait()
    second_a.wait()
    second_b.wait()

    def finish(k, carry):
        at = pl.ds(pl.multiple_of(k * 16, 16), 16)
        a = part_a[y, at].astype(F32) + near_a[at].astype(F32) + far_a[at].astype(F32)
        b = part_b[y, at].astype(F32) + near_b[at].astype(F32) + far_b[at].astype(F32)
        square = jnp.sum(a * a, axis=1, keepdims=True) + jnp.sum(b * b, axis=1, keepdims=True)
        scale = lax.rsqrt(square / WIDTH + EPS)
        for span, half in zip(columns, (a, b)):
            weight = vectors[2:3, span] * gain_post[:, span].astype(F32)
            result[at, span] = (
                lat_all[y, at, span].astype(F32) + half * scale * weight
            ).astype(BF)
        return carry

    lax.fori_loop(0, count // 16, finish, 0)


def mixer(*args):
    dma = pltpu.SemaphoreType.DMA
    vm = pltpu.VMEM
    half = vm((64, HALF), BF)
    in_specs = [VM] * len(args)
    for k in (0, 7, 8, 9, 10, 11, 12, 13, 14):
        in_specs[k] = ANY
    piece = vm((128, DK_HEAD), BF)
    return pl.pallas_call(
        mixer_kernel,
        out_shape=shape_of(64, WIDTH),
        in_specs=in_specs,
        out_specs=VM,
        scratch_shapes=[
            vm((3, 128, 1024), BF), vm((NZ, 8, 128), F32), vm((NZ, 8, 128), F32),
            vm((8, 128), F32), vm((NY, NX, 8, 128), F32), vm((NY, 8, 128), F32),
            vm((NZ, NY, 8, 128), F32), vm((8, WIDTH), F32),
            vm((NY, 64, WIDTH), BF), vm((2, 288, HALF), BF), vm((2, HALF, 1536), BF),
            vm((288, 1536), BF), vm((288, 2 * RANK), BF), vm((2, DV_HEAD, HALF), BF),
            vm((NX, 32, 512), BF), vm((NX, 32, 512), BF),
            vm((NX, 2, 128, DK_HEAD), BF), vm((NX, 2, 128, DK_HEAD), BF), piece, piece, piece, piece,
            vm((8, DK_HEAD), F32), vm((NX, 8, DK_HEAD), F32),
            vm((256, 256), BF), vm((256, DV_HEAD), F32), vm((2, 256, DK_HEAD), BF),
            vm((NZ, 2, 16, DK_HEAD), BF), vm((NZ, 2, 16, DK_HEAD), BF),
            vm((NZ, 2, 16, DK_HEAD), BF), vm((NZ, 2, 16, DK_HEAD), BF),
            vm((8, DK_HEAD), F32), vm((NZ, 8, DK_HEAD), F32),
            vm((8, DK_HEAD), F32), vm((NZ, 8, DK_HEAD), F32),
            vm((NZ, 2, 16, DK_HEAD), BF), vm((NZ, 2, 16, DK_HEAD), BF),
            vm((NX, 2, 128, DK_HEAD), F32),
            vm((NX, 2, 128, DK_HEAD), BF), vm((NX, 2, 128, DK_HEAD), BF),
            vm((256, DV_HEAD), BF),
            vm((NY, 64, HALF), BF), vm((NY, 64, HALF), BF),
            half, half, half, half, half, half, half, half,
            dma((9,)), dma((NZ,)), dma((NZ,)), dma((16,)), dma((16,)), dma((NZ,)), dma((NZ,)),
            dma((6,)), dma((6,)), dma((5,)), dma((5,)),
            dma((5, NX)), dma((5, NX)), dma((5, NZ)), dma((5, NZ)),
            dma((3, NX)), dma((3, NX)), dma((6,)), dma((6,)),
        ],
        compiler_params=pltpu.CompilerParams(
            collective_id=0, has_side_effects=True, vmem_limit_bytes=60 * 2**20
        ),
        name="mixer",
    )(*args)


def body(
    latents, cond, cond_ctx, context, w_shift, w_scale, w_gate, gain_pre, gain_post,
    w_query, w_key, w_value, w_outgate, w_down, decay_up, decay_bias, head_gain, w_out,
):
    result = mixer(
        latents[0], context[0], cond, cond_ctx[None], gain_pre[None], gain_post[None], head_gain[None],
        w_shift, w_scale, w_gate, w_query, w_key, w_value, w_outgate, w_out,
        w_down.T, decay_up, decay_bias,
    )
    return result[None]


def solution(mesh):
    finer = Mesh(
        mesh.devices.reshape(8, 4, mesh.shape["tp"], mesh.shape["dp"]), ("sp_0", "sp_1", "tp", "dp")
    )
    in_specs = (
        P("dp", SP_TP, None),
        P("dp", SP),
        P(SP),
        P("dp", SP, None),
        P(SP, "tp"),
        P(SP, "tp"),
        P(SP, "tp"),
        P(),
        P(),
        P("dp", "tp"),
        P("dp", "tp"),
        P("dp", "tp"),
        P("dp", "tp"),
        P(),
        P(None, None, "tp"),
        P(None, "tp"),
        P("tp"),
        P("tp", "dp"),
    )
    out_specs = P("dp", SP_TP, None)
    return jax.shard_map(body, mesh=finer, in_specs=in_specs, out_specs=out_specs, check_vma=False)
```

```python
import jax
import jax.numpy as jnp
from jax import lax
from jax.experimental import pallas as pl
from jax.experimental.pallas import tpu as pltpu
from jax.sharding import Mesh
from jax.sharding import PartitionSpec as P

DK_HEAD = 256
DV_HEAD = 512
RANK = 16
BLOCK = 128
SP_TP = ("sp_0", "sp_1", "tp")
SP = ("sp_0", "sp_1")
NZ, NX, NY = 8, 4, 4
WIDTH = 4096
HALF = 2048
ANY = pl.BlockSpec(memory_space=pl.ANY)
VM = pl.BlockSpec(memory_space=pltpu.VMEM)
BF, F32 = jnp.bfloat16, jnp.float32


EPS = 1e-06
TAU = 16.0


def matmul(left, right):
    return jnp.dot(left, right, preferred_element_type=jnp.float32)


def rms_scale(vectors, gain):
    return vectors * lax.rsqrt(jnp.mean(vectors * vectors, axis=-1, keepdims=True) + EPS) * gain


def shape_of(*dims, dtype=BF):
    return jax.ShapeDtypeStruct(dims, dtype)


def send(src, dst, send_sem, recv_sem, **where):
    copy = pltpu.make_async_remote_copy(
        src_ref=src,
        dst_ref=dst,
        send_sem=send_sem,
        recv_sem=recv_sem,
        device_id=where,
        device_id_type=pl.DeviceIdType.MESH,
    )
    copy.start()
    return copy


def greet(partners):
    barrier = pltpu.get_barrier_semaphore()
    for where in partners:
        pl.semaphore_signal(
            barrier, inc=1, device_id=where, device_id_type=pl.DeviceIdType.MESH
        )
    return lambda: pl.semaphore_wait(barrier, len(partners))


def position():
    return tuple(lax.axis_index(a) for a in ("sp_0", "sp_1", "tp", "dp"))


def log_sigmoid(v):
    return jnp.minimum(v, 0.0) - jnp.log1p(jnp.exp(-jnp.abs(v)))


def log_decays(lowrank, decay_up, decay_bias):
    return [
        log_sigmoid(
            matmul(lowrank[:, way * RANK : (way + 1) * RANK], decay_up[way])
            + decay_bias[way : way + 1]
        )
        / TAU
        for way in range(2)
    ]


def triangle(n, lower):
    r = lax.broadcasted_iota(jnp.int32, (n, n), 0)
    c = lax.broadcasted_iota(jnp.int32, (n, n), 1)
    return r >= c if lower else r <= c


def running_sum(decay, lower):
    ones = jnp.where(triangle(decay.shape[0], lower), 1.0, 0.0).astype(BF)
    high = decay.astype(BF)
    rest = decay - high.astype(F32)
    middle = rest.astype(BF)
    low = (rest - middle.astype(F32)).astype(BF)
    return matmul(ones, high) + matmul(ones, middle) + matmul(ones, low)


def across(left, right):
    return lax.dot_general(left, right, (((1,), (1,)), ((), ())), preferred_element_type=F32)


def outer(left, right):
    return lax.dot_general(left, right, (((0,), (0,)), ((), ())), preferred_element_type=F32)


def scores_of(q, k, fwd, bwd, store):
    lower, upper = triangle(BLOCK, True), triangle(BLOCK, False)
    bf = lambda a: a.astype(BF)
    for b in range(2):
        sl = slice(b * BLOCK, (b + 1) * BLOCK)
        osl = slice((1 - b) * BLOCK, (2 - b) * BLOCK)
        f, g = fwd[sl], bwd[sl]
        cf, cg = f[BLOCK // 2 : BLOCK // 2 + 1], g[BLOCK // 2 - 1 : BLOCK // 2]
        sf = across(bf(q[sl] * jnp.exp(f - cf)), bf(k[sl] * jnp.exp(cf - f)))
        sb = across(bf(q[sl] * jnp.exp(g - cg)), bf(k[sl] * jnp.exp(cg - g)))
        store[sl, sl] = bf(jnp.where(lower, sf, 0.0) + jnp.where(upper, sb, 0.0))
        if b == 0:
            mine, other, edge = g, bwd[osl], bwd[BLOCK : BLOCK + 1]
        else:
            mine, other, edge = f, fwd[osl], fwd[BLOCK - 1 : BLOCK]
        store[sl, osl] = bf(across(bf(q[sl] * jnp.exp(mine - edge)), bf(k[osl] * jnp.exp(edge - other))))


def arrived_at(ref, sem):
    pltpu.make_async_copy(ref, ref, sem).wait()


def mixer_kernel(
    lat, context, cond, cond_ctx, gain_pre, gain_post, head_gain, w_shift, w_scale, w_gate,
    wq, wk, wv, wg, wo, w_down, decay_up, decay_bias,
    result,
    w_mod, partial, partials, tile, tiles, column_sum, mods, vectors, norms, lat_all, rows, w_all,
    proj, low, w_out,
    pack, packs, states, got_states, relays, relays_e, decays, got_decays, scores, local, entering,
    group, groups, ctx_group, ctx_groups, group_decays, all_decays,
    back, entry, before, leaving, entries, heads, part_a, part_b, near, sum_a, sum_b, relay_a, relay_c,
    s_load, m_sem, l_send, l_recv, w_sem, c_sem, x_sem, z_sem, e_sem, y_sem,
):
    z, x, y, c = position()
    x_peers = [lax.rem(x + d, NX) for d in (1, 3, 2)]
    z_peers = [lax.rem(z + d, NZ) for d in (4, 3, 5, 2, 6, 1, 7)]
    xy_peers = [
        dict(sp_1=lax.rem(x + k // NY, NX), tp=lax.rem(y + k % NY, NY)) for k in range(1, NX * NY)
    ]
    above, below, facing = (lax.rem(y + k, NY) for k in (1, 3, 2))
    up, down = dict(tp=above), dict(tp=below)
    east, west = lax.rem(x + 1, NX), lax.rem(x + 3, NX)
    opposite = lax.rem(x + 2, NX)
    other = dict(dp=1 - c)
    columns = [pl.ds(pl.multiple_of(k * HALF, HALF), HALF) for k in (c, 1 - c)]
    entered = greet([dict(sp_0=p) for p in z_peers] + xy_peers + [other])
    spans = (slice(0, 256), slice(256, 512), slice(512, 1024), slice(1024, 1536))
    sources = list(zip((wq, wk, wv, wg), spans))
    for k, w in enumerate((w_shift, w_scale, w_gate)):
        pltpu.make_async_copy(w, w_mod.at[k], s_load.at[0]).start()
    own_rows = pltpu.make_async_copy(lat, lat_all.at[y], s_load.at[1])
    own_rows.start()
    for w, span in sources:
        pltpu.make_async_copy(w, w_all.at[0, :, span], s_load.at[2]).start()
    own_out = pltpu.make_async_copy(wo, w_out.at[0], s_load.at[3])
    own_out.start()
    line = lax.broadcasted_iota(jnp.int32, (16, 128), 0)
    act = jax.nn.silu(cond[...].astype(F32)).astype(BF).astype(F32)
    act_ctx = jax.nn.silu(cond_ctx[...].astype(F32)).astype(BF).astype(F32)
    arrived_at(w_mod, s_load.at[0])
    total = None
    for k in range(3):
        left = jnp.where(line == k, act, jnp.where(line == k + 3, act_ctx, 0.0)).astype(BF)
        part = matmul(left, w_mod[k])
        total = part if total is None else total + part
    for k in range(NZ):
        partial[k] = total[:8, k * 128 : (k + 1) * 128]
    own_rows.wait()
    entered()
    for p in z_peers:
        send(partial.at[p], partials.at[z], m_sem.at[0], m_sem.at[1], sp_0=p)
    partials[z] = partial[z]
    top, bottom = pl.ds(0, 32), pl.ds(32, 32)
    up_1 = send(lat_all.at[y, top], lat_all.at[y, top], l_send.at[0], l_recv.at[0], **up)
    down_1 = send(lat_all.at[y, bottom], lat_all.at[y, bottom], l_send.at[0], l_recv.at[1], **down)
    for w, span in sources:
        send(w, w_all.at[1, :, span], w_sem.at[0], w_sem.at[1], **other)
    out_weight = send(wo, w_out.at[1], w_sem.at[2], w_sem.at[3], **other)

    def norm_of(source, target, length):
        def step(k, carry):
            v = source[pl.ds(pl.multiple_of(k * 16, 16), 16)].astype(F32)
            square = jnp.sum(v * v, axis=1, keepdims=True)
            norms[pl.ds(pl.multiple_of(target + k * 16, 16), 16)] = jnp.broadcast_to(
                lax.rsqrt(square / WIDTH + EPS), (16, 128)
            )
            return carry

        lax.fori_loop(0, length // 16, step, 0)

    norm_of(context, 0, 32)
    norm_of(lat_all.at[y], 32, 64)
    arrived_at(partials.at[pl.ds(0, NZ - 1)], m_sem.at[1])
    summed = partials[0]
    for k in range(1, NZ):
        summed = summed + partials[k]
    tile[...] = summed
    tiles[y * NX + x] = summed
    for w in xy_peers:
        send(tile, tiles.at[y * NX + x], m_sem.at[2], m_sem.at[3], **w)
    up_2 = send(lat_all.at[y, bottom], lat_all.at[y, bottom], l_send.at[0], l_recv.at[2], **up)
    down_2 = send(lat_all.at[y, top], lat_all.at[y, top], l_send.at[0], l_recv.at[3], **down)
    arrived_at(tiles.at[pl.ds(0, NX * NY - 1)], m_sem.at[3])
    for k in range(NY):
        block = tiles[k * NX] + tiles[k * NX + 1] + tiles[k * NX + 2] + tiles[k * NX + 3]
        column_sum[k] = block
        mods[z, k] = block
    for p in z_peers:
        send(column_sum, mods.at[z], m_sem.at[4], m_sem.at[5], sp_0=p)
    up_1.wait_recv()
    passed = lat_all.at[below, top]
    relay_up = send(passed, passed, l_send.at[0], l_recv.at[4], **up)
    down_1.wait_recv()
    passed = lat_all.at[above, bottom]
    relay_down = send(passed, passed, l_send.at[0], l_recv.at[5], **down)
    up_2.wait_recv()
    norm_of(lat_all.at[below], 96, 64)
    down_2.wait_recv()
    norm_of(lat_all.at[above], 160, 64)
    arrived_at(mods.at[pl.ds(0, NZ - 1)], m_sem.at[5])
    for k in range(NY):
        for j in range(NZ):
            at = (k * NZ + j) * 128
            vectors[:, at : at + 128] = mods[j, k]

    def modulate(source, target, scale_row, shift_row, length):
        def step(k, carry):
            at = pl.ds(pl.multiple_of(k * 16, 16), 16)
            to = pl.ds(pl.multiple_of(target + k * 16, 16), 16)
            norm = norms[to, 0:1]
            for h in range(2):
                weight = gain_pre[columns[h]].reshape(1, HALF).astype(F32) * (
                    1.0 + vectors[scale_row : scale_row + 1, columns[h]]
                )
                shift = vectors[shift_row : shift_row + 1, columns[h]]
                rows[h, to] = (source[at, columns[h]].astype(F32) * norm * weight + shift).astype(BF)
            return carry

        lax.fori_loop(0, length // 16, step, 0)

    def project_rows(at, length, places):
        def step(k, carry):
            span = pl.ds(pl.multiple_of(k * 256, 256), 256)
            out = matmul(rows[0, at : at + length], w_all[0, :, span])
            out = (out + matmul(rows[1, at : at + length], w_all[1, :, span])).astype(BF)
            for offset, place, count in places:
                to = pl.ds(pl.multiple_of(place, 32), count)
                proj[to, span] = out[offset : offset + count]
            return carry

        lax.fori_loop(0, 6, step, 0)
        out = across(rows[0, at : at + length], w_down[:, columns[0]])
        out = (out + across(rows[1, at : at + length], w_down[:, columns[1]])).astype(BF)
        for offset, place, count in places:
            low[pl.ds(pl.multiple_of(place, 32), count)] = out[offset : offset + count]

    modulate(context, 0, 4, 3, 32)
    modulate(lat_all.at[y], 32, 1, 0, 64)
    modulate(lat_all.at[below], 96, 1, 0, 64)
    arrived_at(w_all.at[0], s_load.at[2])
    arrived_at(w_all.at[1], w_sem.at[1])
    project_rows(0, 160, ((0, 256, 32), (32, y * 64, 64), (96, below * 64, 64)))
    for j in range(NX):
        pack[j] = jnp.zeros((32, 512), BF)
        pack[j, :, :DK_HEAD] = proj[256:288, 256:512]
        pack[j, :, DK_HEAD : DK_HEAD + 128] = proj[256:288, 512 + j * 128 : 640 + j * 128]
        pack[j, :, DK_HEAD + 128 : DK_HEAD + 128 + 2 * RANK] = low[256:288]
    for p in x_peers:
        send(pack.at[p], packs.at[x], c_sem.at[0], c_sem.at[1], sp_1=p)
    packs[x] = pack[x]
    modulate(lat_all.at[above], 160, 1, 0, 64)
    relay_up.wait_recv()
    relay_down.wait_recv()
    norm_of(lat_all.at[facing], 224, 64)
    modulate(lat_all.at[facing], 224, 1, 0, 64)
    project_rows(160, 128, ((0, above * 64, 64), (64, facing * 64, 64)))
    decay_f, decay_b = log_decays(low[:256], decay_up[...], decay_bias[...])
    fwd, bwd = running_sum(decay_f, True), running_sum(decay_b, False)
    decays[0:1] = fwd[-1:]
    decays[1:2] = bwd[:1]
    decays[2:8] = jnp.zeros((6, DK_HEAD), F32)
    for p in x_peers:
        send(decays, got_decays.at[x], c_sem.at[2], c_sem.at[3], sp_1=p)
    got_decays[x] = decays[...]
    k = proj[:256, 256:512].astype(F32)
    v = proj[:256, 512:1024]
    first, second = pl.ds(0, 64), pl.ds(64, 64)

    def swap(source, target, relay, way, sems):
        far = source.at[way, opposite]
        there = target.at[way, x]
        sent, got = sems.at[way, 0], sems.at[way, 1]
        passed = sems.at[way, 2]
        send(far.at[first], relay.at[way, 0], sent, passed, sp_1=east)
        send(far.at[second], relay.at[way, 1], sent, passed, sp_1=west)
        send(source.at[way, east], there, sent, got, sp_1=east)
        send(source.at[way, west], there, sent, got, sp_1=west)

    def pass_on(target, relay, way, sems):
        arrived_at(relay.at[way], sems.at[way, 2])
        sent, got = sems.at[way, 0], sems.at[way, 1]
        send(relay.at[way, 0], target.at[way, west, first], sent, got, sp_1=east)
        send(relay.at[way, 1], target.at[way, east, second], sent, got, sp_1=west)

    def swapped(target, way, sems):
        arrived_at(target.at[way, pl.ds(0, NX - 1)], sems.at[way, 1])

    def local_state(way, scaled):
        state = outer(v, (k * scaled).astype(BF)).astype(BF)
        for j in range(NX):
            states[way, j] = state[j * 128 : (j + 1) * 128]
        swap(states, got_states, relays, way, x_sem)
        got_states[way, x] = states[way, x]

    local_state(0, jnp.exp(fwd[-1:] - fwd))
    local_state(1, jnp.exp(bwd[:1] - bwd))
    arrived_at(packs.at[pl.ds(0, NX - 1)], c_sem.at[1])
    ctx = packs[...].reshape(NX * 32, 512)
    ctx_k = ctx[:, :DK_HEAD].astype(F32)
    ctx_v = ctx[:, DK_HEAD : DK_HEAD + 128]
    ctx_lr = ctx[:, DK_HEAD + 128 : DK_HEAD + 128 + 2 * RANK]
    cdf, cdb = log_decays(ctx_lr, decay_up[...], decay_bias[...])
    cf, cb = running_sum(cdf, True), running_sum(cdb, False)
    for way, scaled in enumerate((jnp.exp(cf[-1:] - cf), jnp.exp(cb[:1] - cb))):
        state = outer(ctx_v, (ctx_k * scaled).astype(BF)).astype(BF)
        for j in range(NZ):
            ctx_group[j, way] = state[j * 16 : (j + 1) * 16]
    for p in z_peers:
        send(ctx_group.at[p], ctx_groups.at[z], z_sem.at[0], z_sem.at[1], sp_0=p)
    ctx_groups[z] = ctx_group[z]
    pass_on(got_states, relays, 0, x_sem)
    arrived_at(got_decays.at[pl.ds(0, NX - 1)], c_sem.at[3])
    group_decays[0:2] = sum(got_decays[j, 0:2] for j in range(NX))
    group_decays[2:3] = cf[-1:]
    group_decays[3:4] = cb[:1]
    group_decays[4:8] = jnp.zeros((4, DK_HEAD), F32)
    for p in z_peers:
        send(group_decays, all_decays.at[z], z_sem.at[2], z_sem.at[3], sp_0=p)
    all_decays[z] = group_decays[...]
    pass_on(got_states, relays, 1, x_sem)
    q = proj[:256, :256].astype(F32) * DK_HEAD ** (-0.5)
    scores_of(q, k, fwd, bwd, scores)
    ways = (tuple(range(NX)), tuple(reversed(range(NX))))
    orders = (tuple(range(NZ)), tuple(reversed(range(NZ))))
    for way in range(2):
        swapped(got_states, way, x_sem)
        state = None
        for j in ways[way]:
            piece = got_states[way, j].astype(F32)
            state = piece if state is None else state * jnp.exp(got_decays[j, way : way + 1]) + piece
        state = state.astype(BF)
        for j in range(NZ):
            group[way, j] = state[j * 16 : (j + 1) * 16]
        for p in z_peers:
            send(group.at[way, p], groups.at[way, z], z_sem.at[4 + way], z_sem.at[6 + way], sp_0=p)
        groups[way, z] = group[way, z]
    for way in range(2):
        state = jnp.zeros((128, DK_HEAD), F32)
        for j in ways[way]:
            before[way, j] = state
            state = state * jnp.exp(got_decays[j, way : way + 1]) + got_states[way, j].astype(F32)
    local[...] = matmul(scores[...], v)
    entering[0] = (q * jnp.exp(fwd)).astype(BF)
    entering[1] = (q * jnp.exp(bwd)).astype(BF)
    arrived_at(ctx_groups.at[pl.ds(0, NZ - 1)], z_sem.at[1])
    arrived_at(all_decays.at[pl.ds(0, NZ - 1)], z_sem.at[3])
    starts = []
    for way in range(2):
        state = jnp.zeros((16, DK_HEAD), F32)
        for j in orders[way]:
            state = state * jnp.exp(all_decays[j, 2 + way : 3 + way]) + ctx_groups[j, way].astype(F32)
        starts.append(state)
    for way in range(2):
        arrived_at(groups.at[way, pl.ds(0, NZ - 1)], z_sem.at[6 + way])
        state = starts[way]
        for j in orders[way]:
            back[way, j] = state.astype(BF)
            state = state * jnp.exp(all_decays[j, way : way + 1]) + groups[way, j].astype(F32)
        for p in z_peers:
            send(back.at[way, p], entry.at[way, z], z_sem.at[8 + way], z_sem.at[10 + way], sp_0=p)
        entry[way, z] = back[way, z]
    gate = jax.nn.silu(proj[:256, 1024:1536].astype(F32)) * head_gain[...].reshape(1, DV_HEAD).astype(F32)
    for way in range(2):
        arrived_at(entry.at[way, pl.ds(0, NZ - 1)], z_sem.at[10 + way])
        start = entry[way].reshape(128, DK_HEAD).astype(F32)
        passed = jnp.zeros((1, DK_HEAD), F32)
        for j in ways[way]:
            leaving[way, j] = (start * jnp.exp(passed) + before[way, j]).astype(BF)
            passed = passed + got_decays[j, way : way + 1]
        swap(leaving, entries, relays_e, way, e_sem)
        entries[way, x] = leaving[way, x]
    pass_on(entries, relays_e, 0, e_sem)
    pass_on(entries, relays_e, 1, e_sem)
    own_out.wait()
    out_weight.wait_recv()
    swapped(entries, 0, e_sem)
    out = [
        local[:, j * 128 : (j + 1) * 128] + across(entering[0], entries[0, j]) for j in range(NX)
    ]
    swapped(entries, 1, e_sem)
    out = [o + across(entering[1], entries[1, j]) for j, o in enumerate(out)]
    square = sum(jnp.sum(o * o, axis=1, keepdims=True) for o in out)
    scale = lax.rsqrt(square / DV_HEAD + EPS)
    for j in range(NX):
        heads[:, j * 128 : (j + 1) * 128] = (out[j] * scale * gate[:, j * 128 : (j + 1) * 128]).astype(BF)
    count = 64

    def project(owner, part, half):
        at = heads[pl.ds(pl.multiple_of(owner * count, count), count)]
        part[owner] = matmul(at, w_out[half]).astype(BF)

    project(facing, part_a, 0)
    first_a = send(part_a.at[facing], relay_a, y_sem.at[0], y_sem.at[1], **down)
    project(facing, part_b, 1)
    first_b = send(part_b.at[facing], relay_c, y_sem.at[0], y_sem.at[2], **up)
    project(below, part_b, 1)
    send(part_b.at[below], near.at[1], y_sem.at[0], y_sem.at[3], **down)
    project(above, part_a, 0)
    send(part_a.at[above], near.at[0], y_sem.at[0], y_sem.at[3], **up)
    project(below, part_a, 0)
    project(above, part_b, 1)
    first_a.wait_recv()
    sum_a[...] = (relay_a[...].astype(F32) + part_a[below].astype(F32)).astype(BF)
    send(sum_a, near.at[2], y_sem.at[0], y_sem.at[3], **down)
    first_b.wait_recv()
    sum_b[...] = (relay_c[...].astype(F32) + part_b[above].astype(F32)).astype(BF)
    send(sum_b, near.at[3], y_sem.at[0], y_sem.at[3], **up)
    project(y, part_a, 0)
    project(y, part_b, 1)
    arrived_at(partials.at[pl.ds(0, NZ - 1)], m_sem.at[0])
    arrived_at(tiles.at[pl.ds(0, NX * NY - 1)], m_sem.at[2])
    arrived_at(mods.at[pl.ds(0, NZ - 1)], m_sem.at[4])
    arrived_at(lat_all.at[pl.ds(0, 3)], l_send.at[0])
    arrived_at(w_all.at[1], w_sem.at[0])
    out_weight.wait_send()
    arrived_at(packs.at[pl.ds(0, NX - 1)], c_sem.at[0])
    arrived_at(got_decays.at[pl.ds(0, NX - 1)], c_sem.at[2])
    arrived_at(ctx_groups.at[pl.ds(0, NZ - 1)], z_sem.at[0])
    arrived_at(all_decays.at[pl.ds(0, NZ - 1)], z_sem.at[2])
    for way in range(2):
        arrived_at(states.at[way], x_sem.at[way, 0])
        arrived_at(leaving.at[way], e_sem.at[way, 0])
        arrived_at(groups.at[way, pl.ds(0, NZ - 1)], z_sem.at[4 + way])
        arrived_at(entry.at[way, pl.ds(0, NZ - 1)], z_sem.at[8 + way])
    arrived_at(near, y_sem.at[3])

    def finish(k, carry):
        at = pl.ds(pl.multiple_of(k * 16, 16), 16)
        a = part_a[y, at].astype(F32) + near[0, at].astype(F32) + near[2, at].astype(F32)
        b = part_b[y, at].astype(F32) + near[1, at].astype(F32) + near[3, at].astype(F32)
        square = jnp.sum(a * a, axis=1, keepdims=True) + jnp.sum(b * b, axis=1, keepdims=True)
        scale = lax.rsqrt(square / WIDTH + EPS)
        for span, half in zip(columns, (a, b)):
            weight = vectors[2:3, span] * gain_post[span].reshape(1, HALF).astype(F32)
            result[at, span] = (
                lat_all[y, at, span].astype(F32) + half * scale * weight
            ).astype(BF)
        return carry

    lax.fori_loop(0, count // 16, finish, 0)
    arrived_at(lat_all.at[pl.ds(0, 3)], y_sem.at[0])


def mixer(*args):
    dma = pltpu.SemaphoreType.DMA
    vm = pltpu.VMEM
    half = vm((64, HALF), BF)
    in_specs = [VM] * len(args)
    for k in (0, 7, 8, 9, 10, 11, 12, 13, 14):
        in_specs[k] = ANY
    slices = vm((2, NX, 128, DK_HEAD), BF)
    thin = vm((2, NZ, 16, DK_HEAD), BF)
    return pl.pallas_call(
        mixer_kernel,
        out_shape=shape_of(64, WIDTH),
        in_specs=in_specs,
        out_specs=VM,
        scratch_shapes=[
            vm((3, 128, 1024), BF), vm((NZ, 8, 128), F32), vm((NZ, 8, 128), F32),
            vm((8, 128), F32), vm((NY * NX, 8, 128), F32), vm((NY, 8, 128), F32),
            vm((NZ, NY, 8, 128), F32), vm((8, WIDTH), F32), vm((288, 128), F32),
            vm((NY, 64, WIDTH), BF), vm((2, 288, HALF), BF), vm((2, HALF, 1536), BF),
            vm((288, 1536), BF), vm((288, 2 * RANK), BF), vm((2, DV_HEAD, HALF), BF),
            vm((NX, 32, 512), BF), vm((NX, 32, 512), BF),
            slices, slices, vm((2, 2, 64, DK_HEAD), BF), vm((2, 2, 64, DK_HEAD), BF),
            vm((8, DK_HEAD), F32), vm((NX, 8, DK_HEAD), F32),
            vm((256, 256), BF), vm((256, DV_HEAD), F32), vm((2, 256, DK_HEAD), BF),
            thin, thin, vm((NZ, 2, 16, DK_HEAD), BF), vm((NZ, 2, 16, DK_HEAD), BF),
            vm((8, DK_HEAD), F32), vm((NZ, 8, DK_HEAD), F32),
            thin, thin, vm((2, NX, 128, DK_HEAD), F32), slices, slices,
            vm((256, DV_HEAD), BF),
            vm((NY, 64, HALF), BF), vm((NY, 64, HALF), BF), vm((4, 64, HALF), BF),
            half, half, half, half,
            dma((4,)), dma((6,)), dma((1,)), dma((6,)), dma((4,)), dma((4,)),
            dma((2, 3)), dma((12,)), dma((2, 3)), dma((4,)),
        ],
        compiler_params=pltpu.CompilerParams(
            collective_id=0, has_side_effects=True, vmem_limit_bytes=60 * 2**20
        ),
        name="mixer",
    )(*args)


def body(
    latents, cond, cond_ctx, context, w_shift, w_scale, w_gate, gain_pre, gain_post,
    w_query, w_key, w_value, w_outgate, w_down, decay_up, decay_bias, head_gain, w_out,
):
    result = mixer(
        latents[0], context[0], cond, cond_ctx[None], gain_pre, gain_post, head_gain,
        w_shift, w_scale, w_gate, w_query, w_key, w_value, w_outgate, w_out,
        w_down.T, decay_up, decay_bias,
    )
    return result[None]


def solution(mesh):
    finer = Mesh(
        mesh.devices.reshape(8, 4, mesh.shape["tp"], mesh.shape["dp"]), ("sp_0", "sp_1", "tp", "dp")
    )
    in_specs = (
        P("dp", SP_TP, None),
        P("dp", SP),
        P(SP),
        P("dp", SP, None),
        P(SP, "tp"),
        P(SP, "tp"),
        P(SP, "tp"),
        P(),
        P(),
        P("dp", "tp"),
        P("dp", "tp"),
        P("dp", "tp"),
        P("dp", "tp"),
        P(),
        P(None, None, "tp"),
        P(None, "tp"),
        P("tp"),
        P("tp", "dp"),
    )
    out_specs = P("dp", SP_TP, None)
    return jax.shard_map(body, mesh=finer, in_specs=in_specs, out_specs=out_specs, check_vma=False)
```

```python
import jax
import jax.numpy as jnp
from jax import lax
from jax.experimental import pallas as pl
from jax.experimental.pallas import tpu as pltpu
from jax.sharding import Mesh
from jax.sharding import PartitionSpec as P

DK_HEAD = 256
DV_HEAD = 512
RANK = 16
BLOCK = 128
SP_TP = ("sp_0", "sp_1", "tp")
SP = ("sp_0", "sp_1")
NZ, NX, NY = 8, 4, 4
WIDTH = 4096
HALF = 2048
ANY = pl.BlockSpec(memory_space=pl.ANY)
VM = pl.BlockSpec(memory_space=pltpu.VMEM)
BF, F32 = jnp.bfloat16, jnp.float32


EPS = 1e-06
TAU = 16.0


def matmul(left, right):
    return jnp.dot(left, right, preferred_element_type=jnp.float32)


def rms_scale(vectors, gain):
    return vectors * lax.rsqrt(jnp.mean(vectors * vectors, axis=-1, keepdims=True) + EPS) * gain


def shape_of(*dims, dtype=BF):
    return jax.ShapeDtypeStruct(dims, dtype)


def send(src, dst, send_sem, recv_sem, **where):
    copy = pltpu.make_async_remote_copy(
        src_ref=src,
        dst_ref=dst,
        send_sem=send_sem,
        recv_sem=recv_sem,
        device_id=where,
        device_id_type=pl.DeviceIdType.MESH,
    )
    copy.start()
    return copy


def greet(partners):
    barrier = pltpu.get_barrier_semaphore()
    for where in partners:
        pl.semaphore_signal(
            barrier, inc=1, device_id=where, device_id_type=pl.DeviceIdType.MESH
        )
    return lambda: pl.semaphore_wait(barrier, len(partners))


def position():
    return tuple(lax.axis_index(a) for a in ("sp_0", "sp_1", "tp", "dp"))


def log_sigmoid(v):
    return jnp.minimum(v, 0.0) - jnp.log1p(jnp.exp(-jnp.abs(v)))


def log_decays(lowrank, decay_up, decay_bias):
    return [
        log_sigmoid(
            matmul(lowrank[:, way * RANK : (way + 1) * RANK], decay_up[way])
            + decay_bias[way : way + 1]
        )
        / TAU
        for way in range(2)
    ]


def triangle(n, lower):
    r = lax.broadcasted_iota(jnp.int32, (n, n), 0)
    c = lax.broadcasted_iota(jnp.int32, (n, n), 1)
    return r >= c if lower else r <= c


def running_sums(decay_f, decay_b):
    n = decay_f.shape[0]
    parts = []
    for decay in (decay_f, decay_b):
        high = decay.astype(BF)
        parts += [high, (decay - high.astype(F32)).astype(BF)]
    fwd = matmul(jnp.where(triangle(n, True), 1.0, 0.0).astype(BF), parts[0])
    fwd = fwd + matmul(jnp.where(triangle(n, True), 1.0, 0.0).astype(BF), parts[1])
    bwd = matmul(jnp.where(triangle(n, False), 1.0, 0.0).astype(BF), parts[2])
    bwd = bwd + matmul(jnp.where(triangle(n, False), 1.0, 0.0).astype(BF), parts[3])
    return fwd, bwd


def across(left, right):
    return lax.dot_general(left, right, (((1,), (1,)), ((), ())), preferred_element_type=F32)


def outer(left, right):
    return lax.dot_general(left, right, (((0,), (0,)), ((), ())), preferred_element_type=F32)


def scores_of(q, k, fwd, bwd, store):
    lower, upper = triangle(BLOCK, True), triangle(BLOCK, False)
    bf = lambda a: a.astype(BF)
    for b in range(2):
        sl = slice(b * BLOCK, (b + 1) * BLOCK)
        osl = slice((1 - b) * BLOCK, (2 - b) * BLOCK)
        f, g = fwd[sl], bwd[sl]
        cf, cg = f[BLOCK // 2 : BLOCK // 2 + 1], g[BLOCK // 2 - 1 : BLOCK // 2]
        sf = across(bf(q[sl] * jnp.exp(f - cf)), bf(k[sl] * jnp.exp(cf - f)))
        sb = across(bf(q[sl] * jnp.exp(g - cg)), bf(k[sl] * jnp.exp(cg - g)))
        store[sl, sl] = bf(jnp.where(lower, sf, 0.0) + jnp.where(upper, sb, 0.0))
        if b == 0:
            mine, other, edge = g, bwd[osl], bwd[BLOCK : BLOCK + 1]
        else:
            mine, other, edge = f, fwd[osl], fwd[BLOCK - 1 : BLOCK]
        store[sl, osl] = bf(across(bf(q[sl] * jnp.exp(mine - edge)), bf(k[osl] * jnp.exp(edge - other))))


def arrived_at(ref, sem):
    pltpu.make_async_copy(ref, ref, sem).wait()


def mixer_kernel(
    lat, *inputs_and_rest
):
    (
    context_in, cond_in, cond_ctx_in, gain_pre_in, gain_post_in, head_gain_in, w_shift, w_scale, w_gate,
    wq, wk, wv, wg, wo, w_down_in, decay_up_in, decay_bias_in,
    result,
    context, cond, cond_ctx, gain_pre, gain_post, head_gain, w_down, decay_up, decay_bias,
    factor, offset, w_mod, partial, partials, tile, tiles, column_sum, mods, vectors, norms, lat_all, rows, w_all,
    proj, low, w_out,
    pack, packs, states, got_states, relays, relays_e, decays, got_decays, scores, local, entering,
    group, groups, ctx_group, ctx_groups, group_decays, all_decays,
    back, entry, before, leaving, entries, heads, part_a, part_b, near, sum_a, sum_b, relay_a, relay_c,
    s_load, s_small, m_sem, l_send, l_recv, w_sem, c_sem, x_sem, z_sem, e_sem, y_sem,
    ) = inputs_and_rest
    z, x, y, c = position()
    x_peers = [lax.rem(x + d, NX) for d in (1, 3, 2)]
    z_peers = [lax.rem(z + d, NZ) for d in (4, 3, 5, 2, 6, 1, 7)]
    xy_peers = [
        dict(sp_1=lax.rem(x + k // NY, NX), tp=lax.rem(y + k % NY, NY)) for k in range(1, NX * NY)
    ]
    above, below, facing = (lax.rem(y + k, NY) for k in (1, 3, 2))
    up, down = dict(tp=above), dict(tp=below)
    east, west = lax.rem(x + 1, NX), lax.rem(x + 3, NX)
    opposite = lax.rem(x + 2, NX)
    other = dict(dp=1 - c)
    columns = [pl.ds(pl.multiple_of(k * HALF, HALF), HALF) for k in (c, 1 - c)]
    entered = greet([dict(sp_0=p) for p in z_peers] + xy_peers + [other])
    spans = (slice(0, 256), slice(256, 768), slice(768, 1024), slice(1024, 1536))
    sources = list(zip((wk, wv, wq, wg), spans))
    own_rows = pltpu.make_async_copy(lat, lat_all.at[y], s_load.at[1])
    own_rows.start()
    small = [
        pltpu.make_async_copy(src, dst, s_small.at[k])
        for k, (src, dst) in enumerate(
            [
                (cond_in, cond), (cond_ctx_in, cond_ctx), (context_in, context),
                (gain_pre_in, gain_pre), (gain_post_in, gain_post), (head_gain_in, head_gain),
                (w_down_in, w_down), (decay_up_in, decay_up), (decay_bias_in, decay_bias),
            ]
        )
    ]
    for load in small[:2]:
        load.start()
    for k, w in enumerate((w_shift, w_scale, w_gate)):
        pltpu.make_async_copy(w, w_mod.at[k], s_load.at[0]).start()
    for load in small[2:]:
        load.start()
    for w, span in sources:
        pltpu.make_async_copy(w, w_all.at[0, :, span], s_load.at[2]).start()
    own_out = pltpu.make_async_copy(wo, w_out.at[0], s_load.at[3])
    own_out.start()
    own_rows.wait()
    entered()
    top, bottom = pl.ds(0, 32), pl.ds(32, 32)
    up_1 = send(lat_all.at[y, top], lat_all.at[y, top], l_send.at[0], l_recv.at[0], **up)
    down_1 = send(lat_all.at[y, bottom], lat_all.at[y, bottom], l_send.at[0], l_recv.at[1], **down)
    small[0].wait()
    small[1].wait()
    line = lax.broadcasted_iota(jnp.int32, (16, 128), 0)
    act = jax.nn.silu(cond[...].astype(F32)).astype(BF).astype(F32)
    act_ctx = jax.nn.silu(cond_ctx[...].astype(F32)).astype(BF).astype(F32)
    arrived_at(w_mod, s_load.at[0])
    total = None
    for k in range(3):
        left = jnp.where(line == k, act, jnp.where(line == k + 3, act_ctx, 0.0)).astype(BF)
        part = matmul(left, w_mod[k])
        total = part if total is None else total + part
    for k in range(NZ):
        partial[k] = total[:8, k * 128 : (k + 1) * 128]
    for p in z_peers:
        send(partial.at[p], partials.at[z], m_sem.at[0], m_sem.at[1], sp_0=p)
    partials[z] = partial[z]
    for w, span in sources:
        send(w, w_all.at[1, :, span], w_sem.at[0], w_sem.at[1], **other)
    out_weight = send(wo, w_out.at[1], w_sem.at[2], w_sem.at[3], **other)

    def norm_of(source, target, length):
        def step(k, carry):
            v = source[pl.ds(pl.multiple_of(k * 16, 16), 16)].astype(F32)
            square = jnp.sum(v * v, axis=1, keepdims=True)
            norms[pl.ds(pl.multiple_of(target + k * 16, 16), 16)] = jnp.broadcast_to(
                lax.rsqrt(square / WIDTH + EPS), (16, 128)
            )
            return carry

        lax.fori_loop(0, length // 16, step, 0)

    for load in small[2:]:
        load.wait()
    ones = jnp.ones((1, WIDTH), F32)
    zeros = jnp.zeros((1, WIDTH), F32)
    pre = gain_pre[...].reshape(1, WIDTH).astype(F32)
    post = gain_post[...].reshape(1, WIDTH).astype(F32)
    for k, (by, plus) in enumerate(
        ((ones, zeros), (pre, pre), (post, zeros), (ones, zeros), (pre, pre))
    ):
        factor[k : k + 1] = by
        offset[k : k + 1] = plus
    norm_of(context, 0, 32)
    norm_of(lat_all.at[y], 32, 64)
    arrived_at(partials.at[pl.ds(0, NZ - 1)], m_sem.at[1])
    summed = partials[0]
    for k in range(1, NZ):
        summed = summed + partials[k]
    tile[...] = summed
    tiles[y * NX + x] = summed
    for w in xy_peers:
        send(tile, tiles.at[y * NX + x], m_sem.at[2], m_sem.at[3], **w)
    up_2 = send(lat_all.at[y, bottom], lat_all.at[y, bottom], l_send.at[0], l_recv.at[2], **up)
    down_2 = send(lat_all.at[y, top], lat_all.at[y, top], l_send.at[0], l_recv.at[3], **down)
    arrived_at(tiles.at[pl.ds(0, NX * NY - 1)], m_sem.at[3])
    for k in range(NY):
        block = tiles[k * NX] + tiles[k * NX + 1] + tiles[k * NX + 2] + tiles[k * NX + 3]
        column_sum[k] = block
        mods[z, k] = block
    for p in z_peers:
        send(column_sum, mods.at[z], m_sem.at[4], m_sem.at[5], sp_0=p)
    up_1.wait_recv()
    passed = lat_all.at[below, top]
    relay_up = send(passed, passed, l_send.at[0], l_recv.at[4], **up)
    down_1.wait_recv()
    passed = lat_all.at[above, bottom]
    relay_down = send(passed, passed, l_send.at[0], l_recv.at[5], **down)
    arrived_at(mods.at[pl.ds(0, NZ - 1)], m_sem.at[5])
    for k in range(NY):
        for j in range(NZ):
            at = (k * NZ + j) * 128
            span = slice(at, at + 128)
            vectors[:, span] = mods[j, k] * factor[:, span] + offset[:, span]

    def modulate(source, target, scale_row, shift_row, length, known):
        def step(k, carry):
            at = pl.ds(pl.multiple_of(k * 16, 16), 16)
            to = pl.ds(pl.multiple_of(target + k * 16, 16), 16)
            halves = [source[at, columns[h]].astype(F32) for h in range(2)]
            if known:
                norm = norms[to, 0:1]
            else:
                square = sum(jnp.sum(v * v, axis=1, keepdims=True) for v in halves)
                norm = lax.rsqrt(square / WIDTH + EPS)
            for h in range(2):
                weight = vectors[scale_row : scale_row + 1, columns[h]]
                shift = vectors[shift_row : shift_row + 1, columns[h]]
                rows[h, to] = (halves[h] * norm * weight + shift).astype(BF)
            return carry

        lax.fori_loop(0, length // 16, step, 0)

    def project_rows(at, length, places, chunks):
        def step(k, carry):
            span = pl.ds(pl.multiple_of(k * 256, 256), 256)
            out = matmul(rows[0, at : at + length], w_all[0, :, span])
            out = (out + matmul(rows[1, at : at + length], w_all[1, :, span])).astype(BF)
            for offset, place, count in places:
                to = pl.ds(pl.multiple_of(place, 32), count)
                proj[to, span] = out[offset - at : offset - at + count]
            return carry

        lax.fori_loop(chunks.start, chunks.stop, step, 0)

    def project_down(at, length, places):
        out = across(rows[0, at : at + length], w_down[:, columns[0]])
        out = (out + across(rows[1, at : at + length], w_down[:, columns[1]])).astype(BF)
        for offset, place, count in places:
            low[pl.ds(pl.multiple_of(place, 32), count)] = out[offset - at : offset - at + count]

    modulate(context, 0, 4, 3, 32, True)
    modulate(lat_all.at[y], 32, 1, 0, 64, True)
    up_2.wait_recv()
    modulate(lat_all.at[below], 96, 1, 0, 64, False)
    down_2.wait_recv()
    modulate(lat_all.at[above], 160, 1, 0, 64, False)
    arrived_at(w_all.at[0], s_load.at[2])
    arrived_at(w_all.at[1], w_sem.at[1])
    places = ((32, y * 64, 64), (96, below * 64, 64), (160, above * 64, 64), (224, facing * 64, 64))
    project_rows(0, 224, ((0, 256, 32), *places[:3]), range(0, 3))
    project_down(0, 224, ((0, 256, 32), *places[:3]))
    for j in range(NX):
        pack[j] = jnp.zeros((32, 512), BF)
        pack[j, :, :DK_HEAD] = proj[256:288, 0:256]
        pack[j, :, DK_HEAD : DK_HEAD + 128] = proj[256:288, 256 + j * 128 : 384 + j * 128]
        pack[j, :, DK_HEAD + 128 : DK_HEAD + 128 + 2 * RANK] = low[256:288]
    for p in x_peers:
        send(pack.at[p], packs.at[x], c_sem.at[0], c_sem.at[1], sp_1=p)
    packs[x] = pack[x]
    relay_up.wait_recv()
    relay_down.wait_recv()
    modulate(lat_all.at[facing], 224, 1, 0, 64, False)
    project_rows(224, 64, places[3:], range(0, 3))
    project_down(224, 64, places[3:])
    decay_f, decay_b = log_decays(low[:256], decay_up[...], decay_bias[...])
    fwd, bwd = running_sums(decay_f, decay_b)
    decays[0:1] = fwd[-1:]
    decays[1:2] = bwd[:1]
    decays[2:8] = jnp.zeros((6, DK_HEAD), F32)
    for p in x_peers:
        send(decays, got_decays.at[x], c_sem.at[2], c_sem.at[3], sp_1=p)
    got_decays[x] = decays[...]
    k = proj[:256, :256].astype(F32)
    v = proj[:256, 256:768]
    first, second = pl.ds(0, 64), pl.ds(64, 64)

    def swap(source, target, relay, way, sems):
        far = source.at[way, opposite]
        there = target.at[way, x]
        sent, got = sems.at[way, 0], sems.at[way, 1]
        passed = sems.at[way, 2]
        send(far.at[first], relay.at[way, 0], sent, passed, sp_1=east)
        send(far.at[second], relay.at[way, 1], sent, passed, sp_1=west)
        send(source.at[way, east], there, sent, got, sp_1=east)
        send(source.at[way, west], there, sent, got, sp_1=west)

    def pass_on(target, relay, way, sems):
        arrived_at(relay.at[way], sems.at[way, 2])
        sent, got = sems.at[way, 0], sems.at[way, 1]
        send(relay.at[way, 0], target.at[way, west, first], sent, got, sp_1=east)
        send(relay.at[way, 1], target.at[way, east, second], sent, got, sp_1=west)

    def swapped(target, way, sems):
        arrived_at(target.at[way, pl.ds(0, NX - 1)], sems.at[way, 1])

    def local_state(way, scaled):
        state = outer(v, (k * scaled).astype(BF)).astype(BF)
        for j in range(NX):
            states[way, j] = state[j * 128 : (j + 1) * 128]
        swap(states, got_states, relays, way, x_sem)
        got_states[way, x] = states[way, x]

    local_state(0, jnp.exp(fwd[-1:] - fwd))
    local_state(1, jnp.exp(bwd[:1] - bwd))
    arrived_at(packs.at[pl.ds(0, NX - 1)], c_sem.at[1])
    ctx = packs[...].reshape(NX * 32, 512)
    ctx_k = ctx[:, :DK_HEAD].astype(F32)
    ctx_v = ctx[:, DK_HEAD : DK_HEAD + 128]
    ctx_lr = ctx[:, DK_HEAD + 128 : DK_HEAD + 128 + 2 * RANK]
    cdf, cdb = log_decays(ctx_lr, decay_up[...], decay_bias[...])
    cf, cb = running_sums(cdf, cdb)
    for way, scaled in enumerate((jnp.exp(cf[-1:] - cf), jnp.exp(cb[:1] - cb))):
        state = outer(ctx_v, (ctx_k * scaled).astype(BF)).astype(BF)
        for j in range(NZ):
            ctx_group[j, way] = state[j * 16 : (j + 1) * 16]
    for p in z_peers:
        send(ctx_group.at[p], ctx_groups.at[z], z_sem.at[0], z_sem.at[1], sp_0=p)
    ctx_groups[z] = ctx_group[z]
    project_rows(32, 256, places, range(3, 4))
    pass_on(got_states, relays, 0, x_sem)
    arrived_at(got_decays.at[pl.ds(0, NX - 1)], c_sem.at[3])
    group_decays[0:2] = sum(got_decays[j, 0:2] for j in range(NX))
    group_decays[2:3] = cf[-1:]
    group_decays[3:4] = cb[:1]
    group_decays[4:8] = jnp.zeros((4, DK_HEAD), F32)
    for p in z_peers:
        send(group_decays, all_decays.at[z], z_sem.at[2], z_sem.at[3], sp_0=p)
    all_decays[z] = group_decays[...]
    pass_on(got_states, relays, 1, x_sem)
    q = proj[:256, 768:1024].astype(F32) * DK_HEAD ** (-0.5)
    scores_of(q, k, fwd, bwd, scores)
    ways = (tuple(range(NX)), tuple(reversed(range(NX))))
    orders = (tuple(range(NZ)), tuple(reversed(range(NZ))))
    for way in range(2):
        swapped(got_states, way, x_sem)
        state = None
        for j in ways[way]:
            piece = got_states[way, j].astype(F32)
            state = piece if state is None else state * jnp.exp(got_decays[j, way : way + 1]) + piece
        state = state.astype(BF)
        for j in range(NZ):
            group[way, j] = state[j * 16 : (j + 1) * 16]
        for p in z_peers:
            send(group.at[way, p], groups.at[way, z], z_sem.at[4 + way], z_sem.at[6 + way], sp_0=p)
        groups[way, z] = group[way, z]
    project_rows(32, 256, places, range(4, 6))
    for way in range(2):
        state = jnp.zeros((128, DK_HEAD), F32)
        for j in ways[way]:
            before[way, j] = state
            state = state * jnp.exp(got_decays[j, way : way + 1]) + got_states[way, j].astype(F32)
    local[...] = matmul(scores[...], v)
    entering[0] = (q * jnp.exp(fwd)).astype(BF)
    entering[1] = (q * jnp.exp(bwd)).astype(BF)
    arrived_at(ctx_groups.at[pl.ds(0, NZ - 1)], z_sem.at[1])
    arrived_at(all_decays.at[pl.ds(0, NZ - 1)], z_sem.at[3])
    starts = []
    for way in range(2):
        state = jnp.zeros((16, DK_HEAD), F32)
        for j in orders[way]:
            state = state * jnp.exp(all_decays[j, 2 + way : 3 + way]) + ctx_groups[j, way].astype(F32)
        starts.append(state)
    for way in range(2):
        arrived_at(groups.at[way, pl.ds(0, NZ - 1)], z_sem.at[6 + way])
        state = starts[way]
        for j in orders[way]:
            back[way, j] = state.astype(BF)
            state = state * jnp.exp(all_decays[j, way : way + 1]) + groups[way, j].astype(F32)
        for p in z_peers:
            send(back.at[way, p], entry.at[way, z], z_sem.at[8 + way], z_sem.at[10 + way], sp_0=p)
        entry[way, z] = back[way, z]
    gate = jax.nn.silu(proj[:256, 1024:1536].astype(F32)) * head_gain[...].reshape(1, DV_HEAD).astype(F32)
    for way in range(2):
        arrived_at(entry.at[way, pl.ds(0, NZ - 1)], z_sem.at[10 + way])
        start = entry[way].reshape(128, DK_HEAD).astype(F32)
        passed = jnp.zeros((1, DK_HEAD), F32)
        for j in ways[way]:
            leaving[way, j] = (start * jnp.exp(passed) + before[way, j]).astype(BF)
            passed = passed + got_decays[j, way : way + 1]
        swap(leaving, entries, relays_e, way, e_sem)
        entries[way, x] = leaving[way, x]
    pass_on(entries, relays_e, 0, e_sem)
    pass_on(entries, relays_e, 1, e_sem)
    own_out.wait()
    out_weight.wait_recv()
    swapped(entries, 0, e_sem)
    out = [
        local[:, j * 128 : (j + 1) * 128] + across(entering[0], entries[0, j]) for j in range(NX)
    ]
    swapped(entries, 1, e_sem)
    out = [o + across(entering[1], entries[1, j]) for j, o in enumerate(out)]
    square = sum(jnp.sum(o * o, axis=1, keepdims=True) for o in out)
    scale = lax.rsqrt(square / DV_HEAD + EPS)
    for j in range(NX):
        heads[:, j * 128 : (j + 1) * 128] = (out[j] * scale * gate[:, j * 128 : (j + 1) * 128]).astype(BF)
    count = 64

    def project(owner, part, half):
        at = heads[pl.ds(pl.multiple_of(owner * count, count), count)]
        part[owner] = matmul(at, w_out[half]).astype(BF)

    project(facing, part_a, 0)
    first_a = send(part_a.at[facing], relay_a, y_sem.at[0], y_sem.at[1], **down)
    project(facing, part_b, 1)
    first_b = send(part_b.at[facing], relay_c, y_sem.at[0], y_sem.at[2], **up)
    project(below, part_b, 1)
    send(part_b.at[below], near.at[1], y_sem.at[0], y_sem.at[3], **down)
    project(above, part_a, 0)
    send(part_a.at[above], near.at[0], y_sem.at[0], y_sem.at[3], **up)
    project(below, part_a, 0)
    project(above, part_b, 1)
    first_a.wait_recv()
    sum_a[...] = (relay_a[...].astype(F32) + part_a[below].astype(F32)).astype(BF)
    send(sum_a, near.at[2], y_sem.at[0], y_sem.at[3], **down)
    first_b.wait_recv()
    sum_b[...] = (relay_c[...].astype(F32) + part_b[above].astype(F32)).astype(BF)
    send(sum_b, near.at[3], y_sem.at[0], y_sem.at[3], **up)
    project(y, part_a, 0)
    project(y, part_b, 1)
    arrived_at(partials.at[pl.ds(0, NZ - 1)], m_sem.at[0])
    arrived_at(tiles.at[pl.ds(0, NX * NY - 1)], m_sem.at[2])
    arrived_at(mods.at[pl.ds(0, NZ - 1)], m_sem.at[4])
    arrived_at(lat_all.at[pl.ds(0, 3)], l_send.at[0])
    arrived_at(w_all.at[1], w_sem.at[0])
    out_weight.wait_send()
    arrived_at(packs.at[pl.ds(0, NX - 1)], c_sem.at[0])
    arrived_at(got_decays.at[pl.ds(0, NX - 1)], c_sem.at[2])
    arrived_at(ctx_groups.at[pl.ds(0, NZ - 1)], z_sem.at[0])
    arrived_at(all_decays.at[pl.ds(0, NZ - 1)], z_sem.at[2])
    for way in range(2):
        arrived_at(states.at[way], x_sem.at[way, 0])
        arrived_at(leaving.at[way], e_sem.at[way, 0])
        arrived_at(groups.at[way, pl.ds(0, NZ - 1)], z_sem.at[4 + way])
        arrived_at(entry.at[way, pl.ds(0, NZ - 1)], z_sem.at[8 + way])
    arrived_at(near, y_sem.at[3])

    def finish(k, carry):
        at = pl.ds(pl.multiple_of(k * 16, 16), 16)
        a = part_a[y, at].astype(F32) + near[0, at].astype(F32) + near[2, at].astype(F32)
        b = part_b[y, at].astype(F32) + near[1, at].astype(F32) + near[3, at].astype(F32)
        square = jnp.sum(a * a, axis=1, keepdims=True) + jnp.sum(b * b, axis=1, keepdims=True)
        scale = lax.rsqrt(square / WIDTH + EPS)
        for span, half in zip(columns, (a, b)):
            result[at, span] = (
                lat_all[y, at, span].astype(F32) + half * scale * vectors[2:3, span]
            ).astype(BF)
        return carry

    lax.fori_loop(0, count // 16, finish, 0)
    arrived_at(lat_all.at[pl.ds(0, 3)], y_sem.at[0])


def mixer(*args):
    dma = pltpu.SemaphoreType.DMA
    vm = pltpu.VMEM
    half = vm((64, HALF), BF)
    in_specs = [ANY] * len(args)
    slices = vm((2, NX, 128, DK_HEAD), BF)
    thin = vm((2, NZ, 16, DK_HEAD), BF)
    return pl.pallas_call(
        mixer_kernel,
        out_shape=shape_of(64, WIDTH),
        in_specs=in_specs,
        out_specs=VM,
        scratch_shapes=[
            vm((32, WIDTH), BF), vm((1, 128), BF), vm((1, 128), BF),
            vm((WIDTH,), BF), vm((WIDTH,), BF), vm((DV_HEAD,), BF),
            vm((2 * RANK, WIDTH), BF), vm((2, RANK, DK_HEAD), BF), vm((2, DK_HEAD), F32),
            vm((8, WIDTH), F32), vm((8, WIDTH), F32), vm((3, 128, 1024), BF), vm((NZ, 8, 128), F32), vm((NZ, 8, 128), F32),
            vm((8, 128), F32), vm((NY * NX, 8, 128), F32), vm((NY, 8, 128), F32),
            vm((NZ, NY, 8, 128), F32), vm((8, WIDTH), F32), vm((288, 128), F32),
            vm((NY, 64, WIDTH), BF), vm((2, 288, HALF), BF), vm((2, HALF, 1536), BF),
            vm((288, 1536), BF), vm((288, 2 * RANK), BF), vm((2, DV_HEAD, HALF), BF),
            vm((NX, 32, 512), BF), vm((NX, 32, 512), BF),
            slices, slices, vm((2, 2, 64, DK_HEAD), BF), vm((2, 2, 64, DK_HEAD), BF),
            vm((8, DK_HEAD), F32), vm((NX, 8, DK_HEAD), F32),
            vm((256, 256), BF), vm((256, DV_HEAD), F32), vm((2, 256, DK_HEAD), BF),
            thin, thin, vm((NZ, 2, 16, DK_HEAD), BF), vm((NZ, 2, 16, DK_HEAD), BF),
            vm((8, DK_HEAD), F32), vm((NZ, 8, DK_HEAD), F32),
            thin, thin, vm((2, NX, 128, DK_HEAD), F32), slices, slices,
            vm((256, DV_HEAD), BF),
            vm((NY, 64, HALF), BF), vm((NY, 64, HALF), BF), vm((4, 64, HALF), BF),
            half, half, half, half,
            dma((4,)), dma((9,)), dma((6,)), dma((1,)), dma((6,)), dma((4,)), dma((4,)),
            dma((2, 3)), dma((12,)), dma((2, 3)), dma((4,)),
        ],
        compiler_params=pltpu.CompilerParams(
            collective_id=0, has_side_effects=True, vmem_limit_bytes=60 * 2**20
        ),
        name="mixer",
    )(*args)


def body(
    latents, cond, cond_ctx, context, w_shift, w_scale, w_gate, gain_pre, gain_post,
    w_query, w_key, w_value, w_outgate, w_down, decay_up, decay_bias, head_gain, w_out,
):
    result = mixer(
        latents[0], context[0], cond, cond_ctx[None], gain_pre, gain_post, head_gain,
        w_shift, w_scale, w_gate, w_query, w_key, w_value, w_outgate, w_out,
        w_down.T, decay_up, decay_bias,
    )
    return result[None]


def solution(mesh):
    finer = Mesh(
        mesh.devices.reshape(8, 4, mesh.shape["tp"], mesh.shape["dp"]), ("sp_0", "sp_1", "tp", "dp")
    )
    in_specs = (
        P("dp", SP_TP, None),
        P("dp", SP),
        P(SP),
        P("dp", SP, None),
        P(SP, "tp"),
        P(SP, "tp"),
        P(SP, "tp"),
        P(),
        P(),
        P("dp", "tp"),
        P("dp", "tp"),
        P("dp", "tp"),
        P("dp", "tp"),
        P(),
        P(None, None, "tp"),
        P(None, "tp"),
        P("tp"),
        P("tp", "dp"),
    )
    out_specs = P("dp", SP_TP, None)
    return jax.shard_map(body, mesh=finer, in_specs=in_specs, out_specs=out_specs, check_vma=False)
```

```python
import jax
import jax.numpy as jnp
from jax import lax
from jax.experimental import pallas as pl
from jax.experimental.pallas import tpu as pltpu
from jax.sharding import Mesh
from jax.sharding import PartitionSpec as P

DK_HEAD = 256
DV_HEAD = 512
RANK = 16
BLOCK = 128
SP_TP = ("sp_0", "sp_1", "tp")
SP = ("sp_0", "sp_1")
NZ, NX, NY = 8, 4, 4
WIDTH = 4096
HALF = 2048
WHOLE = 768
REST = HALF - WHOLE
ANY = pl.BlockSpec(memory_space=pl.ANY)
VM = pl.BlockSpec(memory_space=pltpu.VMEM)
BF, F32 = jnp.bfloat16, jnp.float32


EPS = 1e-06
TAU = 16.0


def matmul(left, right):
    return jnp.dot(left, right, preferred_element_type=jnp.float32)


def rms_scale(vectors, gain):
    return vectors * lax.rsqrt(jnp.mean(vectors * vectors, axis=-1, keepdims=True) + EPS) * gain


def shape_of(*dims, dtype=BF):
    return jax.ShapeDtypeStruct(dims, dtype)


def send(src, dst, send_sem, recv_sem, **where):
    copy = pltpu.make_async_remote_copy(
        src_ref=src,
        dst_ref=dst,
        send_sem=send_sem,
        recv_sem=recv_sem,
        device_id=where,
        device_id_type=pl.DeviceIdType.MESH,
    )
    copy.start()
    return copy


def greet(partners):
    barrier = pltpu.get_barrier_semaphore()
    for where in partners:
        pl.semaphore_signal(
            barrier, inc=1, device_id=where, device_id_type=pl.DeviceIdType.MESH
        )
    return lambda: pl.semaphore_wait(barrier, len(partners))


def position():
    return tuple(lax.axis_index(a) for a in ("sp_0", "sp_1", "tp", "dp"))


def log_sigmoid(v):
    return jnp.minimum(v, 0.0) - jnp.log1p(jnp.exp(-jnp.abs(v)))


def log_decays(lowrank, decay_up, decay_bias):
    return [
        log_sigmoid(
            matmul(lowrank[:, way * RANK : (way + 1) * RANK], decay_up[way])
            + decay_bias[way : way + 1]
        )
        / TAU
        for way in range(2)
    ]


def triangle(n, lower):
    r = lax.broadcasted_iota(jnp.int32, (n, n), 0)
    c = lax.broadcasted_iota(jnp.int32, (n, n), 1)
    return r >= c if lower else r <= c


def running_sums(decay_f, decay_b):
    n = decay_f.shape[0]
    parts = []
    for decay in (decay_f, decay_b):
        high = decay.astype(BF)
        parts += [high, (decay - high.astype(F32)).astype(BF)]
    fwd = matmul(jnp.where(triangle(n, True), 1.0, 0.0).astype(BF), parts[0])
    fwd = fwd + matmul(jnp.where(triangle(n, True), 1.0, 0.0).astype(BF), parts[1])
    bwd = matmul(jnp.where(triangle(n, False), 1.0, 0.0).astype(BF), parts[2])
    bwd = bwd + matmul(jnp.where(triangle(n, False), 1.0, 0.0).astype(BF), parts[3])
    return fwd, bwd


def across(left, right):
    return lax.dot_general(left, right, (((1,), (1,)), ((), ())), preferred_element_type=F32)


def outer(left, right):
    return lax.dot_general(left, right, (((0,), (0,)), ((), ())), preferred_element_type=F32)


def scores_of(q, k, fwd, bwd, store):
    lower, upper = triangle(BLOCK, True), triangle(BLOCK, False)
    bf = lambda a: a.astype(BF)
    for b in range(2):
        sl = slice(b * BLOCK, (b + 1) * BLOCK)
        osl = slice((1 - b) * BLOCK, (2 - b) * BLOCK)
        f, g = fwd[sl], bwd[sl]
        cf, cg = f[BLOCK // 2 : BLOCK // 2 + 1], g[BLOCK // 2 - 1 : BLOCK // 2]
        sf = across(bf(q[sl] * jnp.exp(f - cf)), bf(k[sl] * jnp.exp(cf - f)))
        sb = across(bf(q[sl] * jnp.exp(g - cg)), bf(k[sl] * jnp.exp(cg - g)))
        store[sl, sl] = bf(jnp.where(lower, sf, 0.0) + jnp.where(upper, sb, 0.0))
        if b == 0:
            mine, other, edge = g, bwd[osl], bwd[BLOCK : BLOCK + 1]
        else:
            mine, other, edge = f, fwd[osl], fwd[BLOCK - 1 : BLOCK]
        store[sl, osl] = bf(across(bf(q[sl] * jnp.exp(mine - edge)), bf(k[osl] * jnp.exp(edge - other))))


def arrived_at(ref, sem):
    pltpu.make_async_copy(ref, ref, sem).wait()


def mixer_kernel(
    lat, *inputs_and_rest
):
    (
    context_in, cond_in, cond_ctx_in, gain_pre_in, gain_post_in, head_gain_in, w_shift, w_scale, w_gate,
    wq, wk, wv, wg, wo, w_down_in, decay_up_in, decay_bias_in,
    result,
    context, cond, cond_ctx, gain_pre, gain_post, head_gain, w_down, decay_up, decay_bias,
    factor, offset, w_mod, partial, partials, tile, tiles, column_sum, mods, vectors, norms, lat_all, rows, w_all,
    proj, low, w_out,
    pack, packs, states, got_states, relays, relays_e, decays, got_decays, scores, local, entering,
    group, groups, ctx_group, ctx_groups, group_decays, all_decays,
    back, entry, before, leaving, entries, heads, part_a, part_b, near, sum_a, sum_b, relay_a, relay_c,
    w_far, everyone, relay_h, whole, crossing, crossed,
    s_load, s_small, m_sem, l_send, l_recv, w_sem, c_sem, x_sem, z_sem, e_sem, y_sem, f_sem, h_sem,
    ) = inputs_and_rest
    z, x, y, c = position()
    x_peers = [lax.rem(x + d, NX) for d in (1, 3, 2)]
    z_peers = [lax.rem(z + d, NZ) for d in (4, 3, 5, 2, 6, 1, 7)]
    xy_peers = [
        dict(sp_1=lax.rem(x + k // NY, NX), tp=lax.rem(y + k % NY, NY)) for k in range(1, NX * NY)
    ]
    above, below, facing = (lax.rem(y + k, NY) for k in (1, 3, 2))
    up, down = dict(tp=above), dict(tp=below)
    east, west = lax.rem(x + 1, NX), lax.rem(x + 3, NX)
    opposite = lax.rem(x + 2, NX)
    other = dict(dp=1 - c)
    columns = [pl.ds(pl.multiple_of(k * HALF, HALF), HALF) for k in (c, 1 - c)]
    entered = greet([dict(sp_0=p) for p in z_peers] + xy_peers + [other])
    spans = (slice(0, 256), slice(256, 768), slice(768, 1024), slice(1024, 1536))
    sources = list(zip((wk, wv, wq, wg), spans))
    own_rows = pltpu.make_async_copy(lat, lat_all.at[y], s_load.at[1])
    own_rows.start()
    small = [
        pltpu.make_async_copy(src, dst, s_small.at[k])
        for k, (src, dst) in enumerate(
            [
                (cond_in, cond), (cond_ctx_in, cond_ctx), (context_in, context),
                (gain_pre_in, gain_pre), (gain_post_in, gain_post), (head_gain_in, head_gain),
                (w_down_in, w_down), (decay_up_in, decay_up), (decay_bias_in, decay_bias),
            ]
        )
    ]
    for load in small[:2]:
        load.start()
    for k, w in enumerate((w_shift, w_scale, w_gate)):
        pltpu.make_async_copy(w, w_mod.at[k], s_load.at[0]).start()
    for load in small[2:]:
        load.start()
    for w, span in sources:
        pltpu.make_async_copy(w, w_all.at[0, :, span], s_load.at[2]).start()
    own_out = pltpu.make_async_copy(wo, w_out.at[0], s_load.at[3])
    own_out.start()
    own_rows.wait()
    entered()
    top, bottom = pl.ds(0, 32), pl.ds(32, 32)
    up_1 = send(lat_all.at[y, top], lat_all.at[y, top], l_send.at[0], l_recv.at[0], **up)
    down_1 = send(lat_all.at[y, bottom], lat_all.at[y, bottom], l_send.at[0], l_recv.at[1], **down)
    small[0].wait()
    small[1].wait()
    line = lax.broadcasted_iota(jnp.int32, (16, 128), 0)
    act = jax.nn.silu(cond[...].astype(F32)).astype(BF).astype(F32)
    act_ctx = jax.nn.silu(cond_ctx[...].astype(F32)).astype(BF).astype(F32)
    arrived_at(w_mod, s_load.at[0])
    total = None
    for k in range(3):
        left = jnp.where(line == k, act, jnp.where(line == k + 3, act_ctx, 0.0)).astype(BF)
        part = matmul(left, w_mod[k])
        total = part if total is None else total + part
    for k in range(NZ):
        partial[k] = total[:8, k * 128 : (k + 1) * 128]
    for p in z_peers:
        send(partial.at[p], partials.at[z], m_sem.at[0], m_sem.at[1], sp_0=p)
    partials[z] = partial[z]
    for w, span in sources:
        send(w, w_all.at[1, :, span], w_sem.at[0], w_sem.at[1], **other)
    tail = pl.ds(WHOLE, REST)
    out_weight = send(wo.at[:, tail], w_out.at[1, :, tail], w_sem.at[2], w_sem.at[3], **other)

    def norm_of(source, target, length):
        def step(k, carry):
            v = source[pl.ds(pl.multiple_of(k * 16, 16), 16)].astype(F32)
            square = jnp.sum(v * v, axis=1, keepdims=True)
            norms[pl.ds(pl.multiple_of(target + k * 16, 16), 16)] = jnp.broadcast_to(
                lax.rsqrt(square / WIDTH + EPS), (16, 128)
            )
            return carry

        lax.fori_loop(0, length // 16, step, 0)

    for load in small[2:]:
        load.wait()
    ones = jnp.ones((1, WIDTH), F32)
    zeros = jnp.zeros((1, WIDTH), F32)
    pre = gain_pre[...].reshape(1, WIDTH).astype(F32)
    post = gain_post[...].reshape(1, WIDTH).astype(F32)
    for k, (by, plus) in enumerate(
        ((ones, zeros), (pre, pre), (post, zeros), (ones, zeros), (pre, pre))
    ):
        factor[k : k + 1] = by
        offset[k : k + 1] = plus
    norm_of(context, 0, 32)
    norm_of(lat_all.at[y], 32, 64)
    arrived_at(partials.at[pl.ds(0, NZ - 1)], m_sem.at[1])
    summed = partials[0]
    for k in range(1, NZ):
        summed = summed + partials[k]
    tile[...] = summed
    tiles[y * NX + x] = summed
    for w in xy_peers:
        send(tile, tiles.at[y * NX + x], m_sem.at[2], m_sem.at[3], **w)
    up_2 = send(lat_all.at[y, bottom], lat_all.at[y, bottom], l_send.at[0], l_recv.at[2], **up)
    down_2 = send(lat_all.at[y, top], lat_all.at[y, top], l_send.at[0], l_recv.at[3], **down)
    arrived_at(tiles.at[pl.ds(0, NX * NY - 1)], m_sem.at[3])
    for k in range(NY):
        block = tiles[k * NX] + tiles[k * NX + 1] + tiles[k * NX + 2] + tiles[k * NX + 3]
        column_sum[k] = block
        mods[z, k] = block
    for p in z_peers:
        send(column_sum, mods.at[z], m_sem.at[4], m_sem.at[5], sp_0=p)
    up_1.wait_recv()
    passed = lat_all.at[below, top]
    relay_up = send(passed, passed, l_send.at[0], l_recv.at[4], **up)
    down_1.wait_recv()
    passed = lat_all.at[above, bottom]
    relay_down = send(passed, passed, l_send.at[0], l_recv.at[5], **down)
    own_out.wait()
    whole_at, high, low_half = pl.ds(0, WHOLE), pl.ds(0, 256), pl.ds(256, 256)
    far_up = send(w_out.at[0, high, whole_at], w_far.at[2, high], f_sem.at[0], f_sem.at[1], **up)
    far_down = send(w_out.at[0, low_half, whole_at], w_far.at[0, low_half], f_sem.at[0], f_sem.at[2], **down)
    send(w_out.at[0, low_half, whole_at], w_far.at[2, low_half], f_sem.at[0], f_sem.at[3], **up)
    send(w_out.at[0, high, whole_at], w_far.at[0, high], f_sem.at[0], f_sem.at[4], **down)
    arrived_at(mods.at[pl.ds(0, NZ - 1)], m_sem.at[5])
    for k in range(NY):
        for j in range(NZ):
            at = (k * NZ + j) * 128
            span = slice(at, at + 128)
            vectors[:, span] = mods[j, k] * factor[:, span] + offset[:, span]

    def modulate(source, target, scale_row, shift_row, length, known):
        def step(k, carry):
            at = pl.ds(pl.multiple_of(k * 16, 16), 16)
            to = pl.ds(pl.multiple_of(target + k * 16, 16), 16)
            halves = [source[at, columns[h]].astype(F32) for h in range(2)]
            if known:
                norm = norms[to, 0:1]
            else:
                square = sum(jnp.sum(v * v, axis=1, keepdims=True) for v in halves)
                norm = lax.rsqrt(square / WIDTH + EPS)
            for h in range(2):
                weight = vectors[scale_row : scale_row + 1, columns[h]]
                shift = vectors[shift_row : shift_row + 1, columns[h]]
                rows[h, to] = (halves[h] * norm * weight + shift).astype(BF)
            return carry

        lax.fori_loop(0, length // 16, step, 0)

    def project_rows(at, length, places, chunks):
        def step(k, carry):
            span = pl.ds(pl.multiple_of(k * 256, 256), 256)
            out = matmul(rows[0, at : at + length], w_all[0, :, span])
            out = (out + matmul(rows[1, at : at + length], w_all[1, :, span])).astype(BF)
            for offset, place, count in places:
                to = pl.ds(pl.multiple_of(place, 32), count)
                proj[to, span] = out[offset - at : offset - at + count]
            return carry

        lax.fori_loop(chunks.start, chunks.stop, step, 0)

    def project_down(at, length, places):
        out = across(rows[0, at : at + length], w_down[:, columns[0]])
        out = (out + across(rows[1, at : at + length], w_down[:, columns[1]])).astype(BF)
        for offset, place, count in places:
            low[pl.ds(pl.multiple_of(place, 32), count)] = out[offset - at : offset - at + count]

    modulate(context, 0, 4, 3, 32, True)
    modulate(lat_all.at[y], 32, 1, 0, 64, True)
    up_2.wait_recv()
    modulate(lat_all.at[below], 96, 1, 0, 64, False)
    down_2.wait_recv()
    modulate(lat_all.at[above], 160, 1, 0, 64, False)
    arrived_at(w_all.at[0], s_load.at[2])
    arrived_at(w_all.at[1], w_sem.at[1])
    places = ((32, y * 64, 64), (96, below * 64, 64), (160, above * 64, 64), (224, facing * 64, 64))
    project_rows(0, 224, ((0, 256, 32), *places[:3]), range(0, 3))
    project_down(0, 224, ((0, 256, 32), *places[:3]))
    for j in range(NX):
        pack[j] = jnp.zeros((32, 512), BF)
        pack[j, :, :DK_HEAD] = proj[256:288, 0:256]
        pack[j, :, DK_HEAD : DK_HEAD + 128] = proj[256:288, 256 + j * 128 : 384 + j * 128]
        pack[j, :, DK_HEAD + 128 : DK_HEAD + 128 + 2 * RANK] = low[256:288]
    for p in x_peers:
        send(pack.at[p], packs.at[x], c_sem.at[0], c_sem.at[1], sp_1=p)
    packs[x] = pack[x]
    relay_up.wait_recv()
    relay_down.wait_recv()
    modulate(lat_all.at[facing], 224, 1, 0, 64, False)
    project_rows(224, 64, places[3:], range(0, 3))
    project_down(224, 64, places[3:])
    decay_f, decay_b = log_decays(low[:256], decay_up[...], decay_bias[...])
    fwd, bwd = running_sums(decay_f, decay_b)
    decays[0:1] = fwd[-1:]
    decays[1:2] = bwd[:1]
    decays[2:8] = jnp.zeros((6, DK_HEAD), F32)
    for p in x_peers:
        send(decays, got_decays.at[x], c_sem.at[2], c_sem.at[3], sp_1=p)
    got_decays[x] = decays[...]
    k = proj[:256, :256].astype(F32)
    v = proj[:256, 256:768]
    first, second = pl.ds(0, 64), pl.ds(64, 64)

    def swap(source, target, relay, way, sems):
        far = source.at[way, opposite]
        there = target.at[way, x]
        sent, got = sems.at[way, 0], sems.at[way, 1]
        passed = sems.at[way, 2]
        send(far.at[first], relay.at[way, 0], sent, passed, sp_1=east)
        send(far.at[second], relay.at[way, 1], sent, passed, sp_1=west)
        send(source.at[way, east], there, sent, got, sp_1=east)
        send(source.at[way, west], there, sent, got, sp_1=west)

    def pass_on(target, relay, way, sems):
        arrived_at(relay.at[way], sems.at[way, 2])
        sent, got = sems.at[way, 0], sems.at[way, 1]
        send(relay.at[way, 0], target.at[way, west, first], sent, got, sp_1=east)
        send(relay.at[way, 1], target.at[way, east, second], sent, got, sp_1=west)

    def swapped(target, way, sems):
        arrived_at(target.at[way, pl.ds(0, NX - 1)], sems.at[way, 1])

    def local_state(way, scaled):
        state = outer(v, (k * scaled).astype(BF)).astype(BF)
        for j in range(NX):
            states[way, j] = state[j * 128 : (j + 1) * 128]
        swap(states, got_states, relays, way, x_sem)
        got_states[way, x] = states[way, x]

    local_state(0, jnp.exp(fwd[-1:] - fwd))
    local_state(1, jnp.exp(bwd[:1] - bwd))
    arrived_at(packs.at[pl.ds(0, NX - 1)], c_sem.at[1])
    ctx = packs[...].reshape(NX * 32, 512)
    ctx_k = ctx[:, :DK_HEAD].astype(F32)
    ctx_v = ctx[:, DK_HEAD : DK_HEAD + 128]
    ctx_lr = ctx[:, DK_HEAD + 128 : DK_HEAD + 128 + 2 * RANK]
    cdf, cdb = log_decays(ctx_lr, decay_up[...], decay_bias[...])
    cf, cb = running_sums(cdf, cdb)
    for way, scaled in enumerate((jnp.exp(cf[-1:] - cf), jnp.exp(cb[:1] - cb))):
        state = outer(ctx_v, (ctx_k * scaled).astype(BF)).astype(BF)
        for j in range(NZ):
            ctx_group[j, way] = state[j * 16 : (j + 1) * 16]
    for p in z_peers:
        send(ctx_group.at[p], ctx_groups.at[z], z_sem.at[0], z_sem.at[1], sp_0=p)
    ctx_groups[z] = ctx_group[z]
    project_rows(32, 256, places, range(3, 4))
    pass_on(got_states, relays, 0, x_sem)
    arrived_at(got_decays.at[pl.ds(0, NX - 1)], c_sem.at[3])
    group_decays[0:2] = sum(got_decays[j, 0:2] for j in range(NX))
    group_decays[2:3] = cf[-1:]
    group_decays[3:4] = cb[:1]
    group_decays[4:8] = jnp.zeros((4, DK_HEAD), F32)
    for p in z_peers:
        send(group_decays, all_decays.at[z], z_sem.at[2], z_sem.at[3], sp_0=p)
    all_decays[z] = group_decays[...]
    pass_on(got_states, relays, 1, x_sem)
    q = proj[:256, 768:1024].astype(F32) * DK_HEAD ** (-0.5)
    scores_of(q, k, fwd, bwd, scores)
    ways = (tuple(range(NX)), tuple(reversed(range(NX))))
    orders = (tuple(range(NZ)), tuple(reversed(range(NZ))))
    for way in range(2):
        swapped(got_states, way, x_sem)
        state = None
        for j in ways[way]:
            piece = got_states[way, j].astype(F32)
            state = piece if state is None else state * jnp.exp(got_decays[j, way : way + 1]) + piece
        state = state.astype(BF)
        for j in range(NZ):
            group[way, j] = state[j * 16 : (j + 1) * 16]
        for p in z_peers:
            send(group.at[way, p], groups.at[way, z], z_sem.at[4 + way], z_sem.at[6 + way], sp_0=p)
        groups[way, z] = group[way, z]
    project_rows(32, 256, places, range(4, 6))
    far_up.wait_recv()
    send(w_far.at[2, high], w_far.at[1, high], f_sem.at[0], f_sem.at[5], **up)
    far_down.wait_recv()
    send(w_far.at[0, low_half], w_far.at[1, low_half], f_sem.at[0], f_sem.at[6], **down)
    for way in range(2):
        state = jnp.zeros((128, DK_HEAD), F32)
        for j in ways[way]:
            before[way, j] = state
            state = state * jnp.exp(got_decays[j, way : way + 1]) + got_states[way, j].astype(F32)
    local[...] = matmul(scores[...], v)
    entering[0] = (q * jnp.exp(fwd)).astype(BF)
    entering[1] = (q * jnp.exp(bwd)).astype(BF)
    arrived_at(ctx_groups.at[pl.ds(0, NZ - 1)], z_sem.at[1])
    arrived_at(all_decays.at[pl.ds(0, NZ - 1)], z_sem.at[3])
    starts = []
    for way in range(2):
        state = jnp.zeros((16, DK_HEAD), F32)
        for j in orders[way]:
            state = state * jnp.exp(all_decays[j, 2 + way : 3 + way]) + ctx_groups[j, way].astype(F32)
        starts.append(state)
    for way in range(2):
        arrived_at(groups.at[way, pl.ds(0, NZ - 1)], z_sem.at[6 + way])
        state = starts[way]
        for j in orders[way]:
            back[way, j] = state.astype(BF)
            state = state * jnp.exp(all_decays[j, way : way + 1]) + groups[way, j].astype(F32)
        for p in z_peers:
            send(back.at[way, p], entry.at[way, z], z_sem.at[8 + way], z_sem.at[10 + way], sp_0=p)
        entry[way, z] = back[way, z]
    gate = jax.nn.silu(proj[:256, 1024:1536].astype(F32)) * head_gain[...].reshape(1, DV_HEAD).astype(F32)
    for way in range(2):
        arrived_at(entry.at[way, pl.ds(0, NZ - 1)], z_sem.at[10 + way])
        start = entry[way].reshape(128, DK_HEAD).astype(F32)
        passed = jnp.zeros((1, DK_HEAD), F32)
        for j in ways[way]:
            leaving[way, j] = (start * jnp.exp(passed) + before[way, j]).astype(BF)
            passed = passed + got_decays[j, way : way + 1]
        swap(leaving, entries, relays_e, way, e_sem)
        entries[way, x] = leaving[way, x]
    pass_on(entries, relays_e, 0, e_sem)
    pass_on(entries, relays_e, 1, e_sem)
    out_weight.wait_recv()
    swapped(entries, 0, e_sem)
    out = [
        local[:, j * 128 : (j + 1) * 128] + across(entering[0], entries[0, j]) for j in range(NX)
    ]
    swapped(entries, 1, e_sem)
    out = [o + across(entering[1], entries[1, j]) for j, o in enumerate(out)]
    square = sum(jnp.sum(o * o, axis=1, keepdims=True) for o in out)
    scale = lax.rsqrt(square / DV_HEAD + EPS)
    for j in range(NX):
        heads[:, j * 128 : (j + 1) * 128] = (out[j] * scale * gate[:, j * 128 : (j + 1) * 128]).astype(BF)
    count = 64

    def rows_of(owner, offset=0, length=64):
        return pl.ds(pl.multiple_of(owner * count + offset, length), length)

    mine, half_1, half_2 = pl.ds(0, count), pl.ds(0, 32), pl.ds(32, 32)
    pass_up = send(heads.at[rows_of(facing, 0, 32)], relay_h.at[0], h_sem.at[0], h_sem.at[1], **up)
    pass_down = send(heads.at[rows_of(facing, 32, 32)], relay_h.at[1], h_sem.at[0], h_sem.at[2], **down)
    send(heads.at[rows_of(above)], everyone.at[3, mine], h_sem.at[0], h_sem.at[3], **up)
    send(heads.at[rows_of(below)], everyone.at[1, mine], h_sem.at[0], h_sem.at[4], **down)
    everyone[0, :count] = heads[rows_of(y)]

    def project(owner, part, half):
        part[owner] = matmul(heads[rows_of(owner)], w_out[half, :, WHOLE:]).astype(BF)

    project(facing, part_a, 0)
    first_a = send(part_a.at[facing], relay_a, y_sem.at[4], y_sem.at[1], **down)
    project(facing, part_b, 1)
    first_b = send(part_b.at[facing], relay_c, y_sem.at[4], y_sem.at[2], **up)
    pass_up.wait_recv()
    send(relay_h.at[0], everyone.at[2, half_1], h_sem.at[0], h_sem.at[5], **up)
    pass_down.wait_recv()
    send(relay_h.at[1], everyone.at[2, half_2], h_sem.at[0], h_sem.at[6], **down)
    project(below, part_b, 1)
    send(part_b.at[below], near.at[1], y_sem.at[0], y_sem.at[3], **down)
    project(above, part_a, 0)
    send(part_a.at[above], near.at[0], y_sem.at[0], y_sem.at[3], **up)
    project(below, part_a, 0)
    project(above, part_b, 1)
    first_a.wait_recv()
    sum_a[...] = (relay_a[...].astype(F32) + part_a[below].astype(F32)).astype(BF)
    send(sum_a, near.at[2], y_sem.at[0], y_sem.at[3], **down)
    first_b.wait_recv()
    sum_b[...] = (relay_c[...].astype(F32) + part_b[above].astype(F32)).astype(BF)
    send(sum_b, near.at[3], y_sem.at[0], y_sem.at[3], **up)
    arrived_at(everyone.at[3, mine], h_sem.at[3])
    arrived_at(everyone.at[1, mine], h_sem.at[4])
    arrived_at(everyone.at[2, half_1], h_sem.at[5])
    arrived_at(everyone.at[2, half_2], h_sem.at[6])
    theirs = pl.ds(count, count)
    over = send(everyone.at[:, mine], everyone.at[:, theirs], h_sem.at[7], h_sem.at[8], **other)
    project(y, part_a, 0)
    project(y, part_b, 1)
    arrived_at(w_far.at[2, high], f_sem.at[3])
    arrived_at(w_far.at[0, high], f_sem.at[4])
    arrived_at(w_far.at[1, high], f_sem.at[5])
    arrived_at(w_far.at[1, high], f_sem.at[6])
    over.wait()
    sums = matmul(everyone[0], w_out[0, :, :WHOLE])
    for d in range(1, NY):
        sums = sums + matmul(everyone[d], w_far[d - 1])
    whole[...] = sums[:count]
    crossing[...] = sums[count:]
    cross = send(crossing, crossed, h_sem.at[9], h_sem.at[10], **other)
    arrived_at(partials.at[pl.ds(0, NZ - 1)], m_sem.at[0])
    arrived_at(tiles.at[pl.ds(0, NX * NY - 1)], m_sem.at[2])
    arrived_at(mods.at[pl.ds(0, NZ - 1)], m_sem.at[4])
    arrived_at(lat_all.at[pl.ds(0, 3)], l_send.at[0])
    arrived_at(w_all.at[1], w_sem.at[0])
    out_weight.wait_send()
    arrived_at(packs.at[pl.ds(0, NX - 1)], c_sem.at[0])
    arrived_at(got_decays.at[pl.ds(0, NX - 1)], c_sem.at[2])
    arrived_at(ctx_groups.at[pl.ds(0, NZ - 1)], z_sem.at[0])
    arrived_at(all_decays.at[pl.ds(0, NZ - 1)], z_sem.at[2])
    for way in range(2):
        arrived_at(states.at[way], x_sem.at[way, 0])
        arrived_at(leaving.at[way], e_sem.at[way, 0])
        arrived_at(groups.at[way, pl.ds(0, NZ - 1)], z_sem.at[4 + way])
        arrived_at(entry.at[way, pl.ds(0, NZ - 1)], z_sem.at[8 + way])
    arrived_at(heads.at[pl.ds(0, 256)], h_sem.at[0])
    arrived_at(w_far, f_sem.at[0])
    cross.wait()
    arrived_at(near, y_sem.at[3])

    def finish(k, carry):
        at = pl.ds(pl.multiple_of(k * 16, 16), 16)
        a = part_a[y, at].astype(F32) + near[0, at].astype(F32) + near[2, at].astype(F32)
        b = part_b[y, at].astype(F32) + near[1, at].astype(F32) + near[3, at].astype(F32)
        pieces = ((whole[at], c, 0), (a, c, WHOLE), (crossed[at], 1 - c, 0), (b, 1 - c, WHOLE))
        square = sum(jnp.sum(v * v, axis=1, keepdims=True) for v, _, _ in pieces)
        scale = lax.rsqrt(square / WIDTH + EPS)
        for v, half, start in pieces:
            span = pl.ds(pl.multiple_of(half * HALF + start, 128), v.shape[1])
            result[at, span] = (
                lat_all[y, at, span].astype(F32) + v * scale * vectors[2:3, span]
            ).astype(BF)
        return carry

    lax.fori_loop(0, count // 16, finish, 0)
    arrived_at(near, y_sem.at[0])
    arrived_at(near.at[pl.ds(0, 2)], y_sem.at[4])


def mixer(*args):
    dma = pltpu.SemaphoreType.DMA
    vm = pltpu.VMEM
    half = vm((64, REST), BF)
    in_specs = [ANY] * len(args)
    slices = vm((2, NX, 128, DK_HEAD), BF)
    thin = vm((2, NZ, 16, DK_HEAD), BF)
    return pl.pallas_call(
        mixer_kernel,
        out_shape=shape_of(64, WIDTH),
        in_specs=in_specs,
        out_specs=VM,
        scratch_shapes=[
            vm((32, WIDTH), BF), vm((1, 128), BF), vm((1, 128), BF),
            vm((WIDTH,), BF), vm((WIDTH,), BF), vm((DV_HEAD,), BF),
            vm((2 * RANK, WIDTH), BF), vm((2, RANK, DK_HEAD), BF), vm((2, DK_HEAD), F32),
            vm((8, WIDTH), F32), vm((8, WIDTH), F32), vm((3, 128, 1024), BF), vm((NZ, 8, 128), F32), vm((NZ, 8, 128), F32),
            vm((8, 128), F32), vm((NY * NX, 8, 128), F32), vm((NY, 8, 128), F32),
            vm((NZ, NY, 8, 128), F32), vm((8, WIDTH), F32), vm((288, 128), F32),
            vm((NY, 64, WIDTH), BF), vm((2, 288, HALF), BF), vm((2, HALF, 1536), BF),
            vm((288, 1536), BF), vm((288, 2 * RANK), BF), vm((2, DV_HEAD, HALF), BF),
            vm((NX, 32, 512), BF), vm((NX, 32, 512), BF),
            slices, slices, vm((2, 2, 64, DK_HEAD), BF), vm((2, 2, 64, DK_HEAD), BF),
            vm((8, DK_HEAD), F32), vm((NX, 8, DK_HEAD), F32),
            vm((256, 256), BF), vm((256, DV_HEAD), F32), vm((2, 256, DK_HEAD), BF),
            thin, thin, vm((NZ, 2, 16, DK_HEAD), BF), vm((NZ, 2, 16, DK_HEAD), BF),
            vm((8, DK_HEAD), F32), vm((NZ, 8, DK_HEAD), F32),
            thin, thin, vm((2, NX, 128, DK_HEAD), F32), slices, slices,
            vm((256, DV_HEAD), BF),
            vm((NY, 64, REST), BF), vm((NY, 64, REST), BF), vm((4, 64, REST), BF),
            half, half, half, half,
            vm((3, DV_HEAD, WHOLE), BF), vm((NY, 128, DV_HEAD), BF), vm((2, 32, DV_HEAD), BF),
            vm((64, WHOLE), F32), vm((64, WHOLE), F32), vm((64, WHOLE), F32),
            dma((4,)), dma((9,)), dma((6,)), dma((1,)), dma((6,)), dma((4,)), dma((4,)),
            dma((2, 3)), dma((12,)), dma((2, 3)), dma((5,)), dma((7,)), dma((11,)),
        ],
        compiler_params=pltpu.CompilerParams(
            collective_id=0, has_side_effects=True, vmem_limit_bytes=60 * 2**20
        ),
        name="mixer",
    )(*args)


def body(
    latents, cond, cond_ctx, context, w_shift, w_scale, w_gate, gain_pre, gain_post,
    w_query, w_key, w_value, w_outgate, w_down, decay_up, decay_bias, head_gain, w_out,
):
    result = mixer(
        latents[0], context[0], cond, cond_ctx[None], gain_pre, gain_post, head_gain,
        w_shift, w_scale, w_gate, w_query, w_key, w_value, w_outgate, w_out,
        w_down.T, decay_up, decay_bias,
    )
    return result[None]


def solution(mesh):
    finer = Mesh(
        mesh.devices.reshape(8, 4, mesh.shape["tp"], mesh.shape["dp"]), ("sp_0", "sp_1", "tp", "dp")
    )
    in_specs = (
        P("dp", SP_TP, None),
        P("dp", SP),
        P(SP),
        P("dp", SP, None),
        P(SP, "tp"),
        P(SP, "tp"),
        P(SP, "tp"),
        P(),
        P(),
        P("dp", "tp"),
        P("dp", "tp"),
        P("dp", "tp"),
        P("dp", "tp"),
        P(),
        P(None, None, "tp"),
        P(None, "tp"),
        P("tp"),
        P("tp", "dp"),
    )
    out_specs = P("dp", SP_TP, None)
    return jax.shard_map(body, mesh=finer, in_specs=in_specs, out_specs=out_specs, check_vma=False)
```

```python
import jax
import jax.numpy as jnp
from jax import lax
from jax.experimental import pallas as pl
from jax.experimental.pallas import tpu as pltpu
from jax.sharding import Mesh
from jax.sharding import PartitionSpec as P

DK_HEAD = 256
DV_HEAD = 512
RANK = 16
BLOCK = 128
SP_TP = ("sp_0", "sp_1", "tp")
SP = ("sp_0", "sp_1")
NZ, NX, NY = 8, 4, 4
WIDTH = 4096
HALF = 2048
WHOLE = 640
REST = HALF - WHOLE
ANY = pl.BlockSpec(memory_space=pl.ANY)
VM = pl.BlockSpec(memory_space=pltpu.VMEM)
BF, F32 = jnp.bfloat16, jnp.float32


EPS = 1e-06
TAU = 16.0


def matmul(left, right):
    return jnp.dot(left, right, preferred_element_type=jnp.float32)


def rms_scale(vectors, gain):
    return vectors * lax.rsqrt(jnp.mean(vectors * vectors, axis=-1, keepdims=True) + EPS) * gain


def shape_of(*dims, dtype=BF):
    return jax.ShapeDtypeStruct(dims, dtype)


def send(src, dst, send_sem, recv_sem, **where):
    copy = pltpu.make_async_remote_copy(
        src_ref=src,
        dst_ref=dst,
        send_sem=send_sem,
        recv_sem=recv_sem,
        device_id=where,
        device_id_type=pl.DeviceIdType.MESH,
    )
    copy.start()
    return copy


def greet(partners):
    barrier = pltpu.get_barrier_semaphore()
    for where in partners:
        pl.semaphore_signal(
            barrier, inc=1, device_id=where, device_id_type=pl.DeviceIdType.MESH
        )
    return lambda: pl.semaphore_wait(barrier, len(partners))


def position():
    return tuple(lax.axis_index(a) for a in ("sp_0", "sp_1", "tp", "dp"))


def log_sigmoid(v):
    return jnp.minimum(v, 0.0) - jnp.log1p(jnp.exp(-jnp.abs(v)))


def log_decays(lowrank, decay_up, decay_bias):
    return [
        log_sigmoid(
            matmul(lowrank[:, way * RANK : (way + 1) * RANK], decay_up[way])
            + decay_bias[way : way + 1]
        )
        / TAU
        for way in range(2)
    ]


def triangle(n, lower):
    r = lax.broadcasted_iota(jnp.int32, (n, n), 0)
    c = lax.broadcasted_iota(jnp.int32, (n, n), 1)
    return r >= c if lower else r <= c


def running_sums(decay_f, decay_b):
    n = decay_f.shape[0]
    parts = []
    for decay in (decay_f, decay_b):
        high = decay.astype(BF)
        parts += [high, (decay - high.astype(F32)).astype(BF)]
    fwd = matmul(jnp.where(triangle(n, True), 1.0, 0.0).astype(BF), parts[0])
    fwd = fwd + matmul(jnp.where(triangle(n, True), 1.0, 0.0).astype(BF), parts[1])
    bwd = matmul(jnp.where(triangle(n, False), 1.0, 0.0).astype(BF), parts[2])
    bwd = bwd + matmul(jnp.where(triangle(n, False), 1.0, 0.0).astype(BF), parts[3])
    return fwd, bwd


def across(left, right):
    return lax.dot_general(left, right, (((1,), (1,)), ((), ())), preferred_element_type=F32)


def outer(left, right):
    return lax.dot_general(left, right, (((0,), (0,)), ((), ())), preferred_element_type=F32)


def scores_of(q, k, fwd, bwd, store):
    lower, upper = triangle(BLOCK, True), triangle(BLOCK, False)
    bf = lambda a: a.astype(BF)
    for b in range(2):
        sl = slice(b * BLOCK, (b + 1) * BLOCK)
        osl = slice((1 - b) * BLOCK, (2 - b) * BLOCK)
        f, g = fwd[sl], bwd[sl]
        cf, cg = f[BLOCK // 2 : BLOCK // 2 + 1], g[BLOCK // 2 - 1 : BLOCK // 2]
        sf = across(bf(q[sl] * jnp.exp(f - cf)), bf(k[sl] * jnp.exp(cf - f)))
        sb = across(bf(q[sl] * jnp.exp(g - cg)), bf(k[sl] * jnp.exp(cg - g)))
        store[sl, sl] = bf(jnp.where(lower, sf, 0.0) + jnp.where(upper, sb, 0.0))
        if b == 0:
            mine, other, edge = g, bwd[osl], bwd[BLOCK : BLOCK + 1]
        else:
            mine, other, edge = f, fwd[osl], fwd[BLOCK - 1 : BLOCK]
        store[sl, osl] = bf(across(bf(q[sl] * jnp.exp(mine - edge)), bf(k[osl] * jnp.exp(edge - other))))


def arrived_at(ref, sem):
    pltpu.make_async_copy(ref, ref, sem).wait()


def mixer_kernel(
    lat, *inputs_and_rest
):
    (
    context_in, cond_in, cond_ctx_in, gain_pre_in, gain_post_in, head_gain_in, w_shift, w_scale, w_gate,
    wq, wk, wv, wg, wo, w_down_in, decay_up_in, decay_bias_in,
    result,
    context, cond, cond_ctx, gain_pre, gain_post, head_gain, w_down, decay_up, decay_bias,
    factor, offset, w_mod, partial, partials, tile, tiles, column_sum, mods, vectors, norms, lat_all, rows, w_all,
    proj, low, w_out,
    pack, packs, states, got_states, decays, got_decays, scores, local, entering,
    group, groups, ctx_group, ctx_groups, group_decays, all_decays,
    back, entry, before, leaving, entries, heads, part_a, part_b, near, sum_a, sum_b, relay_a, relay_c,
    w_far, everyone, whole, crossing, crossed,
    s_load, s_small, m_sem, l_send, l_recv, w_sem, c_sem, x_sem, z_sem, e_sem, y_sem, f_sem, h_sem,
    ) = inputs_and_rest
    z, x, y, c = position()
    x_peers = [lax.rem(x + d, NX) for d in (1, 3, 2)]
    z_peers = [lax.rem(z + d, NZ) for d in (4, 3, 5, 2, 6, 1, 7)]
    xy_peers = [
        dict(sp_1=lax.rem(x + k // NY, NX), tp=lax.rem(y + k % NY, NY)) for k in range(1, NX * NY)
    ]
    above, below, facing = (lax.rem(y + k, NY) for k in (1, 3, 2))
    up, down = dict(tp=above), dict(tp=below)
    east, west = lax.rem(x + 1, NX), lax.rem(x + 3, NX)
    opposite = lax.rem(x + 2, NX)
    other = dict(dp=1 - c)
    columns = [pl.ds(pl.multiple_of(k * HALF, HALF), HALF) for k in (c, 1 - c)]
    entered = greet([dict(sp_0=p) for p in z_peers] + xy_peers + [other])
    spans = (slice(0, 256), slice(256, 768), slice(768, 1024), slice(1024, 1536))
    sources = list(zip((wk, wv, wq, wg), spans))
    own_rows = pltpu.make_async_copy(lat, lat_all.at[y], s_load.at[1])
    own_rows.start()
    small = [
        pltpu.make_async_copy(src, dst, s_small.at[k])
        for k, (src, dst) in enumerate(
            [
                (cond_in, cond), (cond_ctx_in, cond_ctx), (context_in, context),
                (gain_pre_in, gain_pre), (gain_post_in, gain_post), (head_gain_in, head_gain),
                (w_down_in, w_down), (decay_up_in, decay_up), (decay_bias_in, decay_bias),
            ]
        )
    ]
    for load in small[:2]:
        load.start()
    for k, w in enumerate((w_shift, w_scale, w_gate)):
        pltpu.make_async_copy(w, w_mod.at[k], s_load.at[0]).start()
    for load in small[2:]:
        load.start()
    for w, span in sources:
        pltpu.make_async_copy(w, w_all.at[0, :, span], s_load.at[2]).start()
    own_out = pltpu.make_async_copy(wo, w_out.at[0], s_load.at[3])
    own_out.start()
    own_rows.wait()
    entered()
    top, bottom = pl.ds(0, 32), pl.ds(32, 32)
    up_1 = send(lat_all.at[y, top], lat_all.at[y, top], l_send.at[0], l_recv.at[0], **up)
    down_1 = send(lat_all.at[y, bottom], lat_all.at[y, bottom], l_send.at[0], l_recv.at[1], **down)
    small[0].wait()
    small[1].wait()
    line = lax.broadcasted_iota(jnp.int32, (16, 128), 0)
    act = jax.nn.silu(cond[...].astype(F32)).astype(BF).astype(F32)
    act_ctx = jax.nn.silu(cond_ctx[...].astype(F32)).astype(BF).astype(F32)
    arrived_at(w_mod, s_load.at[0])
    total = None
    for k in range(3):
        left = jnp.where(line == k, act, jnp.where(line == k + 3, act_ctx, 0.0)).astype(BF)
        part = matmul(left, w_mod[k])
        total = part if total is None else total + part
    for k in range(NZ):
        partial[k] = total[:8, k * 128 : (k + 1) * 128]
    for p in z_peers:
        send(partial.at[p], partials.at[z], m_sem.at[0], m_sem.at[1], sp_0=p)
    partials[z] = partial[z]
    for w, span in sources:
        send(w, w_all.at[1, :, span], w_sem.at[0], w_sem.at[1], **other)
    tail = pl.ds(WHOLE, REST)
    out_weight = send(wo.at[:, tail], w_out.at[1, :, tail], w_sem.at[2], w_sem.at[3], **other)

    def norm_of(source, target, length):
        def step(k, carry):
            v = source[pl.ds(pl.multiple_of(k * 16, 16), 16)].astype(F32)
            square = jnp.sum(v * v, axis=1, keepdims=True)
            norms[pl.ds(pl.multiple_of(target + k * 16, 16), 16)] = jnp.broadcast_to(
                lax.rsqrt(square / WIDTH + EPS), (16, 128)
            )
            return carry

        lax.fori_loop(0, length // 16, step, 0)

    for load in small[2:]:
        load.wait()
    ones = jnp.ones((1, WIDTH), F32)
    zeros = jnp.zeros((1, WIDTH), F32)
    pre = gain_pre[...].reshape(1, WIDTH).astype(F32)
    post = gain_post[...].reshape(1, WIDTH).astype(F32)
    for k, (by, plus) in enumerate(
        ((ones, zeros), (pre, pre), (post, zeros), (ones, zeros), (pre, pre))
    ):
        factor[k : k + 1] = by
        offset[k : k + 1] = plus
    norm_of(context, 0, 32)
    norm_of(lat_all.at[y], 32, 64)
    arrived_at(partials.at[pl.ds(0, NZ - 1)], m_sem.at[1])
    summed = partials[0]
    for k in range(1, NZ):
        summed = summed + partials[k]
    tile[...] = summed
    tiles[y * NX + x] = summed
    for w in xy_peers:
        send(tile, tiles.at[y * NX + x], m_sem.at[2], m_sem.at[3], **w)
    up_2 = send(lat_all.at[y, bottom], lat_all.at[y, bottom], l_send.at[0], l_recv.at[2], **up)
    down_2 = send(lat_all.at[y, top], lat_all.at[y, top], l_send.at[0], l_recv.at[3], **down)
    arrived_at(tiles.at[pl.ds(0, NX * NY - 1)], m_sem.at[3])
    for k in range(NY):
        block = tiles[k * NX] + tiles[k * NX + 1] + tiles[k * NX + 2] + tiles[k * NX + 3]
        column_sum[k] = block
        mods[z, k] = block
    for p in z_peers:
        send(column_sum, mods.at[z], m_sem.at[4], m_sem.at[5], sp_0=p)
    up_1.wait_recv()
    passed = lat_all.at[below, top]
    relay_up = send(passed, passed, l_send.at[0], l_recv.at[4], **up)
    down_1.wait_recv()
    passed = lat_all.at[above, bottom]
    relay_down = send(passed, passed, l_send.at[0], l_recv.at[5], **down)
    own_out.wait()
    whole_at, high, low_half = pl.ds(0, WHOLE), pl.ds(0, 256), pl.ds(256, 256)
    far_up = send(w_out.at[0, high, whole_at], w_far.at[2, high], f_sem.at[0], f_sem.at[1], **up)
    far_down = send(w_out.at[0, low_half, whole_at], w_far.at[0, low_half], f_sem.at[0], f_sem.at[2], **down)
    send(w_out.at[0, low_half, whole_at], w_far.at[2, low_half], f_sem.at[0], f_sem.at[3], **up)
    send(w_out.at[0, high, whole_at], w_far.at[0, high], f_sem.at[0], f_sem.at[4], **down)
    arrived_at(mods.at[pl.ds(0, NZ - 1)], m_sem.at[5])
    for k in range(NY):
        for j in range(NZ):
            at = (k * NZ + j) * 128
            span = slice(at, at + 128)
            vectors[:, span] = mods[j, k] * factor[:, span] + offset[:, span]

    def modulate(source, target, scale_row, shift_row, length, known):
        def step(k, carry):
            at = pl.ds(pl.multiple_of(k * 16, 16), 16)
            to = pl.ds(pl.multiple_of(target + k * 16, 16), 16)
            halves = [source[at, columns[h]].astype(F32) for h in range(2)]
            if known:
                norm = norms[to, 0:1]
            else:
                square = sum(jnp.sum(v * v, axis=1, keepdims=True) for v in halves)
                norm = lax.rsqrt(square / WIDTH + EPS)
            for h in range(2):
                weight = vectors[scale_row : scale_row + 1, columns[h]]
                shift = vectors[shift_row : shift_row + 1, columns[h]]
                rows[h, to] = (halves[h] * norm * weight + shift).astype(BF)
            return carry

        lax.fori_loop(0, length // 16, step, 0)

    def project_rows(at, length, places, chunks):
        def step(k, carry):
            span = pl.ds(pl.multiple_of(k * 256, 256), 256)
            out = matmul(rows[0, at : at + length], w_all[0, :, span])
            out = (out + matmul(rows[1, at : at + length], w_all[1, :, span])).astype(BF)
            for offset, place, count in places:
                to = pl.ds(pl.multiple_of(place, 32), count)
                proj[to, span] = out[offset - at : offset - at + count]
            return carry

        lax.fori_loop(chunks.start, chunks.stop, step, 0)

    def project_down(at, length, places):
        out = across(rows[0, at : at + length], w_down[:, columns[0]])
        out = (out + across(rows[1, at : at + length], w_down[:, columns[1]])).astype(BF)
        for offset, place, count in places:
            low[pl.ds(pl.multiple_of(place, 32), count)] = out[offset - at : offset - at + count]

    modulate(context, 0, 4, 3, 32, True)
    modulate(lat_all.at[y], 32, 1, 0, 64, True)
    up_2.wait_recv()
    modulate(lat_all.at[below], 96, 1, 0, 64, False)
    down_2.wait_recv()
    modulate(lat_all.at[above], 160, 1, 0, 64, False)
    arrived_at(w_all.at[0], s_load.at[2])
    arrived_at(w_all.at[1], w_sem.at[1])
    places = ((32, y * 64, 64), (96, below * 64, 64), (160, above * 64, 64), (224, facing * 64, 64))
    project_rows(0, 224, ((0, 256, 32), *places[:3]), range(0, 3))
    project_down(0, 224, ((0, 256, 32), *places[:3]))
    for j in range(NX):
        pack[j] = jnp.zeros((32, 512), BF)
        pack[j, :, :DK_HEAD] = proj[256:288, 0:256]
        pack[j, :, DK_HEAD : DK_HEAD + 128] = proj[256:288, 256 + j * 128 : 384 + j * 128]
        pack[j, :, DK_HEAD + 128 : DK_HEAD + 128 + 2 * RANK] = low[256:288]
    for p in x_peers:
        send(pack.at[p], packs.at[x], c_sem.at[0], c_sem.at[1], sp_1=p)
    packs[x] = pack[x]
    relay_up.wait_recv()
    relay_down.wait_recv()
    modulate(lat_all.at[facing], 224, 1, 0, 64, False)
    project_rows(224, 64, places[3:], range(0, 3))
    project_down(224, 64, places[3:])
    decay_f, decay_b = log_decays(low[:256], decay_up[...], decay_bias[...])
    fwd, bwd = running_sums(decay_f, decay_b)
    decays[0:1] = fwd[-1:]
    decays[1:2] = bwd[:1]
    decays[2:8] = jnp.zeros((6, DK_HEAD), F32)
    for p in x_peers:
        send(decays, got_decays.at[x], c_sem.at[2], c_sem.at[3], sp_1=p)
    got_decays[x] = decays[...]
    k = proj[:256, :256].astype(F32)
    v = proj[:256, 256:768]

    def swap(source, target, way, sems):
        for p in (opposite, east, west):
            send(source.at[way, p], target.at[way, x], sems.at[way, 0], sems.at[way, 1], sp_1=p)

    def swapped(target, way, sems):
        arrived_at(target.at[way, pl.ds(0, NX - 1)], sems.at[way, 1])

    def local_state(way, scaled):
        state = outer(v, (k * scaled).astype(BF)).astype(BF)
        for j in range(NX):
            states[way, j] = state[j * 128 : (j + 1) * 128]
        swap(states, got_states, way, x_sem)
        got_states[way, x] = states[way, x]

    local_state(0, jnp.exp(fwd[-1:] - fwd))
    local_state(1, jnp.exp(bwd[:1] - bwd))
    arrived_at(packs.at[pl.ds(0, NX - 1)], c_sem.at[1])
    ctx = packs[...].reshape(NX * 32, 512)
    ctx_k = ctx[:, :DK_HEAD].astype(F32)
    ctx_v = ctx[:, DK_HEAD : DK_HEAD + 128]
    ctx_lr = ctx[:, DK_HEAD + 128 : DK_HEAD + 128 + 2 * RANK]
    cdf, cdb = log_decays(ctx_lr, decay_up[...], decay_bias[...])
    cf, cb = running_sums(cdf, cdb)
    for way, scaled in enumerate((jnp.exp(cf[-1:] - cf), jnp.exp(cb[:1] - cb))):
        state = outer(ctx_v, (ctx_k * scaled).astype(BF)).astype(BF)
        for j in range(NZ):
            ctx_group[j, way] = state[j * 16 : (j + 1) * 16]
    for p in z_peers:
        send(ctx_group.at[p], ctx_groups.at[z], z_sem.at[0], z_sem.at[1], sp_0=p)
    ctx_groups[z] = ctx_group[z]
    project_rows(32, 256, places, range(3, 4))
    arrived_at(got_decays.at[pl.ds(0, NX - 1)], c_sem.at[3])
    group_decays[0:2] = sum(got_decays[j, 0:2] for j in range(NX))
    group_decays[2:3] = cf[-1:]
    group_decays[3:4] = cb[:1]
    group_decays[4:8] = jnp.zeros((4, DK_HEAD), F32)
    for p in z_peers:
        send(group_decays, all_decays.at[z], z_sem.at[2], z_sem.at[3], sp_0=p)
    all_decays[z] = group_decays[...]
    q = proj[:256, 768:1024].astype(F32) * DK_HEAD ** (-0.5)
    scores_of(q, k, fwd, bwd, scores)
    ways = (tuple(range(NX)), tuple(reversed(range(NX))))
    orders = (tuple(range(NZ)), tuple(reversed(range(NZ))))
    for way in range(2):
        swapped(got_states, way, x_sem)
        state = None
        for j in ways[way]:
            piece = got_states[way, j].astype(F32)
            state = piece if state is None else state * jnp.exp(got_decays[j, way : way + 1]) + piece
        state = state.astype(BF)
        for j in range(NZ):
            group[way, j] = state[j * 16 : (j + 1) * 16]
        for p in z_peers:
            send(group.at[way, p], groups.at[way, z], z_sem.at[4 + way], z_sem.at[6 + way], sp_0=p)
        groups[way, z] = group[way, z]
    project_rows(32, 256, places, range(4, 6))
    far_up.wait_recv()
    send(w_far.at[2, high], w_far.at[1, high], f_sem.at[0], f_sem.at[5], **up)
    far_down.wait_recv()
    send(w_far.at[0, low_half], w_far.at[1, low_half], f_sem.at[0], f_sem.at[6], **down)
    for way in range(2):
        state = jnp.zeros((128, DK_HEAD), F32)
        for j in ways[way]:
            before[way, j] = state
            state = state * jnp.exp(got_decays[j, way : way + 1]) + got_states[way, j].astype(F32)
    local[...] = matmul(scores[...], v)
    entering[0] = (q * jnp.exp(fwd)).astype(BF)
    entering[1] = (q * jnp.exp(bwd)).astype(BF)
    arrived_at(ctx_groups.at[pl.ds(0, NZ - 1)], z_sem.at[1])
    arrived_at(all_decays.at[pl.ds(0, NZ - 1)], z_sem.at[3])
    starts = []
    for way in range(2):
        state = jnp.zeros((16, DK_HEAD), F32)
        for j in orders[way]:
            state = state * jnp.exp(all_decays[j, 2 + way : 3 + way]) + ctx_groups[j, way].astype(F32)
        starts.append(state)
    for way in range(2):
        arrived_at(groups.at[way, pl.ds(0, NZ - 1)], z_sem.at[6 + way])
        state = starts[way]
        for j in orders[way]:
            back[way, j] = state.astype(BF)
            state = state * jnp.exp(all_decays[j, way : way + 1]) + groups[way, j].astype(F32)
        for p in z_peers:
            send(back.at[way, p], entry.at[way, z], z_sem.at[8 + way], z_sem.at[10 + way], sp_0=p)
        entry[way, z] = back[way, z]
    gate = jax.nn.silu(proj[:256, 1024:1536].astype(F32)) * head_gain[...].reshape(1, DV_HEAD).astype(F32)
    for way in range(2):
        arrived_at(entry.at[way, pl.ds(0, NZ - 1)], z_sem.at[10 + way])
        start = entry[way].reshape(128, DK_HEAD).astype(F32)
        passed = jnp.zeros((1, DK_HEAD), F32)
        for j in ways[way]:
            leaving[way, j] = (start * jnp.exp(passed) + before[way, j]).astype(BF)
            passed = passed + got_decays[j, way : way + 1]
        swap(leaving, entries, way, e_sem)
        entries[way, x] = leaving[way, x]
    out_weight.wait_recv()
    swapped(entries, 0, e_sem)
    out = [
        local[:, j * 128 : (j + 1) * 128] + across(entering[0], entries[0, j]) for j in range(NX)
    ]
    swapped(entries, 1, e_sem)
    out = [o + across(entering[1], entries[1, j]) for j, o in enumerate(out)]
    square = sum(jnp.sum(o * o, axis=1, keepdims=True) for o in out)
    scale = lax.rsqrt(square / DV_HEAD + EPS)
    for j in range(NX):
        heads[:, j * 128 : (j + 1) * 128] = (out[j] * scale * gate[:, j * 128 : (j + 1) * 128]).astype(BF)
    count = 64

    def rows_of(owner):
        return pl.ds(pl.multiple_of(owner * count, count), count)

    mine = pl.ds(0, count)
    send(heads.at[rows_of(facing)], everyone.at[2, mine], h_sem.at[0], h_sem.at[1], tp=facing)
    send(heads.at[rows_of(above)], everyone.at[3, mine], h_sem.at[0], h_sem.at[1], **up)
    send(heads.at[rows_of(below)], everyone.at[1, mine], h_sem.at[0], h_sem.at[1], **down)
    everyone[0, :count] = heads[rows_of(y)]

    def project(owner, part, half):
        part[owner] = matmul(heads[rows_of(owner)], w_out[half, :, WHOLE:]).astype(BF)

    project(facing, part_a, 0)
    first_a = send(part_a.at[facing], relay_a, y_sem.at[4], y_sem.at[1], **down)
    project(facing, part_b, 1)
    first_b = send(part_b.at[facing], relay_c, y_sem.at[4], y_sem.at[2], **up)
    project(below, part_b, 1)
    send(part_b.at[below], near.at[1], y_sem.at[0], y_sem.at[3], **down)
    project(above, part_a, 0)
    send(part_a.at[above], near.at[0], y_sem.at[0], y_sem.at[3], **up)
    project(below, part_a, 0)
    project(above, part_b, 1)
    arrived_at(everyone.at[pl.ds(1, 3), mine], h_sem.at[1])
    theirs = pl.ds(count, count)
    over = send(everyone.at[:, mine], everyone.at[:, theirs], h_sem.at[2], h_sem.at[3], **other)
    project(y, part_a, 0)
    project(y, part_b, 1)
    first_a.wait_recv()
    sum_a[...] = (relay_a[...].astype(F32) + part_a[below].astype(F32)).astype(BF)
    send(sum_a, near.at[2], y_sem.at[0], y_sem.at[3], **down)
    first_b.wait_recv()
    sum_b[...] = (relay_c[...].astype(F32) + part_b[above].astype(F32)).astype(BF)
    send(sum_b, near.at[3], y_sem.at[0], y_sem.at[3], **up)
    arrived_at(w_far.at[2, high], f_sem.at[3])
    arrived_at(w_far.at[0, high], f_sem.at[4])
    arrived_at(w_far.at[1, high], f_sem.at[5])
    arrived_at(w_far.at[1, high], f_sem.at[6])
    over.wait()
    sums = matmul(everyone[0], w_out[0, :, :WHOLE])
    for d in range(1, NY):
        sums = sums + matmul(everyone[d], w_far[d - 1])
    whole[...] = sums[:count]
    crossing[...] = sums[count:]
    cross = send(crossing, crossed, h_sem.at[4], h_sem.at[5], **other)
    arrived_at(partials.at[pl.ds(0, NZ - 1)], m_sem.at[0])
    arrived_at(tiles.at[pl.ds(0, NX * NY - 1)], m_sem.at[2])
    arrived_at(mods.at[pl.ds(0, NZ - 1)], m_sem.at[4])
    arrived_at(lat_all.at[pl.ds(0, 3)], l_send.at[0])
    arrived_at(w_all.at[1], w_sem.at[0])
    out_weight.wait_send()
    arrived_at(packs.at[pl.ds(0, NX - 1)], c_sem.at[0])
    arrived_at(got_decays.at[pl.ds(0, NX - 1)], c_sem.at[2])
    arrived_at(ctx_groups.at[pl.ds(0, NZ - 1)], z_sem.at[0])
    arrived_at(all_decays.at[pl.ds(0, NZ - 1)], z_sem.at[2])
    for way in range(2):
        arrived_at(states.at[way, pl.ds(0, NX - 1)], x_sem.at[way, 0])
        arrived_at(leaving.at[way, pl.ds(0, NX - 1)], e_sem.at[way, 0])
        arrived_at(groups.at[way, pl.ds(0, NZ - 1)], z_sem.at[4 + way])
        arrived_at(entry.at[way, pl.ds(0, NZ - 1)], z_sem.at[8 + way])
    arrived_at(heads.at[pl.ds(0, 192)], h_sem.at[0])
    arrived_at(w_far, f_sem.at[0])
    cross.wait()
    arrived_at(near, y_sem.at[3])

    def finish(k, carry):
        at = pl.ds(pl.multiple_of(k * 16, 16), 16)
        a = part_a[y, at].astype(F32) + near[0, at].astype(F32) + near[2, at].astype(F32)
        b = part_b[y, at].astype(F32) + near[1, at].astype(F32) + near[3, at].astype(F32)
        pieces = ((whole[at], c, 0), (a, c, WHOLE), (crossed[at], 1 - c, 0), (b, 1 - c, WHOLE))
        square = sum(jnp.sum(v * v, axis=1, keepdims=True) for v, _, _ in pieces)
        scale = lax.rsqrt(square / WIDTH + EPS)
        for v, half, start in pieces:
            span = pl.ds(pl.multiple_of(half * HALF + start, 128), v.shape[1])
            result[at, span] = (
                lat_all[y, at, span].astype(F32) + v * scale * vectors[2:3, span]
            ).astype(BF)
        return carry

    lax.fori_loop(0, count // 16, finish, 0)
    arrived_at(near, y_sem.at[0])
    arrived_at(near.at[pl.ds(0, 2)], y_sem.at[4])


def mixer(*args):
    dma = pltpu.SemaphoreType.DMA
    vm = pltpu.VMEM
    half = vm((64, REST), BF)
    in_specs = [ANY] * len(args)
    slices = vm((2, NX, 128, DK_HEAD), BF)
    thin = vm((2, NZ, 16, DK_HEAD), BF)
    return pl.pallas_call(
        mixer_kernel,
        out_shape=shape_of(64, WIDTH),
        in_specs=in_specs,
        out_specs=VM,
        scratch_shapes=[
            vm((32, WIDTH), BF), vm((1, 128), BF), vm((1, 128), BF),
            vm((WIDTH,), BF), vm((WIDTH,), BF), vm((DV_HEAD,), BF),
            vm((2 * RANK, WIDTH), BF), vm((2, RANK, DK_HEAD), BF), vm((2, DK_HEAD), F32),
            vm((8, WIDTH), F32), vm((8, WIDTH), F32), vm((3, 128, 1024), BF), vm((NZ, 8, 128), F32), vm((NZ, 8, 128), F32),
            vm((8, 128), F32), vm((NY * NX, 8, 128), F32), vm((NY, 8, 128), F32),
            vm((NZ, NY, 8, 128), F32), vm((8, WIDTH), F32), vm((288, 128), F32),
            vm((NY, 64, WIDTH), BF), vm((2, 288, HALF), BF), vm((2, HALF, 1536), BF),
            vm((288, 1536), BF), vm((288, 2 * RANK), BF), vm((2, DV_HEAD, HALF), BF),
            vm((NX, 32, 512), BF), vm((NX, 32, 512), BF),
            slices, slices,
            vm((8, DK_HEAD), F32), vm((NX, 8, DK_HEAD), F32),
            vm((256, 256), BF), vm((256, DV_HEAD), F32), vm((2, 256, DK_HEAD), BF),
            thin, thin, vm((NZ, 2, 16, DK_HEAD), BF), vm((NZ, 2, 16, DK_HEAD), BF),
            vm((8, DK_HEAD), F32), vm((NZ, 8, DK_HEAD), F32),
            thin, thin, vm((2, NX, 128, DK_HEAD), F32), slices, slices,
            vm((256, DV_HEAD), BF),
            vm((NY, 64, REST), BF), vm((NY, 64, REST), BF), vm((4, 64, REST), BF),
            half, half, half, half,
            vm((3, DV_HEAD, WHOLE), BF), vm((NY, 128, DV_HEAD), BF),
            vm((64, WHOLE), F32), vm((64, WHOLE), F32), vm((64, WHOLE), F32),
            dma((4,)), dma((9,)), dma((6,)), dma((1,)), dma((6,)), dma((4,)), dma((4,)),
            dma((2, 2)), dma((12,)), dma((2, 2)), dma((5,)), dma((7,)), dma((6,)),
        ],
        compiler_params=pltpu.CompilerParams(
            collective_id=0, has_side_effects=True, vmem_limit_bytes=60 * 2**20
        ),
        name="mixer",
    )(*args)


def body(
    latents, cond, cond_ctx, context, w_shift, w_scale, w_gate, gain_pre, gain_post,
    w_query, w_key, w_value, w_outgate, w_down, decay_up, decay_bias, head_gain, w_out,
):
    result = mixer(
        latents[0], context[0], cond, cond_ctx[None], gain_pre, gain_post, head_gain,
        w_shift, w_scale, w_gate, w_query, w_key, w_value, w_outgate, w_out,
        w_down.T, decay_up, decay_bias,
    )
    return result[None]


def solution(mesh):
    finer = Mesh(
        mesh.devices.reshape(8, 4, mesh.shape["tp"], mesh.shape["dp"]), ("sp_0", "sp_1", "tp", "dp")
    )
    in_specs = (
        P("dp", SP_TP, None),
        P("dp", SP),
        P(SP),
        P("dp", SP, None),
        P(SP, "tp"),
        P(SP, "tp"),
        P(SP, "tp"),
        P(),
        P(),
        P("dp", "tp"),
        P("dp", "tp"),
        P("dp", "tp"),
        P("dp", "tp"),
        P(),
        P(None, None, "tp"),
        P(None, "tp"),
        P("tp"),
        P("tp", "dp"),
    )
    out_specs = P("dp", SP_TP, None)
    return jax.shard_map(body, mesh=finer, in_specs=in_specs, out_specs=out_specs, check_vma=False)
```
